32 devices in a mesh: rep: 2 (over y), fs: 4 (over z), tp: 4 (over x, core).
Axes of the slice: x: 2, y: 2, z: 4, core: 2. Of those that a mesh axis runs over, the one named last changes fastest.
Arguments:
- tokens: bfloat16 [4096, 2048], P(('rep', 'fs', 'tp')), may hold values from -6 to 6
- norm_gain: float32 [2048], replicated, may hold values from 0.1 to 1.9
- w_gate: bfloat16 [2048, 3072], P('fs', 'tp'), may hold values from -0.125 to 0.125
- w_up: bfloat16 [2048, 3072], P('fs', 'tp'), may hold values from -0.125 to 0.125
- w_down: bfloat16 [3072, 2048], P('tp', 'fs'), may hold values from -0.109375 to 0.109375
- post_gain: float32 [2048], replicated, may hold values from 0.1 to 1.9
Outputs:
- result: bfloat16 [4096, 2048], P(('rep', 'fs', 'tp'))
The draws below stay inside these ranges and needn't reach their ends.
All inputs are finite; a program needn't handle non-finite values.
Results may differ from the reference program's by a relative error of at most 0.014.
Values may be sent and summed in bfloat16 or wider, within the bound.
A program may use at most 64 MiB of HBM per device.

```python
import jax
import jax.numpy as jnp
from jax import lax

D = 2048
FF = 3072
TOKENS = 4096
N_TP = 4


def block_scale(own_key, dims, split, smallest, top_value):
    level, own = 1.0, jax.random.fold_in(own_key, 6)
    for axis_at, blocks in split:
        heights = jnp.exp(jax.random.uniform(jax.random.fold_in(own, axis_at), (blocks,), jnp.float32, smallest / len(split), top_value / len(split)))
        level = level * jnp.repeat(heights, dims[axis_at] // blocks).reshape([-1 if axis == axis_at else 1 for axis in range(len(dims))])
    return level


def bell_draw(rng, dims, width, limit, split=(), held_as=jnp.bfloat16):
    values = width * jax.random.normal(rng, dims, jnp.float32)
    if split:
        values = values * block_scale(rng, dims, split, -0.22, 0.18)
    return jnp.clip(values, -limit, limit).astype(held_as)


def setup_inputs(seed: int = 0) -> dict:
    streams_of = jax.random.split(jax.random.key(seed), 7)
    return {
        "tokens": bell_draw(streams_of[0], (TOKENS, D), 1.0, 6.0, ((0, 32),)),
        "norm_gain": jnp.clip(1.0 + 0.18 * jax.random.normal(streams_of[1], (D,), jnp.float32), 0.1, 1.9),
        "w_gate": bell_draw(streams_of[2], (D, FF), D ** -0.5, 0.125, ((0, 4), (1, 4))),
        "w_up": bell_draw(streams_of[3], (D, FF), D ** -0.5, 0.125, ((0, 4), (1, 4))),
        "w_down": bell_draw(streams_of[4], (FF, D), FF ** -0.5, 0.109375, ((0, 4), (1, 4))),
        "post_gain": jnp.clip(1.0 + 0.18 * jax.random.normal(streams_of[5], (D,), jnp.float32), 0.1, 1.9),
    }


EPS = 1e-06

def rms_scale(values, gain):
    return values * lax.rsqrt(lax.optimization_barrier(jnp.mean(values * values, axis=-1, keepdims=True)) + EPS) * gain

def reference(tokens, norm_gain, w_gate, w_up, w_down, post_gain):
    normed = rms_scale(tokens.astype(jnp.float32), norm_gain).astype(jnp.bfloat16)
    gate = jnp.dot(normed, w_gate, preferred_element_type=jnp.float32)
    up = jnp.dot(normed, w_up, preferred_element_type=jnp.float32)
    hidden = (jax.nn.silu(gate) * up).astype(jnp.bfloat16)
    block = FF // N_TP
    summed = jnp.zeros((tokens.shape[0], D), jnp.float32)
    for index in range(N_TP):
        partial_block = jnp.dot(hidden[:, index * block:(index + 1) * block], w_down[index * block:(index + 1) * block], preferred_element_type=jnp.float32).astype(jnp.bfloat16)
        partial_block = lax.optimization_barrier(partial_block)
        summed = summed + partial_block.astype(jnp.float32)
    return rms_scale(summed, post_gain).astype(jnp.bfloat16)
```

```python
import functools

import jax
import jax.numpy as jnp
from jax import lax
from jax.experimental import pallas as pl
from jax.experimental.pallas import tpu as pltpu
from jax.sharding import PartitionSpec as P

EPS = 1e-06
MESH = pl.DeviceIdType.MESH
PIECE = 256
LANES = 128


def rms_scale(values, gain):
    return values * lax.rsqrt(jnp.mean(values * values, axis=-1, keepdims=True) + EPS) * gain


def plain_body(tokens, norm_gain, w_gate, w_up, w_down, post_gain):
    own_normed = rms_scale(tokens.astype(jnp.float32), norm_gain).astype(jnp.bfloat16)
    normed = lax.all_gather(own_normed, "tp", axis=0, tiled=True)
    gate = jnp.dot(
        normed, lax.all_gather(w_gate, "fs", axis=0, tiled=True), preferred_element_type=jnp.float32
    )
    up = jnp.dot(
        normed, lax.all_gather(w_up, "fs", axis=0, tiled=True), preferred_element_type=jnp.float32
    )
    hidden = (jax.nn.silu(gate) * up).astype(jnp.bfloat16)
    terms = jnp.dot(
        hidden, lax.all_gather(w_down, "fs", axis=1, tiled=True), preferred_element_type=jnp.float32
    )
    summed = lax.psum_scatter(
        terms.astype(jnp.bfloat16), "tp", scatter_dimension=0, tiled=True
    ).astype(jnp.float32)
    return rms_scale(summed, post_gain).astype(jnp.bfloat16)


def kernel(
    n, rows, depth, part, width, cuts, lanes,
    tok_ref, gain_ref, wg_ref, wu_ref, wd_ref, post_ref, out_ref,
    raw, tok, gu, dn, hid, hdel, kept, pair_out, pair_in, cross_out, cross_in, fin,
    tok_l, gu_l, dn_l, z_s, z_r, tok_s, tok_r, gu_s, gu_r, dn_s, dn_r, hid_s, hid_r,
    pair_s, pair_r, cross_s, cross_r,
):
    r, k, t = lax.axis_index("rep"), lax.axis_index("fs"), lax.axis_index("tp")
    x, c = t // 2, t % 2
    t_pair, t_x, r_y = x * 2 + (1 - c), (1 - x) * 2 + c, 1 - r
    t_px = (1 - x) * 2 + (1 - c)
    partner, along_x, along_y, diag = {"tp": t_pair}, {"tp": t_x}, {"rep": r_y}, {"rep": r_y, "tp": t_x}
    left = k < n // 2
    last = jnp.where(left, 0, n - 1)
    near = jnp.where(left, 1, n - 2)
    far_near, far_last = n - 1 - near, n - 1 - last
    at_end = k == last
    in_middle = k != last
    inner, outer = {"fs": jnp.where(left, k + 1, k - 1)}, {"fs": last}
    blocks = part // lanes
    sub = width // cuts
    half = pl.multiple_of(r * part, part)
    halves = rows // 2

    def gu_load(b, q):
        ref = (wg_ref, wu_ref)[q]
        at = pl.ds(pl.multiple_of(k * depth, depth), depth)
        return pltpu.make_async_copy(
            ref.at[:, pl.ds(half + b * lanes, lanes)], gu.at[b, at, pl.ds(q * lanes, lanes)], gu_l.at[b, q]
        )

    def dn_load(j):
        return pltpu.make_async_copy(
            wd_ref.at[pl.ds(half, part), pl.ds(j * sub, sub)], dn.at[k, j], dn_l.at[j]
        )

    tok_load = pltpu.make_async_copy(tok_ref, raw, tok_l)

    tok_load.start()
    for b in range(blocks):
        for q in (0, 1):
            gu_load(b, q).start()
    for j in range(cuts):
        dn_load(j).start()

    barrier = pltpu.get_barrier_semaphore()
    for where in (partner, along_x, along_y, diag, inner):
        pl.semaphore_signal(barrier, inc=1, device_id=where, device_id_type=MESH)

    @pl.when(in_middle)
    def _():
        pl.semaphore_signal(barrier, inc=1, device_id=outer, device_id_type=MESH)

    pl.semaphore_wait(barrier, 5 + jnp.where(in_middle, 1, 0))

    def remote(ref, send, recv, where, to=None):
        return pltpu.make_async_remote_copy(
            ref, ref if to is None else to, send, recv, device_id=where, device_id_type=MESH
        )

    def gu_at(s, b):
        return gu.at[b, pl.ds(pl.multiple_of(s * depth, depth), depth)]

    def gu_send(kind, b):
        s = last if kind else k
        return remote(gu_at(s, b), gu_s.at[kind, b], gu_r.at[s, b], inner)

    def gu_wait(s, b):
        remote(gu_at(s, b), gu_s.at[0, b], gu_r.at[s, b], inner).wait_recv()

    def dn_send(way, s, j):
        return remote(dn.at[s, j], dn_s.at[way, s, j], dn_r.at[s, j], outer if way else inner)

    def dn_wait(s, j):
        remote(dn.at[s, j], dn_s.at[0, s, j], dn_r.at[s, j], inner).wait_recv()

    def rows_of(p, r_at, t_at, h):
        return tok.at[p, pl.ds((r_at * 4 + t_at) * rows + h * halves, halves)]

    def z_send(h):
        return remote(rows_of(0, r, t, h), z_s.at[h], z_r.at[h], inner, rows_of(1, r, t, h))

    def z_wait(h):
        remote(rows_of(1, r, t, h), z_s.at[h], z_r.at[h], inner).wait_recv()

    U, L = 0, 1
    sends = [
        ((r, t, U), along_x), ((r, t, L), along_x), ((r, t, U), along_y), ((r, t, L), along_y),
        ((r, t_x, U), along_y), ((r_y, t, L), along_x),
        ((r, t, U), partner), ((r, t, L), partner),
        ((r, t_x, U), partner), ((r, t_x, L), partner),
        ((r_y, t, U), partner), ((r_y, t, L), partner),
        ((r_y, t_x, U), partner), ((r_y, t_x, L), partner),
    ]
    lands = [
        (r, t_x, U), (r, t_x, L), (r_y, t, U), (r_y, t, L),
        (r_y, t_x, U), (r_y, t_x, L),
        (r, t_pair, U), (r, t_pair, L),
        (r, t_px, U), (r, t_px, L),
        (r_y, t_pair, U), (r_y, t_pair, L),
        (r_y, t_px, U), (r_y, t_px, L),
    ]

    def tok_send(p, i):
        at, where = sends[i]
        return remote(rows_of(p, *at), tok_s.at[p, i], tok_r.at[p, i], where)

    def go(p, *which):
        for i in which:
            tok_send(p, i).start()

    def got(p, *which):
        for i in which:
            remote(rows_of(p, *lands[i]), tok_s.at[p, i], tok_r.at[p, i], partner).wait_recv()

    quarter = 2 * rows

    def hid_send(b, m):
        at = (pl.ds(pl.multiple_of(m * quarter, quarter), quarter), pl.ds(b * lanes, lanes))
        return remote(hdel.at[at], hid_s.at[b, m], hid_r.at[b, m], outer, hid.at[at])

    def hid_wait(b, m):
        at = (pl.ds(pl.multiple_of(m * quarter, quarter), quarter), pl.ds(b * lanes, lanes))
        remote(hid.at[at], hid_s.at[b, m], hid_r.at[b, m], partner).wait_recv()

    def gated(p, b, m):
        at = pl.ds(pl.multiple_of(m * quarter, quarter), quarter)
        both = jnp.dot(tok[p, at, :], gu[b], preferred_element_type=jnp.float32)
        gate, up = both[:, :lanes], both[:, lanes:]
        value = (gate / (1.0 + jnp.exp(-gate)) * up).astype(jnp.bfloat16)
        (hdel if p else hid)[at, pl.ds(b * lanes, lanes)] = value

    def own_block(b):
        @pl.loop(0, 4)
        def _(m):
            gated(0, b, m)

    def passed_block(b):
        @pl.loop(0, 4)
        def _(m):
            gated(1, b, m)
            hid_send(b, m).start()

    def send_own_gu():
        for b in range(blocks):
            gu_load(b, 0).wait()
            gu_load(b, 1).wait()
            gu_send(0, b).start()

    @pl.when(in_middle)
    def _():
        send_own_gu()
        for j in range(cuts):
            dn_load(j).wait()
            dn_send(1, k, j).start()

    tok_load.wait()
    tile = 32
    first = (r * 4 + t) * rows

    @pl.loop(0, rows // tile)
    def _(i):
        at = pl.ds(pl.multiple_of(i * tile, tile), tile)
        to = pl.ds(pl.multiple_of(first + i * tile, tile), tile)
        tok[0, to, :] = rms_scale(raw[at, :].astype(jnp.float32), gain_ref[...]).astype(jnp.bfloat16)

    @pl.when(at_end)
    def _():
        z_send(U).start()
        z_send(L).start()
        send_own_gu()
        for j in range(cuts):
            dn_load(j).wait()
            dn_send(0, k, j).start()

    @pl.when(in_middle)
    def _():
        go(0, 0, 2, 6, 7)
        z_wait(U)
        go(1, 0, 2, 6)
        got(0, 0)
        go(0, 8)
        got(0, 2)
        go(0, 10)
        z_wait(L)
        go(1, 1, 3, 7)
        got(1, 0)
        go(1, 4, 8)
        got(1, 2)
        go(1, 10)
        gu_wait(last, 0)
        gu_send(1, 0).start()
        got(1, 3)
        go(1, 5, 11)
        got(1, 1)
        go(1, 9)
        go(0, 1, 3, 4)
        for b in range(1, blocks - 1):
            gu_wait(last, b)
            gu_send(1, b).start()
        got(1, 4)
        go(1, 12)
        got(1, 5)
        go(1, 13)
        got(1, 6, 7, 8, 9, 10, 11, 12, 13)
        for b in range(blocks - 1):
            gu_wait(far_near, b)
            gu_wait(far_last, b)
            passed_block(b)
            if b == 0:
                gu_wait(last, blocks - 1)
                gu_send(1, blocks - 1).start()
                for j in range(cuts):
                    dn_send(0, k, j).start()
        got(0, 3)
        go(0, 5, 11)
        got(0, 1)
        go(0, 9)
        got(0, 4)
        go(0, 12)
        got(0, 5)
        go(0, 13)
        got(0, 6, 7, 8, 9, 10, 11, 12, 13)
        for b in range(blocks - 1):
            own_block(b)
        gu_wait(far_near, blocks - 1)
        gu_wait(far_last, blocks - 1)
        passed_block(blocks - 1)
        own_block(blocks - 1)

    mine = r * 2 + x
    others = ((r * 2 + (1 - x), along_x), (r_y * 2 + x, along_y), (r_y * 2 + (1 - x), diag))

    def pair_copy(p):
        return pltpu.make_async_remote_copy(
            pair_out.at[p], pair_in.at[p], pair_s.at[p], pair_r.at[p], device_id=partner, device_id_type=MESH
        )

    def cross_copy(p, to, where):
        return pltpu.make_async_remote_copy(
            cross_out.at[p, to], cross_in.at[p, mine], cross_s.at[p, to], cross_r.at[p, mine],
            device_id=where, device_id_type=MESH,
        )

    def source(i):
        near_or_last = jnp.where(i == 0, k, near + last - k)
        return jnp.where(i < 2, near_or_last, jnp.where(i == 2, far_near, far_last))

    def product(m, core, s, j):
        at = pl.ds(pl.multiple_of((m * 2 + core) * rows, rows), rows)
        return jnp.dot(hid[at, :], dn[s, j], preferred_element_type=jnp.float32)

    def finish(i, j, slot):
        p = source(i) * cuts + j
        pair_copy(p).wait_recv()
        for to, where in (others[2], others[0], others[1]):
            cross_out[p, to] = (kept[slot, to] + pair_in[p, to].astype(jnp.float32)).astype(jnp.bfloat16)
        for to, where in (others[2], others[0], others[1]):
            cross_copy(p, to, where).start()
        fin[p] = kept[slot, mine] + pair_in[p, mine].astype(jnp.float32)

    @pl.loop(0, n * cuts)
    def _(at):
        i, j, slot = at // cuts, at % cuts, at % 2
        s = source(i)
        p = s * cuts + j

        @pl.when(at > 0)
        def _():
            finish((at - 1) // cuts, (at - 1) % cuts, 1 - slot)

        @pl.when(i > 0)
        def _():
            dn_wait(s, j)

        @pl.when((i == 1) & in_middle)
        def _():
            dn_send(0, s, j).start()

        @pl.when((i > 1) & in_middle)
        def _():
            dn_send(1, s, j).start()

        @pl.loop(0, 4)
        def _(m):
            @pl.when((at == 0) & at_end)
            def _():
                for b in range(blocks):
                    hid_wait(b, m)

            pair_out[p, m] = product(m, 1 - c, s, j).astype(jnp.bfloat16)

        pair_copy(p).start()

        @pl.loop(0, 4)
        def _(m):
            kept[slot, m] = product(m, c, s, j)

    finish(n - 1, cuts - 1, (n * cuts - 1) % 2)

    for p in range(n * cuts):
        for other, _ in others:
            pltpu.make_async_remote_copy(
                cross_out.at[p, 0], cross_in.at[p, other], cross_s.at[p, 0],
                cross_r.at[p, other], device_id=along_x, device_id_type=MESH,
            ).wait_recv()

    piece = 32

    @pl.loop(0, rows // piece)
    def _(i):
        at = pl.ds(pl.multiple_of(i * piece, piece), piece)
        parts = []
        for p in range(n * cuts):
            total = fin[p, at, :]
            for other, _ in others:
                total = total + cross_in[p, other, at, :].astype(jnp.float32)
            parts.append(total)
        square = sum(jnp.sum(b * b, axis=-1, keepdims=True) for b in parts)
        scale = lax.rsqrt(square / (n * width) + EPS)
        for p in range(n * cuts):
            cols = pl.ds(p * sub, sub)
            out_ref[at, cols] = (parts[p] * scale * post_ref[:, cols]).astype(out_ref.dtype)

    for b in range(blocks):
        gu_send(0, b).wait_send()

    @pl.when(at_end)
    def _():
        z_send(U).wait_send()
        z_send(L).wait_send()
        for j in range(cuts):
            dn_send(0, k, j).wait_send()

    @pl.when(in_middle)
    def _():
        for p in (0, 1):
            for i in range(len(sends)):
                tok_send(p, i).wait_send()
        for b in range(blocks):
            gu_send(1, b).wait_send()
            for m in range(4):
                hid_send(b, m).wait_send()
        for j in range(cuts):
            dn_send(0, k, j).wait_send()
            dn_send(0, last, j).wait_send()
            dn_send(1, k, j).wait_send()
            dn_send(1, far_near, j).wait_send()
            dn_send(1, far_last, j).wait_send()

    for p in range(n * cuts):
        pair_copy(p).wait_send()
        for to, where in others:
            cross_copy(p, to, where).wait_send()


def chain_body(n, tokens, norm_gain, w_gate, w_up, w_down, post_gain):
    rows, model = tokens.shape
    depth, block = w_gate.shape
    width = w_down.shape[1]
    part = block // 2
    cuts = max(1, width // PIECE)
    sub = width // cuts
    blocks = part // LANES
    vmem, dma = pltpu.VMEM, pltpu.SemaphoreType.DMA
    low, full = jnp.bfloat16, jnp.float32
    anywhere = pl.BlockSpec(memory_space=pl.ANY)
    inside = pl.BlockSpec(memory_space=vmem)
    return pl.pallas_call(
        functools.partial(kernel, n, rows, depth, part, width, cuts, LANES),
        out_shape=jax.ShapeDtypeStruct((rows, model), low),
        in_specs=[anywhere, inside, anywhere, anywhere, anywhere, inside],
        out_specs=inside,
        scratch_shapes=[
            vmem((rows, model), low),
            vmem((2, 8 * rows, model), low),
            vmem((blocks, n * depth, 2 * LANES), low),
            vmem((n, cuts, part, sub), low),
            vmem((8 * rows, part), low),
            vmem((8 * rows, part), low),
            vmem((2, 4, rows, sub), full),
            vmem((n * cuts, 4, rows, sub), low),
            vmem((n * cuts, 4, rows, sub), low),
            vmem((n * cuts, 4, rows, sub), low),
            vmem((n * cuts, 4, rows, sub), low),
            vmem((n * cuts, rows, sub), full),
            dma(()),
            dma((blocks, 2)),
            dma((cuts,)),
            dma((2,)),
            dma((2,)),
            dma((2, 14)),
            dma((2, 14)),
            dma((2, blocks)),
            dma((n, blocks)),
            dma((2, n, cuts)),
            dma((n, cuts)),
            dma((blocks, 4)),
            dma((blocks, 4)),
            dma((n * cuts,)),
            dma((n * cuts,)),
            dma((n * cuts, 4)),
            dma((n * cuts, 4)),
        ],
        compiler_params=pltpu.CompilerParams(
            collective_id=0, has_side_effects=True, vmem_limit_bytes=56 * 2**20
        ),
    )(tokens, norm_gain.reshape(1, -1), w_gate, w_up, w_down, post_gain.reshape(1, -1))


def solution(mesh):
    n = mesh.shape["fs"]

    def body(tokens, norm_gain, w_gate, w_up, w_down, post_gain):
        args = (tokens, norm_gain, w_gate, w_up, w_down, post_gain)
        rows = tokens.shape[0]
        fits = (
            mesh.shape["rep"] == 2 and mesh.shape["tp"] == 4 and n == 4 and rows <= 128
            and rows % 64 == 0 and w_gate.shape[1] % 256 == 0 and w_down.shape[1] % PIECE == 0
        )
        return chain_body(n, *args) if fits else plain_body(*args)

    return jax.shard_map(
        body,
        mesh=mesh,
        in_specs=(
            P(("rep", "fs", "tp"), None),
            P(),
            P("fs", "tp"),
            P("fs", "tp"),
            P("tp", "fs"),
            P(),
        ),
        out_specs=P(("rep", "fs", "tp"), None),
        check_vma=False,
    )
```

```python
import functools

import jax
import jax.numpy as jnp
from jax import lax
from jax.experimental import pallas as pl
from jax.experimental.pallas import tpu as pltpu
from jax.sharding import PartitionSpec as P

EPS = 1e-06
MESH = pl.DeviceIdType.MESH
PIECE = 256
LANES = 128


def rms_scale(values, gain):
    return values * lax.rsqrt(jnp.mean(values * values, axis=-1, keepdims=True) + EPS) * gain


def plain_body(tokens, norm_gain, w_gate, w_up, w_down, post_gain):
    own_normed = rms_scale(tokens.astype(jnp.float32), norm_gain).astype(jnp.bfloat16)
    normed = lax.all_gather(own_normed, "tp", axis=0, tiled=True)
    gate = jnp.dot(
        normed, lax.all_gather(w_gate, "fs", axis=0, tiled=True), preferred_element_type=jnp.float32
    )
    up = jnp.dot(
        normed, lax.all_gather(w_up, "fs", axis=0, tiled=True), preferred_element_type=jnp.float32
    )
    hidden = (jax.nn.silu(gate) * up).astype(jnp.bfloat16)
    terms = jnp.dot(
        hidden, lax.all_gather(w_down, "fs", axis=1, tiled=True), preferred_element_type=jnp.float32
    )
    summed = lax.psum_scatter(
        terms.astype(jnp.bfloat16), "tp", scatter_dimension=0, tiled=True
    ).astype(jnp.float32)
    return rms_scale(summed, post_gain).astype(jnp.bfloat16)


def kernel(
    n, rows, depth, part, width, cuts, lanes,
    tok_ref, gain_ref, wg_ref, wu_ref, wd_ref, post_ref, out_ref,
    raw, tok, gu, dn, hid, hdel, kept, pair_out, pair_in, half_out, half_in, full_out, full_in, fin, squares,
    tok_l, gu_l, dn_l, z_s, z_r, tok_s, tok_r, gu_s, gu_r, dn_s, dn_r, hid_s, hid_r,
    pair_s, pair_r, half_s, half_r, full_s, full_r,
):
    r, k, t = lax.axis_index("rep"), lax.axis_index("fs"), lax.axis_index("tp")
    x, c = t // 2, t % 2
    t_pair, t_x, r_y = x * 2 + (1 - c), (1 - x) * 2 + c, 1 - r
    t_px = (1 - x) * 2 + (1 - c)
    partner, along_x, along_y, diag = {"tp": t_pair}, {"tp": t_x}, {"rep": r_y}, {"rep": r_y, "tp": t_x}
    left = k < n // 2
    last = jnp.where(left, 0, n - 1)
    near = jnp.where(left, 1, n - 2)
    far_near, far_last = n - 1 - near, n - 1 - last
    at_end = k == last
    in_middle = k != last
    inner, outer = {"fs": jnp.where(left, k + 1, k - 1)}, {"fs": last}
    blocks = part // lanes
    sub = width // cuts
    half = pl.multiple_of(r * part, part)
    piece = rows // 4

    def gu_load(b, q):
        ref = (wg_ref, wu_ref)[q]
        at = pl.ds(pl.multiple_of(k * depth, depth), depth)
        return pltpu.make_async_copy(
            ref.at[:, pl.ds(half + b * lanes, lanes)], gu.at[b, at, pl.ds(q * lanes, lanes)], gu_l.at[b, q]
        )

    def dn_load(j):
        return pltpu.make_async_copy(
            wd_ref.at[pl.ds(half, part), pl.ds(j * sub, sub)], dn.at[k, j], dn_l.at[j]
        )

    tok_load = pltpu.make_async_copy(tok_ref, raw, tok_l)

    tok_load.start()
    for b in range(blocks):
        for q in (0, 1):
            gu_load(b, q).start()
    for j in range(cuts):
        dn_load(j).start()

    barrier = pltpu.get_barrier_semaphore()
    for where in (partner, along_x, along_y, diag, inner):
        pl.semaphore_signal(barrier, inc=1, device_id=where, device_id_type=MESH)

    @pl.when(in_middle)
    def _():
        pl.semaphore_signal(barrier, inc=1, device_id=outer, device_id_type=MESH)

    pl.semaphore_wait(barrier, 5 + jnp.where(in_middle, 1, 0))

    def remote(ref, send, recv, where, to=None):
        return pltpu.make_async_remote_copy(
            ref, ref if to is None else to, send, recv, device_id=where, device_id_type=MESH
        )

    def gu_at(s, b):
        return gu.at[b, pl.ds(pl.multiple_of(s * depth, depth), depth)]

    def gu_send(kind, b):
        s = last if kind else k
        return remote(gu_at(s, b), gu_s.at[kind, b], gu_r.at[s, b], inner)

    def gu_wait(s, b):
        remote(gu_at(s, b), gu_s.at[0, b], gu_r.at[s, b], inner).wait_recv()

    def dn_send(way, s, j):
        return remote(dn.at[s, j], dn_s.at[way, s, j], dn_r.at[s, j], outer if way else inner)

    def dn_wait(s, j):
        remote(dn.at[s, j], dn_s.at[0, s, j], dn_r.at[s, j], inner).wait_recv()

    def rows_of(p, r_at, t_at, first, count):
        base = ((t_at % 2) * 4 + r_at * 2 + t_at // 2) * rows
        return tok.at[p, pl.ds(base + first * piece, count * piece)]

    def z_send(i):
        return remote(rows_of(0, r, t, i, 1), z_s.at[i], z_r.at[i], inner, rows_of(1, r, t, i, 1))

    def z_wait(i):
        remote(rows_of(1, r, t, i, 1), z_s.at[i], z_r.at[i], inner).wait_recv()

    sends = (
        [((r, t, i, 1), along_x) for i in range(4)]
        + [((r, t, i, 1), along_y) for i in range(4)]
        + [((r, t_x, 0, 1), along_y), ((r, t_x, 1, 1), along_y), ((r_y, t, 2, 1), along_x), ((r_y, t, 3, 1), along_x)]
        + [((r_at, t_at, i, 2), partner) for r_at, t_at in ((r, t), (r, t_x), (r_y, t), (r_y, t_x)) for i in (0, 2)]
    )
    lands = (
        [(r, t_x, i, 1) for i in range(4)]
        + [(r_y, t, i, 1) for i in range(4)]
        + [(r_y, t_x, i, 1) for i in range(4)]
        + [(r_at, t_at, i, 2) for r_at, t_at in ((r, t_pair), (r, t_px), (r_y, t_pair), (r_y, t_px)) for i in (0, 2)]
    )

    def tok_send(p, i):
        at, where = sends[i]
        return remote(rows_of(p, *at), tok_s.at[p, i], tok_r.at[p, i], where)

    def go(p, *which):
        for i in which:
            tok_send(p, i).start()

    def got(p, *which):
        for i in which:
            remote(rows_of(p, *lands[i]), tok_s.at[p, i], tok_r.at[p, i], partner).wait_recv()

    quarter = 2 * rows

    def hid_send(b, m):
        at = (pl.ds(pl.multiple_of(m * quarter, quarter), quarter), pl.ds(b * lanes, lanes))
        return remote(hdel.at[at], hid_s.at[b, m], hid_r.at[b, m], outer, hid.at[at])

    def hid_wait(b, m):
        at = (pl.ds(pl.multiple_of(m * quarter, quarter), quarter), pl.ds(b * lanes, lanes))
        remote(hid.at[at], hid_s.at[b, m], hid_r.at[b, m], partner).wait_recv()

    def gated(p, b, m):
        at = pl.ds(pl.multiple_of(m * quarter, quarter), quarter)
        both = jnp.dot(tok[p, at, :], gu[b], preferred_element_type=jnp.float32)
        gate, up = both[:, :lanes], both[:, lanes:]
        value = (gate / (1.0 + jnp.exp(-gate)) * up).astype(jnp.bfloat16)
        (hdel if p else hid)[at, pl.ds(b * lanes, lanes)] = value

    def own_block(b, r_at):
        @pl.loop(0, 2)
        def _(i):
            gated(0, b, i * 2 + r_at)

    def passed_block(b):
        @pl.loop(0, 4)
        def _(i):
            m = ((1 - c) * 2 + i) % 4
            gated(1, b, m)
            hid_send(b, m).start()

    def send_own_gu():
        for b in range(blocks):
            gu_load(b, 0).wait()
            gu_load(b, 1).wait()
            gu_send(0, b).start()

    @pl.when(in_middle)
    def _():
        send_own_gu()
        for j in range(cuts):
            dn_load(j).wait()
            dn_send(1, k, j).start()

    tok_load.wait()
    tile = 32
    first = (c * 4 + r * 2 + x) * rows

    @pl.loop(0, rows // tile)
    def _(i):
        at = pl.ds(pl.multiple_of(i * tile, tile), tile)
        to = pl.ds(pl.multiple_of(first + i * tile, tile), tile)
        tok[0, to, :] = rms_scale(raw[at, :].astype(jnp.float32), gain_ref[...]).astype(jnp.bfloat16)

    @pl.when(at_end)
    def _():
        for i in range(4):
            z_send(i).start()
        send_own_gu()
        for j in range(cuts):
            dn_load(j).wait()
            dn_send(0, k, j).start()

    @pl.when(in_middle)
    def _():
        go(0, 0, 1, 6, 7, 12, 13)
        z_wait(0)
        go(1, 0, 4)
        got(0, 0, 1)
        go(0, 14)
        got(0, 6, 7)
        go(0, 17)
        z_wait(1)
        go(1, 1, 5, 12)
        got(1, 0, 4)
        z_wait(2)
        go(1, 2, 6)
        got(1, 1, 5)
        go(1, 14, 16)
        z_wait(3)
        go(1, 3, 7, 13, 8, 9)
        got(1, 6)
        go(1, 10)
        got(1, 7)
        go(1, 11, 17)
        got(1, 2, 3)
        go(1, 15)
        go(0, 2, 3, 4, 5, 8, 9, 10, 11)
        gu_wait(last, 0)
        gu_send(1, 0).start()
        gu_wait(last, 1)
        gu_send(1, 1).start()
        got(1, 8, 9)
        go(1, 18)
        got(1, 10, 11)
        go(1, 19)
        got(1, 12, 13, 14, 15, 16, 17, 18, 19)
        gu_wait(far_near, 0)
        gu_wait(far_last, 0)
        passed_block(0)
        got(0, 2, 3)
        go(0, 15)
        got(0, 4, 5)
        go(0, 16)
        gu_wait(last, 2)
        gu_send(1, 2).start()
        gu_wait(far_near, 1)
        gu_wait(far_last, 1)
        passed_block(1)
        got(0, 12, 13, 14, 15)
        own_block(0, r)
        own_block(1, r)
        dn_wait(last, 0)
        got(0, 8, 9)
        go(0, 18)
        got(0, 10, 11)
        go(0, 19)
        gu_wait(far_near, 2)
        gu_wait(far_last, 2)
        for j in range(cuts):
            dn_send(0, k, j).start()
        dn_send(0, last, 0).start()
        passed_block(2)
        dn_wait(last, 1)
        dn_send(0, last, 1).start()
        own_block(2, r)
        got(0, 16, 17, 18, 19)
        own_block(0, r_y)
        own_block(1, r_y)
        dn_wait(far_near, 0)
        dn_send(1, far_near, 0).start()
        own_block(2, r_y)

    mine, at_x, at_y, at_diag = r * 2 + x, r * 2 + (1 - x), r_y * 2 + x, r_y * 2 + (1 - x)
    chunks = n * cuts
    slots = 2
    mid = sub // 2

    def of(m):
        return pl.ds(pl.multiple_of(m * rows, rows), rows)

    def pair_copy(p):
        return remote(pair_out.at[p], pair_s.at[p], pair_r.at[p], partner, pair_in.at[p])

    def half_copy(p, way):
        return remote(
            half_out.at[p, way], half_s.at[p, way], half_r.at[p, way], along_y if way else along_x, half_in.at[p, way]
        )

    def full_copy(p, way):
        return remote(
            full_out.at[p, way], full_s.at[p, way], full_r.at[p, way], along_y if way else along_x, full_in.at[p, way]
        )

    def source(i):
        near_or_last = jnp.where(i == 0, k, near + last - k)
        return jnp.where(i < 2, near_or_last, jnp.where(i == 2, far_near, far_last))

    def place(at):
        return source(at // cuts) * cuts + at % cuts

    def product(core, s, j):
        at = pl.ds(pl.multiple_of(core * 4 * rows, 4 * rows), 4 * rows)
        return jnp.dot(hid[at, :], dn[s, j], preferred_element_type=jnp.float32)

    def finish_pair(at):
        p, slot = place(at), at % slots
        pair_copy(p).wait_recv()

        def summed(m):
            return kept[slot, of(m), :] + pair_in[p, of(m), :].astype(jnp.float32)

        across = summed(at_diag).astype(jnp.bfloat16)
        half_out[p, 0] = across[:, :mid]
        half_out[p, 1] = across[:, mid:]
        half_copy(p, 0).start()
        half_copy(p, 1).start()
        kept[slot, of(at_x), :] = summed(at_x)
        kept[slot, of(at_y), :] = summed(at_y)
        fin[p] = summed(mine)

    def finish_half(at):
        p, slot = place(at), at % slots
        half_copy(p, 1).wait_recv()
        full_out[p, 0, :, :mid] = kept[slot, of(at_x), :mid].astype(jnp.bfloat16)
        full_out[p, 0, :, mid:] = (kept[slot, of(at_x), mid:] + half_in[p, 1].astype(jnp.float32)).astype(jnp.bfloat16)
        full_copy(p, 0).start()
        half_copy(p, 0).wait_recv()
        full_out[p, 1, :, mid:] = kept[slot, of(at_y), mid:].astype(jnp.bfloat16)
        full_out[p, 1, :, :mid] = (kept[slot, of(at_y), :mid] + half_in[p, 0].astype(jnp.float32)).astype(jnp.bfloat16)
        full_copy(p, 1).start()

    def pass_down(s, j):
        dn_wait(s, j)
        dn_send(1, s, j).start()

    @pl.loop(0, chunks)
    def _(at):
        i, j, slot = at // cuts, at % cuts, at % slots
        s = source(i)
        p = s * cuts + j

        for step, (from_s, from_j) in ((1, (far_near, 1)), (2, (far_last, 0)), (4, (far_last, 1))):
            @pl.when(in_middle & (at == step))
            def _():
                pass_down(from_s, from_j)

        @pl.when((i > 0) & at_end)
        def _():
            dn_wait(s, j)

        def arrived(core):
            @pl.when((at == 0) & at_end)
            def _():
                for b in range(blocks):
                    for half_at in (0, 1):
                        hid_wait(b, core * 2 + half_at)

        arrived(1 - c)
        pair_out[p] = product(1 - c, s, j).astype(jnp.bfloat16)
        pair_copy(p).start()
        arrived(c)
        kept[slot] = product(c, s, j)
        finish_pair(at)

        @pl.when(at > 0)
        def _():
            finish_half(at - 1)

    finish_half(chunks - 1)

    for b in range(blocks):
        gu_send(0, b).wait_send()

    @pl.when(at_end)
    def _():
        for i in range(4):
            z_send(i).wait_send()
        for j in range(cuts):
            dn_send(0, k, j).wait_send()

    @pl.when(in_middle)
    def _():
        for p in (0, 1):
            for i in range(len(sends)):
                tok_send(p, i).wait_send()
        for b in range(blocks):
            gu_send(1, b).wait_send()
            for m in range(4):
                hid_send(b, m).wait_send()
        for j in range(cuts):
            dn_send(0, k, j).wait_send()
            dn_send(0, last, j).wait_send()
            dn_send(1, k, j).wait_send()
            dn_send(1, far_near, j).wait_send()
            dn_send(1, far_last, j).wait_send()

    for p in range(chunks):
        pair_copy(p).wait_send()
        for way in (0, 1):
            half_copy(p, way).wait_send()

    squares[...] = jnp.zeros_like(squares)

    @pl.loop(0, chunks)
    def _(at):
        p = place(at)
        for way in (0, 1):
            full_copy(p, way).wait_send()
            full_copy(p, way).wait_recv()
        total = fin[p] + full_in[p, 0].astype(jnp.float32) + full_in[p, 1].astype(jnp.float32)
        fin[p] = total
        squares[...] += total[:, :mid] * total[:, :mid] + total[:, mid:] * total[:, mid:]

    scale = lax.rsqrt(jnp.sum(squares[...], axis=-1, keepdims=True) / (n * width) + EPS)
    for p in range(chunks):
        cols = pl.ds(p * sub, sub)
        out_ref[:, cols] = (fin[p] * scale * post_ref[:, cols]).astype(out_ref.dtype)


def chain_body(n, tokens, norm_gain, w_gate, w_up, w_down, post_gain):
    rows, model = tokens.shape
    depth, block = w_gate.shape
    width = w_down.shape[1]
    part = block // 2
    cuts = max(1, width // PIECE)
    sub = width // cuts
    blocks = part // LANES
    vmem, dma = pltpu.VMEM, pltpu.SemaphoreType.DMA
    low, full = jnp.bfloat16, jnp.float32
    anywhere = pl.BlockSpec(memory_space=pl.ANY)
    inside = pl.BlockSpec(memory_space=vmem)
    return pl.pallas_call(
        functools.partial(kernel, n, rows, depth, part, width, cuts, LANES),
        out_shape=pltpu.VMEM((rows, model), low),
        in_specs=[anywhere, inside, anywhere, anywhere, anywhere, inside],
        out_specs=inside,
        scratch_shapes=[
            vmem((rows, model), low),
            vmem((2, 8 * rows, model), low),
            vmem((blocks, n * depth, 2 * LANES), low),
            vmem((n, cuts, part, sub), low),
            vmem((8 * rows, part), low),
            vmem((8 * rows, part), low),
            vmem((2, 4 * rows, sub), full),
            vmem((n * cuts, 4 * rows, sub), low),
            vmem((n * cuts, 4 * rows, sub), low),
            vmem((n * cuts, 2, rows, sub // 2), low),
            vmem((n * cuts, 2, rows, sub // 2), low),
            vmem((n * cuts, 2, rows, sub), low),
            vmem((n * cuts, 2, rows, sub), low),
            vmem((n * cuts, rows, sub), full),
            vmem((rows, sub // 2), full),
            dma(()),
            dma((blocks, 2)),
            dma((cuts,)),
            dma((4,)),
            dma((4,)),
            dma((2, 20)),
            dma((2, 20)),
            dma((2, blocks)),
            dma((n, blocks)),
            dma((2, n, cuts)),
            dma((n, cuts)),
            dma((blocks, 4)),
            dma((blocks, 4)),
            dma((n * cuts,)),
            dma((n * cuts,)),
            dma((n * cuts, 2)),
            dma((n * cuts, 2)),
            dma((n * cuts, 2)),
            dma((n * cuts, 2)),
        ],
        compiler_params=pltpu.CompilerParams(
            collective_id=0, has_side_effects=True, vmem_limit_bytes=56 * 2**20
        ),
    )(tokens, norm_gain.reshape(1, -1), w_gate, w_up, w_down, post_gain.reshape(1, -1))


def solution(mesh):
    n = mesh.shape["fs"]

    def body(tokens, norm_gain, w_gate, w_up, w_down, post_gain):
        args = (tokens, norm_gain, w_gate, w_up, w_down, post_gain)
        rows = tokens.shape[0]
        fits = (
            mesh.shape["rep"] == 2 and mesh.shape["tp"] == 4 and n == 4 and rows <= 128
            and w_gate.shape[1] == 6 * LANES and w_down.shape[1] == 2 * PIECE
            and rows % 64 == 0 and w_gate.shape[1] % 256 == 0 and w_down.shape[1] % PIECE == 0
        )
        return chain_body(n, *args) if fits else plain_body(*args)

    return jax.shard_map(
        body,
        mesh=mesh,
        in_specs=(
            P(("rep", "fs", "tp"), None),
            P(),
            P("fs", "tp"),
            P("fs", "tp"),
            P("tp", "fs"),
            P(),
        ),
        out_specs=P(("rep", "fs", "tp"), None),
        check_vma=False,
    )
```

```python
import functools

import jax
import jax.numpy as jnp
from jax import lax
from jax.experimental import pallas as pl
from jax.experimental.pallas import tpu as pltpu
from jax.sharding import PartitionSpec as P

EPS = 1e-06
MESH = pl.DeviceIdType.MESH
PIECE = 256
LANES = 128


def rms_scale(values, gain):
    return values * lax.rsqrt(jnp.mean(values * values, axis=-1, keepdims=True) + EPS) * gain


def plain_body(tokens, norm_gain, w_gate, w_up, w_down, post_gain):
    own_normed = rms_scale(tokens.astype(jnp.float32), norm_gain).astype(jnp.bfloat16)
    normed = lax.all_gather(own_normed, "tp", axis=0, tiled=True)
    gate = jnp.dot(
        normed, lax.all_gather(w_gate, "fs", axis=0, tiled=True), preferred_element_type=jnp.float32
    )
    up = jnp.dot(
        normed, lax.all_gather(w_up, "fs", axis=0, tiled=True), preferred_element_type=jnp.float32
    )
    hidden = (jax.nn.silu(gate) * up).astype(jnp.bfloat16)
    terms = jnp.dot(
        hidden, lax.all_gather(w_down, "fs", axis=1, tiled=True), preferred_element_type=jnp.float32
    )
    summed = lax.psum_scatter(
        terms.astype(jnp.bfloat16), "tp", scatter_dimension=0, tiled=True
    ).astype(jnp.float32)
    return rms_scale(summed, post_gain).astype(jnp.bfloat16)


def kernel(
    n, rows, depth, part, width, cuts, lanes,
    tok_ref, gain_ref, wg_ref, wu_ref, wd_ref, post_ref, out_ref,
    raw, tok, gu, dn, hid, hdel, kept, pair_out, pair_in, half_out, half_in, full_out, full_in, fin, squares,
    tok_l, gu_l, dn_l, z_s, z_r, tok_s, tok_r, gu_s, gu_r, dn_s, dn_r, hid_s, hid_r,
    pair_s, pair_r, half_s, half_r, full_s, full_r,
):
    r, k, t = lax.axis_index("rep"), lax.axis_index("fs"), lax.axis_index("tp")
    x, c = t // 2, t % 2
    t_pair, t_x, r_y = x * 2 + (1 - c), (1 - x) * 2 + c, 1 - r
    t_px = (1 - x) * 2 + (1 - c)
    partner, along_x, along_y, diag = {"tp": t_pair}, {"tp": t_x}, {"rep": r_y}, {"rep": r_y, "tp": t_x}
    left = k < n // 2
    last = jnp.where(left, 0, n - 1)
    near = jnp.where(left, 1, n - 2)
    far_near, far_last = n - 1 - near, n - 1 - last
    at_end = k == last
    in_middle = k != last
    inner, outer = {"fs": jnp.where(left, k + 1, k - 1)}, {"fs": last}
    blocks = part // lanes
    sub = width // cuts
    half = pl.multiple_of(r * part, part)
    piece = rows // 4
    own_depth = pl.ds(pl.multiple_of(k * depth, depth), depth)

    def gu_load(b, q):
        ref = (wg_ref, wu_ref)[q]
        return pltpu.make_async_copy(
            ref.at[:, pl.ds(half + b * lanes, lanes)], gu.at[b, own_depth, pl.ds(q * lanes, lanes)], gu_l.at[b]
        )

    def dn_load(j):
        return pltpu.make_async_copy(wd_ref.at[pl.ds(half, part), pl.ds(j * sub, sub)], dn.at[k, j], dn_l)

    tok_load = pltpu.make_async_copy(tok_ref, raw, tok_l)

    tok_load.start()
    for b in range(blocks):
        for q in (0, 1):
            gu_load(b, q).start()
    for j in range(cuts):
        dn_load(j).start()

    barrier = pltpu.get_barrier_semaphore()
    for where in (partner, along_x, along_y, diag, inner):
        pl.semaphore_signal(barrier, inc=1, device_id=where, device_id_type=MESH)

    @pl.when(in_middle)
    def _():
        pl.semaphore_signal(barrier, inc=1, device_id=outer, device_id_type=MESH)

    pl.semaphore_wait(barrier, 5 + jnp.where(in_middle, 1, 0))

    def remote(ref, send, recv, where, to=None):
        return pltpu.make_async_remote_copy(
            ref, ref if to is None else to, send, recv, device_id=where, device_id_type=MESH
        )

    def gu_at(s, b):
        return gu.at[b, pl.ds(pl.multiple_of(s * depth, depth), depth)]

    def gu_send(kind, b):
        return remote(
            gu_at(last if kind else k, b), gu_s.at[kind], gu_r.at[b + jnp.where(in_middle, blocks, 0)], inner
        )

    def gu_pass(b):
        remote(gu_at(last, b), gu_s.at[1], gu_r.at[b], inner).wait_recv()
        gu_send(1, b).start()

    def gu_wait(b):
        remote(gu.at[b, pl.ds(0, 2 * depth)], gu_s.at[0], gu_r.at[blocks + b], inner).wait_recv()

    def dn_send(way, s, j):
        return remote(dn.at[s, j], dn_s.at[way], dn_r.at[s, j], outer if way else inner)

    def dn_wait(s, j):
        remote(dn.at[s, j], dn_s.at[0], dn_r.at[s, j], inner).wait_recv()

    def pass_down(way, s, j):
        dn_wait(s, j)
        dn_send(way, s, j).start()

    def rows_of(p, r_at, t_at, first, count):
        base = (r_at * 4 + (t_at % 2) * 2 + t_at // 2) * rows
        return tok.at[p, pl.ds(base + first * piece, count * piece)]

    def z_send(i):
        return remote(rows_of(0, r, t, i, 1), z_s, z_r.at[i], inner, rows_of(1, r, t, i, 1))

    def z_wait(i):
        remote(rows_of(1, r, t, i, 1), z_s, z_r.at[i], inner).wait_recv()

    sends = (
        [((r, t, i, 1), along_x) for i in range(4)]
        + [((r, t, i, 1), along_y) for i in range(4)]
        + [((r, t_x, 0, 1), along_y), ((r, t_x, 1, 1), along_y), ((r_y, t, 2, 1), along_x), ((r_y, t, 3, 1), along_x)]
        + [((r_at, t_at, i, 2), partner) for r_at, t_at in ((r, t), (r, t_x), (r_y, t), (r_y, t_x)) for i in (0, 2)]
    )
    groups = (
        ((0, 1), (6, 7), (2, 3), (4, 5), (8, 9), (10, 11), (12, 13, 14, 15), (16, 17, 18, 19)),
        ((0, 4), (1, 5), (6,), (7,), (2, 3), (8, 9), (10, 11), (12, 13, 14, 15, 16, 17, 18, 19)),
    )

    def group_of(p, i):
        return [g for g, held in enumerate(groups[p]) if i in held][0]

    def go(p, *which):
        for i in which:
            at, where = sends[i]
            remote(rows_of(p, *at), tok_s.at[p], tok_r.at[p, group_of(p, i)], where).start()

    def got(p, *which):
        g = group_of(p, which[0])
        assert groups[p][g] == which
        count = sum(1 if i < 12 else 2 for i in which) * piece
        remote(tok.at[p, pl.ds(0, count)], tok_s.at[p], tok_r.at[p, g], partner).wait_recv()

    quarter = 2 * rows
    halves = 4 * rows

    def half_rows(r_at):
        return pl.ds(pl.multiple_of(r_at * halves, halves), halves)

    def hid_send(b, r_at):
        at = (half_rows(r_at), pl.ds(b * lanes, lanes))
        return remote(hdel.at[at], hid_s, hid_r.at[r_at], outer, hid.at[at])

    def hid_wait(r_at):
        remote(hid.at[half_rows(r_at)], hid_s, hid_r.at[r_at], partner).wait_recv()

    def gated(p, b, r_at):
        at = half_rows(r_at)
        both = jnp.dot(tok[p, at, :], gu[b], preferred_element_type=jnp.float32)
        gate, up = both[:, :lanes], both[:, lanes:]
        value = (gate / (1.0 + jnp.exp(-gate)) * up).astype(jnp.bfloat16)
        (hdel if p else hid)[at, pl.ds(b * lanes, lanes)] = value

    def passed_block(b):
        @pl.loop(0, 2)
        def _(i):
            r_at = (r_y + i) % 2
            gated(1, b, r_at)
            hid_send(b, r_at).start()

    def own_block(b, r_at):
        gated(0, b, r_at)

    def send_own_gu():
        for b in range(blocks):
            pltpu.make_async_copy(gu.at[b, own_depth], gu.at[b, own_depth], gu_l.at[b]).wait()
            gu_send(0, b).start()

    def send_own_dn(way):
        pltpu.make_async_copy(dn.at[k], dn.at[k], dn_l).wait()
        for j in range(cuts):
            dn_send(way, k, j).start()

    @pl.when(in_middle)
    def _():
        send_own_gu()
        send_own_dn(1)

    tok_load.wait()
    tile = 32
    first = (r * 4 + c * 2 + x) * rows

    @pl.loop(0, rows // tile)
    def _(i):
        at = pl.ds(pl.multiple_of(i * tile, tile), tile)
        to = pl.ds(pl.multiple_of(first + i * tile, tile), tile)
        tok[0, to, :] = rms_scale(raw[at, :].astype(jnp.float32), gain_ref[...]).astype(jnp.bfloat16)

    @pl.when(at_end)
    def _():
        for i in range(4):
            z_send(i).start()
        send_own_gu()
        send_own_dn(0)

    @pl.when(in_middle)
    def _():
        go(0, 0, 1, 6, 7, 12, 13)
        z_wait(0)
        go(1, 0, 4)
        got(0, 0, 1)
        go(0, 14)
        got(0, 6, 7)
        go(0, 17)
        z_wait(1)
        go(1, 1, 5, 12)
        got(1, 0, 4)
        z_wait(2)
        go(1, 2, 6)
        got(1, 1, 5)
        go(1, 14, 16)
        z_wait(3)
        go(1, 13, 3, 7, 8, 9)
        got(1, 6)
        go(1, 10)
        got(1, 7)
        go(1, 17, 11)
        got(1, 2, 3)
        go(1, 15)
        gu_pass(0)
        go(0, 2, 4)
        gu_pass(1)
        got(1, 8, 9)
        go(1, 18)
        got(1, 10, 11)
        go(1, 19)
        go(0, 3, 5, 8, 10)
        got(1, 12, 13, 14, 15, 16, 17, 18, 19)
        gu_wait(0)
        passed_block(0)
        go(0, 9, 11)
        got(0, 2, 3)
        go(0, 15)
        got(0, 4, 5)
        go(0, 16)
        gu_pass(2)
        gu_wait(1)
        passed_block(1)
        got(0, 12, 13, 14, 15)
        own_block(0, r)
        own_block(1, r)
        dn_wait(last, 0)
        got(0, 8, 9)
        go(0, 18)
        got(0, 10, 11)
        go(0, 19)
        gu_wait(2)
        for j in range(cuts):
            dn_send(0, k, j).start()
        dn_send(0, last, 0).start()
        passed_block(2)
        own_block(2, r)
        pass_down(0, last, 1)
        got(0, 16, 17, 18, 19)
        own_block(0, r_y)
        own_block(1, r_y)
        own_block(2, r_y)
        pass_down(1, far_near, 0)

    chunks = n * cuts
    mid = sub // 2
    here, there = 0, 1

    def pair_copy(p, side):
        return remote(pair_out.at[p, side], pair_s, pair_r.at[p, side], partner, pair_in.at[p, side])

    def half_copy(p, way):
        return remote(
            half_out.at[p, way], half_s, half_r.at[p], along_y if way else along_x, half_in.at[p, way]
        )

    def full_copy(p, way):
        return remote(
            full_out.at[p, way], full_s, full_r.at[p], along_y if way else along_x, full_in.at[p, way]
        )

    def source(i):
        near_or_last = jnp.where(i == 0, k, near + last - k)
        return jnp.where(i < 2, near_or_last, jnp.where(i == 2, far_near, far_last))

    def place(at):
        return source(at // cuts) * cuts + at % cuts

    def product(at, side):
        s, j, p = source(at // cuts), at % cuts, place(at)
        r_at = r_y if side == there else r
        first = pl.multiple_of(r_at * halves, halves)

        def part_of(core):
            rows_at = pl.ds(pl.multiple_of(first + core * quarter, quarter), quarter)
            return jnp.dot(hid[rows_at, :], dn[s, j], preferred_element_type=jnp.float32)

        pair_out[p, side] = part_of(1 - c).astype(jnp.bfloat16)
        pair_copy(p, side).start()
        kept[p, side] = part_of(c)

    def of(m):
        return pl.ds(pl.multiple_of(m * rows, rows), rows)

    def summed(p, side, x_at):
        return kept[p, side, of(x_at), :] + pair_in[p, side, of(x_at), :].astype(jnp.float32)

    def finish_there(at):
        p = place(at)
        pair_copy(p, there).wait_recv()
        across = summed(p, there, 1 - x).astype(jnp.bfloat16)
        half_out[p, 0] = across[:, :mid]
        half_out[p, 1] = across[:, mid:]
        half_copy(p, 0).start()
        half_copy(p, 1).start()
        kept[p, there, of(x), :] = summed(p, there, x)

    def finish_here(at):
        p = place(at)
        pair_copy(p, here).wait_recv()
        kept[p, here, of(1 - x), :] = summed(p, here, 1 - x)
        fin[p] = summed(p, here, x)

    def finish_half(at):
        p = place(at)
        remote(half_in.at[p], half_s, half_r.at[p], partner).wait_recv()
        to_x, to_y = (here, of(1 - x)), (there, of(x))
        full_out[p, 0, :, :mid] = kept[(p, *to_x, slice(0, mid))].astype(jnp.bfloat16)
        full_out[p, 0, :, mid:] = (kept[(p, *to_x, slice(mid, sub))] + half_in[p, 1].astype(jnp.float32)).astype(jnp.bfloat16)
        full_copy(p, 0).start()
        full_out[p, 1, :, mid:] = kept[(p, *to_y, slice(mid, sub))].astype(jnp.bfloat16)
        full_out[p, 1, :, :mid] = (kept[(p, *to_y, slice(0, mid))] + half_in[p, 0].astype(jnp.float32)).astype(jnp.bfloat16)
        full_copy(p, 1).start()

    early = 2 * cuts

    @pl.when(at_end)
    def _():
        for j in range(cuts):
            dn_wait(near, j)
        hid_wait(r_y)

    @pl.loop(0, early)
    def _(at):
        product(at, there)

        @pl.when(at > 0)
        def _():
            finish_there(at - 1)

    @pl.when(at_end)
    def _():
        hid_wait(r)

    @pl.when(in_middle)
    def _():
        pass_down(1, far_near, 1)

    @pl.loop(0, early)
    def _(at):
        product(at, here)

        @pl.when(at == 0)
        def _():
            finish_there(early - 1)

        @pl.when(at > 0)
        def _():
            finish_here(at - 1)
            finish_half(at - 1)

        @pl.when(in_middle & (at == 2))
        def _():
            pass_down(1, far_last, 0)

    @pl.loop(early, chunks)
    def _(at):
        @pl.when(at_end)
        def _():
            dn_wait(source(at // cuts), at % cuts)

        @pl.when(in_middle & (at == early))
        def _():
            pass_down(1, far_last, 1)

        product(at, there)
        product(at, here)

        @pl.when(at == early)
        def _():
            finish_here(at - 1)
            finish_half(at - 1)

        finish_there(at)
        finish_here(at)

        @pl.when(at > early)
        def _():
            finish_half(at - 1)

    finish_half(chunks - 1)

    remote(gu.at[:, pl.ds(0, depth)], gu_s.at[0], gu_r.at[0], inner).wait_send()

    @pl.when(at_end)
    def _():
        remote(tok.at[0, pl.ds(0, rows)], z_s, z_r.at[0], inner).wait_send()
        remote(dn.at[0], dn_s.at[0], dn_r.at[0, 0], inner).wait_send()

    @pl.when(in_middle)
    def _():
        for p in (0, 1):
            total = sum(1 if i < 12 else 2 for i in range(len(sends))) * piece
            remote(tok.at[p, pl.ds(0, total)], tok_s.at[p], tok_r.at[p, 0], partner).wait_send()
        remote(gu.at[:, pl.ds(0, depth)], gu_s.at[1], gu_r.at[0], inner).wait_send()
        remote(hdel, hid_s, hid_r.at[0], outer).wait_send()
        remote(dn.at[pl.ds(0, 2)], dn_s.at[0], dn_r.at[0, 0], inner).wait_send()
        remote(dn.at[pl.ds(0, 3)], dn_s.at[1], dn_r.at[0, 0], outer).wait_send()

    remote(pair_out, pair_s, pair_r.at[0, 0], partner).wait_send()
    remote(half_out, half_s, half_r.at[0], along_x).wait_send()

    squares[...] = jnp.zeros_like(squares)

    @pl.loop(0, chunks)
    def _(at):
        p = place(at)
        remote(full_in.at[p], full_s, full_r.at[p], along_x).wait_recv()
        total = fin[p] + full_in[p, 0].astype(jnp.float32) + full_in[p, 1].astype(jnp.float32)
        fin[p] = total
        squares[...] += total[:, :mid] * total[:, :mid] + total[:, mid:] * total[:, mid:]

    scale = lax.rsqrt(jnp.sum(squares[...], axis=-1, keepdims=True) / (n * width) + EPS)
    for p in range(chunks):
        cols = pl.ds(p * sub, sub)
        out_ref[:, cols] = (fin[p] * scale * post_ref[:, cols]).astype(out_ref.dtype)

    remote(full_out, full_s, full_r.at[0], along_x).wait_send()


def chain_body(n, tokens, norm_gain, w_gate, w_up, w_down, post_gain):
    rows, model = tokens.shape
    depth, block = w_gate.shape
    width = w_down.shape[1]
    part = block // 2
    cuts = width // PIECE
    sub = width // cuts
    blocks = part // LANES
    chunks = n * cuts
    vmem, dma = pltpu.VMEM, pltpu.SemaphoreType.DMA
    low, full = jnp.bfloat16, jnp.float32
    anywhere = pl.BlockSpec(memory_space=pl.ANY)
    inside = pl.BlockSpec(memory_space=vmem)
    return pl.pallas_call(
        functools.partial(kernel, n, rows, depth, part, width, cuts, LANES),
        out_shape=pltpu.VMEM((rows, model), low),
        in_specs=[anywhere, inside, anywhere, anywhere, anywhere, inside],
        out_specs=inside,
        scratch_shapes=[
            vmem((rows, model), low),
            vmem((2, 8 * rows, model), low),
            vmem((blocks, n * depth, 2 * LANES), low),
            vmem((n, cuts, part, sub), low),
            vmem((8 * rows, part), low),
            vmem((8 * rows, part), low),
            vmem((chunks, 2, 2 * rows, sub), full),
            vmem((chunks, 2, 2 * rows, sub), low),
            vmem((chunks, 2, 2 * rows, sub), low),
            vmem((chunks, 2, rows, sub // 2), low),
            vmem((chunks, 2, rows, sub // 2), low),
            vmem((chunks, 2, rows, sub), low),
            vmem((chunks, 2, rows, sub), low),
            vmem((chunks, rows, sub), full),
            vmem((rows, sub // 2), full),
            dma(()),
            dma((blocks,)),
            dma(()),
            dma(()),
            dma((4,)),
            dma((2,)),
            dma((2, 8)),
            dma((2,)),
            dma((2 * blocks,)),
            dma((2,)),
            dma((n, cuts)),
            dma(()),
            dma((2,)),
            dma(()),
            dma((chunks, 2)),
            dma(()),
            dma((chunks,)),
            dma(()),
            dma((chunks,)),
        ],
        compiler_params=pltpu.CompilerParams(
            collective_id=0, has_side_effects=True, vmem_limit_bytes=56 * 2**20
        ),
    )(tokens, norm_gain.reshape(1, -1), w_gate, w_up, w_down, post_gain.reshape(1, -1))


def solution(mesh):
    n = mesh.shape["fs"]

    def body(tokens, norm_gain, w_gate, w_up, w_down, post_gain):
        args = (tokens, norm_gain, w_gate, w_up, w_down, post_gain)
        rows = tokens.shape[0]
        fits = (
            mesh.shape["rep"] == 2 and mesh.shape["tp"] == 4 and n == 4 and rows <= 128 and rows % 128 == 0
            and w_gate.shape[1] == 6 * LANES and w_down.shape[1] == 2 * PIECE
        )
        return chain_body(n, *args) if fits else plain_body(*args)

    return jax.shard_map(
        body,
        mesh=mesh,
        in_specs=(
            P(("rep", "fs", "tp"), None),
            P(),
            P("fs", "tp"),
            P("fs", "tp"),
            P("tp", "fs"),
            P(),
        ),
        out_specs=P(("rep", "fs", "tp"), None),
        check_vma=False,
    )
```

```python
import functools

import jax
import jax.numpy as jnp
from jax import lax
from jax.experimental import pallas as pl
from jax.experimental.pallas import tpu as pltpu
from jax.sharding import PartitionSpec as P

EPS = 1e-06
MESH = pl.DeviceIdType.MESH
PIECE = 256
LANES = 128


def rms_scale(values, gain):
    return values * lax.rsqrt(jnp.mean(values * values, axis=-1, keepdims=True) + EPS) * gain


def plain_body(tokens, norm_gain, w_gate, w_up, w_down, post_gain):
    own_normed = rms_scale(tokens.astype(jnp.float32), norm_gain).astype(jnp.bfloat16)
    normed = lax.all_gather(own_normed, "tp", axis=0, tiled=True)
    gate = jnp.dot(
        normed, lax.all_gather(w_gate, "fs", axis=0, tiled=True), preferred_element_type=jnp.float32
    )
    up = jnp.dot(
        normed, lax.all_gather(w_up, "fs", axis=0, tiled=True), preferred_element_type=jnp.float32
    )
    hidden = (jax.nn.silu(gate) * up).astype(jnp.bfloat16)
    terms = jnp.dot(
        hidden, lax.all_gather(w_down, "fs", axis=1, tiled=True), preferred_element_type=jnp.float32
    )
    summed = lax.psum_scatter(
        terms.astype(jnp.bfloat16), "tp", scatter_dimension=0, tiled=True
    ).astype(jnp.float32)
    return rms_scale(summed, post_gain).astype(jnp.bfloat16)


def kernel(
    n, rows, depth, part, width, cuts, lanes,
    tok_ref, gain_ref, wg_ref, wu_ref, wd_ref, post_ref, out_ref,
    raw, tok, gu, dn, hid, kept, pair_out, pair_in, half_out, half_in, full_out, full_in, fin, res_out, res_in, squares,
    tok_l, gu_l, dn_l, z_s, z_r, tok_s, tok_r, gu_s, gu_r, dn_s, dn_r, hid_s, hid_r,
    pair_s, pair_r, half_s, half_r, full_s, full_r, res_s, res_r,
):
    r, k, t = lax.axis_index("rep"), lax.axis_index("fs"), lax.axis_index("tp")
    x, c = t // 2, t % 2
    t_pair, t_x, r_y = x * 2 + (1 - c), (1 - x) * 2 + c, 1 - r
    t_px = (1 - x) * 2 + (1 - c)
    partner, along_x, along_y, diag = {"tp": t_pair}, {"tp": t_x}, {"rep": r_y}, {"rep": r_y, "tp": t_x}
    left = k < n // 2
    last = jnp.where(left, 0, n - 1)
    near = jnp.where(left, 1, n - 2)
    far_near, far_last = n - 1 - near, n - 1 - last
    at_end = k == last
    in_middle = k != last
    inner, outer = {"fs": jnp.where(left, k + 1, k - 1)}, {"fs": last}
    blocks = part // lanes
    sub = width // cuts
    half = pl.multiple_of(r * part, part)
    piece = rows // 4
    own_depth = pl.ds(pl.multiple_of(k * depth, depth), depth)

    def gu_load(b, q):
        ref = (wg_ref, wu_ref)[q]
        return pltpu.make_async_copy(
            ref.at[:, pl.ds(half + b * lanes, lanes)], gu.at[b, own_depth, pl.ds(q * lanes, lanes)], gu_l.at[b]
        )

    def dn_load(j):
        return pltpu.make_async_copy(wd_ref.at[pl.ds(half, part), pl.ds(j * sub, sub)], dn.at[k * cuts + j], dn_l)

    tok_load = pltpu.make_async_copy(tok_ref, raw, tok_l)

    tok_load.start()
    for b in range(blocks):
        for q in (0, 1):
            gu_load(b, q).start()
    for j in range(cuts):
        dn_load(j).start()

    barrier = pltpu.get_barrier_semaphore()
    for where in (partner, along_x, along_y, diag, inner):
        pl.semaphore_signal(barrier, inc=1, device_id=where, device_id_type=MESH)

    @pl.when(in_middle)
    def _():
        pl.semaphore_signal(barrier, inc=1, device_id=outer, device_id_type=MESH)

    pl.semaphore_wait(barrier, 5 + jnp.where(in_middle, 1, 0))

    def remote(ref, send, recv, where, to=None):
        return pltpu.make_async_remote_copy(
            ref, ref if to is None else to, send, recv, device_id=where, device_id_type=MESH
        )

    def gu_at(s, b):
        return gu.at[b, pl.ds(pl.multiple_of(s * depth, depth), depth)]

    def gu_send(kind, b):
        return remote(
            gu_at(last if kind else k, b), gu_s.at[kind], gu_r.at[b + jnp.where(in_middle, blocks, 0)], inner
        )

    def gu_pass(b):
        remote(gu_at(last, b), gu_s.at[1], gu_r.at[b], inner).wait_recv()
        gu_send(1, b).start()

    def gu_wait(b):
        remote(gu.at[b, pl.ds(0, 2 * depth)], gu_s.at[0], gu_r.at[blocks + b], inner).wait_recv()

    def dn_send(way, s, j):
        at = s * cuts + j
        return remote(dn.at[at], dn_s.at[way], dn_r.at[at], outer if way else inner)

    def dn_wait(s, j):
        at = s * cuts + j
        remote(dn.at[at], dn_s.at[0], dn_r.at[at], inner).wait_recv()

    def pass_down(way, s, j):
        dn_wait(s, j)
        dn_send(way, s, j).start()

    def rows_of(p, r_at, t_at, first, count, core):
        other = (t_at % 2 + core) % 2
        base = (r_at * 4 + other * 2 + t_at // 2) * rows
        return tok.at[p, pl.ds(base + first * piece, count * piece)]

    def z_send(i):
        return remote(rows_of(0, r, t, i, 1, c), z_s, z_r.at[i], inner, rows_of(1, r, t, i, 1, c))

    def z_wait(i):
        remote(rows_of(1, r, t, i, 1, c), z_s, z_r.at[i], inner).wait_recv()

    sends = (
        [((r, t, i, 1), along_x) for i in range(4)]
        + [((r, t, i, 1), along_y) for i in range(4)]
        + [((r, t_x, 0, 1), along_y), ((r, t_x, 1, 1), along_y), ((r_y, t, 2, 1), along_x), ((r_y, t, 3, 1), along_x)]
        + [((r_at, t_at, i, 2), partner) for r_at, t_at in ((r, t), (r, t_x), (r_y, t), (r_y, t_x)) for i in (0, 2)]
    )
    groups = (
        ((0, 1), (6, 7), (2, 3), (4, 5), (8, 9), (10, 11), (12, 13, 14, 15), (16, 17, 18, 19)),
        ((0, 4), (1, 5), (6,), (7,), (2, 3), (8, 9), (10, 11), (12, 13, 14, 15, 16, 17, 18, 19)),
    )

    def group_of(p, i):
        return [g for g, held in enumerate(groups[p]) if i in held][0]

    def go(p, *which):
        for i in which:
            at, where = sends[i]
            to = rows_of(p, *at, 1 - c if i >= 12 else c)
            remote(rows_of(p, *at, c), tok_s.at[p], tok_r.at[p, group_of(p, i)], where, to).start()

    def got(p, *which):
        g = group_of(p, which[0])
        assert groups[p][g] == which
        count = sum(1 if i < 12 else 2 for i in which) * piece
        remote(tok.at[p, pl.ds(0, count)], tok_s.at[p], tok_r.at[p, g], partner).wait_recv()

    quarter = 2 * rows
    halves = 4 * rows

    def half_rows(r_at):
        return pl.ds(pl.multiple_of(r_at * halves, halves), halves)

    def hid_at(p, b, r_at):
        return hid.at[p, half_rows(r_at), pl.ds(pl.multiple_of(b * lanes, lanes), lanes)]

    def hid_send(b, r_at):
        return remote(hid_at(1, b, r_at), hid_s, hid_r.at[r_at], outer, hid_at(0, b, r_at))

    def hid_wait(r_at):
        remote(hid.at[0, half_rows(r_at)], hid_s, hid_r.at[r_at], partner).wait_recv()

    def gated(p, b, r_at):
        both = jnp.dot(tok[p, half_rows(r_at), :], gu[b], preferred_element_type=jnp.float32)
        gate, up = both[:, :lanes], both[:, lanes:]
        hid_at(p, b, r_at)[...] = (gate / (1.0 + jnp.exp(-gate)) * up).astype(jnp.bfloat16)

    def send_own_gu():
        for b in range(blocks):
            pltpu.make_async_copy(gu.at[b, own_depth], gu.at[b, own_depth], gu_l.at[b]).wait()
            gu_send(0, b).start()

    def send_own_dn(way):
        own = dn.at[pl.ds(k * cuts, cuts)]
        pltpu.make_async_copy(own, own, dn_l).wait()
        for j in range(cuts):
            dn_send(way, k, j).start()

    @pl.when(in_middle)
    def _():
        send_own_gu()
        send_own_dn(1)

    tok_load.wait()
    tile = 32
    first = (r * 4 + x) * rows

    @pl.loop(0, rows // tile)
    def _(i):
        at = pl.ds(pl.multiple_of(i * tile, tile), tile)
        to = pl.ds(pl.multiple_of(first + i * tile, tile), tile)
        tok[0, to, :] = rms_scale(raw[at, :].astype(jnp.float32), gain_ref[...]).astype(jnp.bfloat16)

    @pl.when(at_end)
    def _():
        for i in range(4):
            z_send(i).start()
        send_own_gu()
        send_own_dn(0)

    @pl.when(in_middle)
    def _():
        @pl.loop(0, 12)
        def _(at_step):
            def step(at):
                return pl.when(at_step == at)

            @step(0)
            def _():
                go(0, 0, 1, 6, 7, 12, 13)
                z_wait(0)
                go(1, 0, 4)
                got(0, 0, 1)
                go(0, 14)
                got(0, 6, 7)
                go(0, 17)
                z_wait(1)
                go(1, 1, 5, 12)
                got(1, 0, 4)
                z_wait(2)
                go(1, 2, 6)
                got(1, 1, 5)
                go(1, 14, 16)
                z_wait(3)
                go(1, 13, 3, 7, 8, 9)
                got(1, 6)
                go(1, 10)
                got(1, 7)
                go(1, 17, 11)
                got(1, 2, 3)
                go(1, 15)
                gu_pass(0)
                go(0, 2, 4)
                gu_pass(1)
                got(1, 8, 9)
                go(1, 18)
                got(1, 10, 11)
                go(1, 19)
                go(0, 3, 5, 8, 10)
                got(1, 12, 13, 14, 15, 16, 17, 18, 19)
                gu_wait(0)

            @step(2)
            def _():
                go(0, 9, 11)
                got(0, 2, 3)
                go(0, 15)
                got(0, 4, 5)
                go(0, 16)
                gu_pass(2)
                gu_wait(1)

            @step(4)
            def _():
                got(0, 12, 13, 14, 15)

            @step(6)
            def _():
                dn_wait(last, 0)
                got(0, 8, 9)
                go(0, 18)
                got(0, 10, 11)
                go(0, 19)
                gu_wait(2)
                for j in range(cuts):
                    dn_send(0, k, j).start()
                dn_send(0, last, 0).start()

            @step(9)
            def _():
                pass_down(0, last, 1)
                got(0, 16, 17, 18, 19)

            passed = (at_step < 4) | (at_step == 6) | (at_step == 7)
            b = jnp.where(at_step < 4, at_step // 2, jnp.where(at_step < 6, at_step - 4, jnp.where(at_step < 9, 2, at_step - 9)))
            r_at = jnp.where(passed, (r_y + at_step % 2) % 2, jnp.where(at_step < 9, r, r_y))
            gated(jnp.where(passed, 1, 0), b, r_at)

            @pl.when(passed)
            def _():
                hid_send(b, r_at).start()

        pass_down(1, far_near, 0)

    chunks = n * cuts
    mid = sub // 2
    here, there = 0, 1

    def pair_copy(p, side):
        return remote(pair_out.at[p, side], pair_s, pair_r.at[p, side], partner, pair_in.at[p, side])

    def half_copy(p, way):
        return remote(
            half_out.at[p, way], half_s, half_r.at[p], along_y if way else along_x, half_in.at[p, way]
        )

    def full_copy(p, way):
        return remote(
            full_out.at[p, way], full_s, full_r.at[p], along_y if way else along_x, full_in.at[p, way]
        )

    def source(i):
        near_or_last = jnp.where(i == 0, k, near + last - k)
        return jnp.where(i < 2, near_or_last, jnp.where(i == 2, far_near, far_last))

    def place(at):
        return jnp.where(at < chunks, source(at // cuts) * cuts + at % cuts, chunks)

    def product(at, side):
        p = place(at)
        held = jnp.where(at < chunks, p, far_last * cuts + cuts - 1)
        rows_at = half_rows(r_y if side == there else r)
        both = jnp.dot(hid[jnp.where(at < chunks, 0, 1), rows_at, :], dn[held], preferred_element_type=jnp.float32)
        pair_out[p, side] = both[quarter:].astype(jnp.bfloat16)
        pair_copy(p, side).start()
        kept[p, side] = both[:quarter]

    def of(m):
        return pl.ds(pl.multiple_of(m * rows, rows), rows)

    def summed(p, side, x_at):
        return kept[p, side, of(x_at), :] + pair_in[p, side, of(x_at), :].astype(jnp.float32)

    def finish_there(at):
        p = place(at)
        pair_copy(p, there).wait_recv()
        across = summed(p, there, 1 - x).astype(jnp.bfloat16)
        half_out[p, 0] = across[:, :mid]
        half_out[p, 1] = across[:, mid:]
        half_copy(p, 0).start()
        half_copy(p, 1).start()
        kept[p, there, of(x), :] = summed(p, there, x)

    def finish_here(at):
        p = place(at)
        pair_copy(p, here).wait_recv()
        kept[p, here, of(1 - x), :] = summed(p, here, 1 - x)
        fin[p] = summed(p, here, x)

    def finish_half(at):
        p = place(at)
        remote(half_in.at[p], half_s, half_r.at[p], partner).wait_recv()
        to_x, to_y = (here, of(1 - x)), (there, of(x))
        full_out[p, 0, :, :mid] = kept[(p, *to_x, slice(0, mid))].astype(jnp.bfloat16)
        full_out[p, 0, :, mid:] = (kept[(p, *to_x, slice(mid, sub))] + half_in[p, 1].astype(jnp.float32)).astype(jnp.bfloat16)
        full_copy(p, 0).start()
        full_out[p, 1, :, mid:] = kept[(p, *to_y, slice(mid, sub))].astype(jnp.bfloat16)
        full_out[p, 1, :, :mid] = (kept[(p, *to_y, slice(0, mid))] + half_in[p, 0].astype(jnp.float32)).astype(jnp.bfloat16)
        full_copy(p, 1).start()

    early = 2 * cuts

    @pl.when(at_end)
    def _():
        for j in range(cuts):
            dn_wait(near, j)
        hid_wait(r_y)

    @pl.loop(0, early)
    def _(at):
        product(at, there)

        @pl.when(at > 0)
        def _():
            finish_there(at - 1)

    @pl.when(at_end)
    def _():
        hid_wait(r)

    @pl.when(in_middle)
    def _():
        pass_down(1, far_near, 1)

    @pl.loop(0, early)
    def _(at):
        product(at, here)

        @pl.when(at == 0)
        def _():
            finish_there(early - 1)

        @pl.when(at > 0)
        def _():
            finish_here(at - 1)
            finish_half(at - 1)

        @pl.when(in_middle & (at == 2))
        def _():
            pass_down(1, far_last, 0)

    def order(i):
        return jnp.where(in_middle & (i >= 2), jnp.where(i == 2, chunks, early + i - 1), early + i)

    @pl.loop(0, chunks - early + 1)
    def _(i):
        at = order(i)

        @pl.when(at_end & (i < 3))
        def _():
            dn_wait(source(at // cuts), at % cuts)

        @pl.when(in_middle & (i == 2))
        def _():
            dn_wait(far_last, cuts - 1)

        @pl.when(in_middle | (i < 3))
        def _():
            product(at, there)
            product(at, here)

        @pl.when(i == 0)
        def _():
            finish_here(early - 1)
            finish_half(early - 1)

        @pl.when(in_middle | (i < 3))
        def _():
            finish_there(at)
            finish_here(at)

        @pl.when((i > 0) & (in_middle | (i < 4)))
        def _():
            finish_half(order(i - 1))

    @pl.when(in_middle)
    def _():
        finish_half(chunks - 1)

    remote(gu.at[:, pl.ds(0, depth)], gu_s.at[0], gu_r.at[0], inner).wait_send()

    @pl.when(at_end)
    def _():
        remote(tok.at[0, pl.ds(0, rows)], z_s, z_r.at[0], inner).wait_send()
        remote(dn.at[pl.ds(0, cuts)], dn_s.at[0], dn_r.at[0], inner).wait_send()
        remote(pair_out.at[pl.ds(0, chunks - 1)], pair_s, pair_r.at[0, 0], partner).wait_send()
        remote(half_out.at[pl.ds(0, chunks - 1)], half_s, half_r.at[0], along_x).wait_send()

    @pl.when(in_middle)
    def _():
        for p in (0, 1):
            total = sum(1 if i < 12 else 2 for i in range(len(sends))) * piece
            remote(tok.at[p, pl.ds(0, total)], tok_s.at[p], tok_r.at[p, 0], partner).wait_send()
        remote(gu.at[:, pl.ds(0, depth)], gu_s.at[1], gu_r.at[0], inner).wait_send()
        remote(hid.at[1], hid_s, hid_r.at[0], outer).wait_send()
        remote(dn.at[pl.ds(0, 2 * cuts)], dn_s.at[0], dn_r.at[0], inner).wait_send()
        remote(dn.at[pl.ds(0, 3 * cuts - 1)], dn_s.at[1], dn_r.at[0], outer).wait_send()
        remote(pair_out, pair_s, pair_r.at[0, 0], partner).wait_send()
        remote(half_out, half_s, half_r.at[0], along_x).wait_send()

    squares[...] = jnp.zeros_like(squares)

    result = remote(res_out, res_s, res_r, outer, res_in)

    def collect(at):
        p = place(at)
        remote(full_in.at[p], full_s, full_r.at[p], along_x).wait_recv()
        return fin[p] + full_in[p, 0].astype(jnp.float32) + full_in[p, 1].astype(jnp.float32)

    def settle(at, total):
        fin[place(at)] = total
        squares[...] += total[:, :mid] * total[:, :mid] + total[:, mid:] * total[:, mid:]

    @pl.loop(0, chunks)
    def _(at):
        @pl.when(in_middle & (at == chunks - 2))
        def _():
            res_out[...] = collect(chunks).astype(jnp.bfloat16)
            result.start()

        @pl.when(in_middle | (at < chunks - 1))
        def _():
            settle(at, collect(at))

    @pl.when(at_end)
    def _():
        result.wait_recv()
        settle(chunks - 1, res_in[...].astype(jnp.float32))

    scale = lax.rsqrt(jnp.sum(squares[...], axis=-1, keepdims=True) / (n * width) + EPS)
    for p in range(chunks):
        cols = pl.ds(p * sub, sub)
        out_ref[:, cols] = (fin[p] * scale * post_ref[:, cols]).astype(out_ref.dtype)

    @pl.when(at_end)
    def _():
        remote(full_out.at[pl.ds(0, chunks - 1)], full_s, full_r.at[0], along_x).wait_send()

    @pl.when(in_middle)
    def _():
        remote(full_out, full_s, full_r.at[0], along_x).wait_send()
        result.wait_send()


def chain_body(n, tokens, norm_gain, w_gate, w_up, w_down, post_gain):
    rows, model = tokens.shape
    depth, block = w_gate.shape
    width = w_down.shape[1]
    part = block // 2
    cuts = width // PIECE
    sub = width // cuts
    blocks = part // LANES
    chunks = n * cuts
    vmem, dma = pltpu.VMEM, pltpu.SemaphoreType.DMA
    low, full = jnp.bfloat16, jnp.float32
    anywhere = pl.BlockSpec(memory_space=pl.ANY)
    inside = pl.BlockSpec(memory_space=vmem)
    return pl.pallas_call(
        functools.partial(kernel, n, rows, depth, part, width, cuts, LANES),
        out_shape=pltpu.VMEM((rows, model), low),
        in_specs=[anywhere, inside, anywhere, anywhere, anywhere, inside],
        out_specs=inside,
        scratch_shapes=[
            vmem((rows, model), low),
            vmem((2, 8 * rows, model), low),
            vmem((blocks, n * depth, 2 * LANES), low),
            vmem((chunks, part, sub), low),
            vmem((2, 8 * rows, part), low),
            vmem((chunks + 1, 2, 2 * rows, sub), full),
            vmem((chunks + 1, 2, 2 * rows, sub), low),
            vmem((chunks + 1, 2, 2 * rows, sub), low),
            vmem((chunks + 1, 2, rows, sub // 2), low),
            vmem((chunks + 1, 2, rows, sub // 2), low),
            vmem((chunks + 1, 2, rows, sub), low),
            vmem((chunks + 1, 2, rows, sub), low),
            vmem((chunks + 1, rows, sub), full),
            vmem((rows, sub), low),
            vmem((rows, sub), low),
            vmem((rows, sub // 2), full),
            dma(()),
            dma((blocks,)),
            dma(()),
            dma(()),
            dma((4,)),
            dma((2,)),
            dma((2, 8)),
            dma((2,)),
            dma((2 * blocks,)),
            dma((2,)),
            dma((chunks,)),
            dma(()),
            dma((2,)),
            dma(()),
            dma((chunks + 1, 2)),
            dma(()),
            dma((chunks + 1,)),
            dma(()),
            dma((chunks + 1,)),
            dma(()),
            dma(()),
        ],
        compiler_params=pltpu.CompilerParams(
            collective_id=0, has_side_effects=True, vmem_limit_bytes=56 * 2**20
        ),
    )(tokens, norm_gain.reshape(1, -1), w_gate, w_up, w_down, post_gain.reshape(1, -1))


def solution(mesh):
    n = mesh.shape["fs"]

    def body(tokens, norm_gain, w_gate, w_up, w_down, post_gain):
        args = (tokens, norm_gain, w_gate, w_up, w_down, post_gain)
        rows = tokens.shape[0]
        fits = (
            mesh.shape["rep"] == 2 and mesh.shape["tp"] == 4 and n == 4 and rows <= 128 and rows % 128 == 0
            and w_gate.shape[1] == 6 * LANES and w_down.shape[1] == 2 * PIECE
        )
        return chain_body(n, *args) if fits else plain_body(*args)

    return jax.shard_map(
        body,
        mesh=mesh,
        in_specs=(
            P(("rep", "fs", "tp"), None),
            P(),
            P("fs", "tp"),
            P("fs", "tp"),
            P("tp", "fs"),
            P(),
        ),
        out_specs=P(("rep", "fs", "tp"), None),
        check_vma=False,
    )
```

```python
import functools

import jax
import jax.numpy as jnp
from jax import lax
from jax.experimental import pallas as pl
from jax.experimental.pallas import tpu as pltpu
from jax.sharding import PartitionSpec as P

EPS = 1e-06
MESH = pl.DeviceIdType.MESH
PIECE = 256
LANES = 128


def rms_scale(values, gain):
    return values * lax.rsqrt(jnp.mean(values * values, axis=-1, keepdims=True) + EPS) * gain


def plain_body(tokens, norm_gain, w_gate, w_up, w_down, post_gain):
    own_normed = rms_scale(tokens.astype(jnp.float32), norm_gain).astype(jnp.bfloat16)
    normed = lax.all_gather(own_normed, "tp", axis=0, tiled=True)
    gate = jnp.dot(
        normed, lax.all_gather(w_gate, "fs", axis=0, tiled=True), preferred_element_type=jnp.float32
    )
    up = jnp.dot(
        normed, lax.all_gather(w_up, "fs", axis=0, tiled=True), preferred_element_type=jnp.float32
    )
    hidden = (jax.nn.silu(gate) * up).astype(jnp.bfloat16)
    terms = jnp.dot(
        hidden, lax.all_gather(w_down, "fs", axis=1, tiled=True), preferred_element_type=jnp.float32
    )
    summed = lax.psum_scatter(
        terms.astype(jnp.bfloat16), "tp", scatter_dimension=0, tiled=True
    ).astype(jnp.float32)
    return rms_scale(summed, post_gain).astype(jnp.bfloat16)


def kernel(
    n, rows, depth, part, width, cuts, lanes,
    tok_ref, gain_ref, wg_ref, wu_ref, wd_ref, post_ref, out_ref,
    raw, tok, gu, dn, hid, kept, pair_out, pair_in, half_out, half_in, full_out, full_in, fin, res_out, res_in, squares,
    tok_l, gu_l, dn_l, z_s, z_r, tok_s, tok_r, gu_s, gu_r, dn_s, dn_r, hid_s, hid_r,
    pair_s, pair_r, half_s, half_r, full_s, full_r, res_s, res_r,
):
    r, k, t = lax.axis_index("rep"), lax.axis_index("fs"), lax.axis_index("tp")
    x, c = t // 2, t % 2
    t_pair, t_x, r_y = x * 2 + (1 - c), (1 - x) * 2 + c, 1 - r
    t_px = (1 - x) * 2 + (1 - c)
    partner, along_x, along_y, diag = {"tp": t_pair}, {"tp": t_x}, {"rep": r_y}, {"rep": r_y, "tp": t_x}
    left = k < n // 2
    last = jnp.where(left, 0, n - 1)
    near = jnp.where(left, 1, n - 2)
    far_near, far_last = n - 1 - near, n - 1 - last
    at_end = k == last
    in_middle = k != last
    inner, outer = {"fs": jnp.where(left, k + 1, k - 1)}, {"fs": last}
    blocks = part // lanes
    sub = width // cuts
    half = pl.multiple_of(r * part, part)
    piece = rows // 4
    own_depth = pl.ds(pl.multiple_of(k * depth, depth), depth)

    def gu_load(b, q):
        ref = (wg_ref, wu_ref)[q]
        return pltpu.make_async_copy(
            ref.at[:, pl.ds(half + b * lanes, lanes)], gu.at[b, own_depth, pl.ds(q * lanes, lanes)], gu_l.at[b]
        )

    def dn_load(j):
        return pltpu.make_async_copy(wd_ref.at[pl.ds(half, part), pl.ds(j * sub, sub)], dn.at[k * cuts + j], dn_l)

    tok_load = pltpu.make_async_copy(tok_ref, raw, tok_l)

    tok_load.start()
    for b in range(blocks):
        for q in (0, 1):
            gu_load(b, q).start()
    for j in range(cuts):
        dn_load(j).start()

    barrier = pltpu.get_barrier_semaphore()
    for where in (partner, along_x, along_y, diag, inner):
        pl.semaphore_signal(barrier, inc=1, device_id=where, device_id_type=MESH)

    @pl.when(in_middle)
    def _():
        pl.semaphore_signal(barrier, inc=1, device_id=outer, device_id_type=MESH)

    tok_load.wait()
    tile = 32
    first = (r * 4 + x) * rows

    @pl.loop(0, rows // tile)
    def _(i):
        at = pl.ds(pl.multiple_of(i * tile, tile), tile)
        to = pl.ds(pl.multiple_of(first + i * tile, tile), tile)
        tok[0, to, :] = rms_scale(raw[at, :].astype(jnp.float32), gain_ref[...]).astype(jnp.bfloat16)

    pl.semaphore_wait(barrier, 5 + jnp.where(in_middle, 1, 0))

    def remote(ref, send, recv, where, to=None):
        return pltpu.make_async_remote_copy(
            ref, ref if to is None else to, send, recv, device_id=where, device_id_type=MESH
        )

    def gu_at(s, b):
        return gu.at[b, pl.ds(pl.multiple_of(s * depth, depth), depth)]

    def gu_send(kind, b):
        return remote(
            gu_at(last if kind else k, b), gu_s.at[kind], gu_r.at[b + jnp.where(in_middle, blocks, 0)], inner
        )

    def gu_pass(b):
        remote(gu_at(last, b), gu_s.at[1], gu_r.at[b], inner).wait_recv()
        gu_send(1, b).start()

    def gu_wait(b):
        remote(gu.at[b, pl.ds(0, 2 * depth)], gu_s.at[0], gu_r.at[blocks + b], inner).wait_recv()

    def dn_send(way, s, j):
        at = s * cuts + j
        return remote(dn.at[at], dn_s.at[way], dn_r.at[at], outer if way else inner)

    def dn_wait(s, j):
        at = s * cuts + j
        remote(dn.at[at], dn_s.at[0], dn_r.at[at], inner).wait_recv()

    def pass_down(way, s, j):
        dn_wait(s, j)
        dn_send(way, s, j).start()

    def rows_of(p, r_at, t_at, first, count, core):
        other = (t_at % 2 + core) % 2
        base = (r_at * 4 + other * 2 + t_at // 2) * rows
        return tok.at[p, pl.ds(base + first * piece, count * piece)]

    def z_send(i):
        return remote(rows_of(0, r, t, i, 1, c), z_s, z_r.at[i], inner, rows_of(1, r, t, i, 1, c))

    def z_wait(i):
        remote(rows_of(1, r, t, i, 1, c), z_s, z_r.at[i], inner).wait_recv()

    sends = (
        [((r, t, i, 1), along_x) for i in range(4)]
        + [((r, t, i, 1), along_y) for i in range(4)]
        + [((r, t_x, 0, 1), along_y), ((r, t_x, 1, 1), along_y), ((r_y, t, 2, 1), along_x), ((r_y, t, 3, 1), along_x)]
        + [((r_at, t_at, i, 2), partner) for r_at, t_at in ((r, t), (r, t_x), (r_y, t), (r_y, t_x)) for i in (0, 2)]
    )
    groups = (
        ((0, 1), (6, 7), (2, 3), (4, 5), (8, 9), (10, 11), (12, 13, 14, 15), (16, 17, 18, 19)),
        ((0, 4), (1, 5), (6,), (7,), (2, 3), (8, 9), (10, 11), (12, 13, 14, 15, 16, 17, 18, 19)),
    )

    def group_of(p, i):
        return [g for g, held in enumerate(groups[p]) if i in held][0]

    def go(p, *which):
        for i in which:
            at, where = sends[i]
            to = rows_of(p, *at, 1 - c if i >= 12 else c)
            remote(rows_of(p, *at, c), tok_s.at[p], tok_r.at[p, group_of(p, i)], where, to).start()

    def got(p, *which):
        g = group_of(p, which[0])
        assert groups[p][g] == which
        count = sum(1 if i < 12 else 2 for i in which) * piece
        remote(tok.at[p, pl.ds(0, count)], tok_s.at[p], tok_r.at[p, g], partner).wait_recv()

    quarter = 2 * rows
    halves = 4 * rows

    def half_rows(r_at):
        return pl.ds(pl.multiple_of(r_at * halves, halves), halves)

    def hid_at(p, b, r_at):
        return hid.at[p, half_rows(r_at), pl.ds(pl.multiple_of(b * lanes, lanes), lanes)]

    def hid_send(b, r_at):
        return remote(hid_at(1, b, r_at), hid_s, hid_r.at[r_at], outer, hid_at(0, b, r_at))

    def hid_wait(r_at):
        remote(hid.at[0, half_rows(r_at)], hid_s, hid_r.at[r_at], partner).wait_recv()

    def gated(p, b, r_at):
        both = jnp.dot(tok[p, half_rows(r_at), :], gu[b], preferred_element_type=jnp.float32)
        gate, up = both[:, :lanes], both[:, lanes:]
        hid_at(p, b, r_at)[...] = (gate / (1.0 + jnp.exp(-gate)) * up).astype(jnp.bfloat16)

    def send_own_gu():
        for b in range(blocks):
            pltpu.make_async_copy(gu.at[b, own_depth], gu.at[b, own_depth], gu_l.at[b]).wait()
            gu_send(0, b).start()

    def send_own_dn(way):
        own = dn.at[pl.ds(k * cuts, cuts)]
        pltpu.make_async_copy(own, own, dn_l).wait()
        for j in range(cuts):
            dn_send(way, k, j).start()

    @pl.when(in_middle)
    def _():
        send_own_gu()
        send_own_dn(1)

    @pl.when(at_end)
    def _():
        for i in range(4):
            z_send(i).start()
        send_own_gu()
        send_own_dn(0)

    @pl.when(in_middle)
    def _():
        @pl.loop(0, 12)
        def _(at_step):
            def step(at):
                return pl.when(at_step == at)

            @step(0)
            def _():
                go(0, 0, 1, 6, 7, 12, 13)
                z_wait(0)
                go(1, 0, 4)
                got(0, 0, 1)
                go(0, 14)
                got(0, 6, 7)
                go(0, 17)
                z_wait(1)
                go(1, 1, 5, 12)
                got(1, 0, 4)
                z_wait(2)
                go(1, 2, 6)
                got(1, 1, 5)
                go(1, 14, 16)
                z_wait(3)
                go(1, 13, 3, 7, 8, 9)
                got(1, 6)
                go(1, 10)
                got(1, 7)
                go(1, 17, 11)
                got(1, 2, 3)
                go(1, 15)
                gu_pass(0)
                go(0, 2, 4)
                gu_pass(1)
                got(1, 8, 9)
                go(1, 18)
                got(1, 10, 11)
                go(1, 19)
                go(0, 3, 5, 8, 10)
                got(1, 12, 13, 14, 15, 16, 17, 18, 19)
                gu_wait(0)

            @step(2)
            def _():
                go(0, 9, 11)
                got(0, 2, 3)
                go(0, 15)
                got(0, 4, 5)
                go(0, 16)
                gu_pass(2)
                gu_wait(1)

            @step(4)
            def _():
                got(0, 12, 13, 14, 15)

            @step(6)
            def _():
                dn_wait(last, 0)
                got(0, 8, 9)
                go(0, 18)
                got(0, 10, 11)
                go(0, 19)
                gu_wait(2)
                for j in range(cuts):
                    dn_send(0, k, j).start()
                dn_send(0, last, 0).start()

            @step(9)
            def _():
                pass_down(0, last, 1)
                got(0, 16, 17, 18, 19)

            passed = (at_step < 4) | (at_step == 6) | (at_step == 7)
            b = jnp.where(at_step < 4, at_step // 2, jnp.where(at_step < 6, at_step - 4, jnp.where(at_step < 9, 2, at_step - 9)))
            r_at = jnp.where(passed, (r_y + at_step % 2) % 2, jnp.where(at_step < 9, r, r_y))
            gated(jnp.where(passed, 1, 0), b, r_at)

            @pl.when(passed)
            def _():
                hid_send(b, r_at).start()

    chunks = n * cuts
    mid = sub // 2
    here, there = 0, 1

    def pair_copy(p, side):
        return remote(pair_out.at[p, side], pair_s, pair_r.at[p, side], partner, pair_in.at[p, side])

    def half_copy(p, way):
        return remote(
            half_out.at[p, way], half_s, half_r.at[p], along_y if way else along_x, half_in.at[p, way]
        )

    def full_copy(p, way, part_at):
        return remote(
            full_out.at[p, way, part_at], full_s, full_r.at[p], along_y if way else along_x, full_in.at[p, way, part_at]
        )

    def source(i):
        near_or_last = jnp.where(i == 0, k, near + last - k)
        return jnp.where(i < 2, near_or_last, jnp.where(i == 2, far_near, far_last))

    def place(at):
        return jnp.where(at < chunks, source(at // cuts) * cuts + at % cuts, chunks)

    def product(at, side):
        p = place(at)
        held = jnp.where(at < chunks, p, far_last * cuts + cuts - 1)
        rows_at = half_rows(r_y if side == there else r)
        both = jnp.dot(hid[jnp.where(at < chunks, 0, 1), rows_at, :], dn[held], preferred_element_type=jnp.float32)
        pair_out[p, side] = both[quarter:].astype(jnp.bfloat16)
        pair_copy(p, side).start()
        kept[p, side] = both[:quarter]

    def of(m):
        return pl.ds(pl.multiple_of(m * rows, rows), rows)

    def summed(p, side, x_at):
        return kept[p, side, of(x_at), :] + pair_in[p, side, of(x_at), :].astype(jnp.float32)

    def finish_there(at):
        p = place(at)
        pair_copy(p, there).wait_recv()
        across = summed(p, there, 1 - x).astype(jnp.bfloat16)
        half_out[p, 0] = across[:, :mid]
        half_out[p, 1] = across[:, mid:]
        half_copy(p, 0).start()
        half_copy(p, 1).start()
        value = summed(p, there, x)
        kept[p, there, of(x), :mid] = value[:, :mid]
        full_out[p, 1, 1] = value[:, mid:].astype(jnp.bfloat16)
        full_copy(p, 1, 1).start()

    def finish_here(at):
        p = place(at)
        pair_copy(p, here).wait_recv()
        value = summed(p, here, 1 - x)
        kept[p, here, of(1 - x), mid:] = value[:, mid:]
        full_out[p, 0, 0] = value[:, :mid].astype(jnp.bfloat16)
        full_copy(p, 0, 0).start()
        fin[p] = summed(p, here, x)

    def finish_half(at):
        p = place(at)
        remote(half_in.at[p], half_s, half_r.at[p], partner).wait_recv()
        full_out[p, 0, 1] = (kept[p, here, of(1 - x), mid:] + half_in[p, 1].astype(jnp.float32)).astype(jnp.bfloat16)
        full_copy(p, 0, 1).start()
        full_out[p, 1, 0] = (kept[p, there, of(x), :mid] + half_in[p, 0].astype(jnp.float32)).astype(jnp.bfloat16)
        full_copy(p, 1, 0).start()

    early = 2 * cuts

    @pl.when(at_end)
    def _():
        for j in range(cuts):
            dn_wait(near, j)
        hid_wait(r_y)

    @pl.loop(0, early)
    def _(at):
        product(at, there)

        @pl.when(at > 0)
        def _():
            finish_there(at - 1)

        @pl.when(in_middle & (at == 1))
        def _():
            pass_down(1, far_near, 0)

    @pl.when(at_end)
    def _():
        hid_wait(r)

    @pl.loop(0, early)
    def _(at):
        product(at, here)

        @pl.when(at == 0)
        def _():
            finish_there(early - 1)

        @pl.when(at > 0)
        def _():
            finish_here(at - 1)
            finish_half(at - 1)

        @pl.when(in_middle & (at == 1))
        def _():
            pass_down(1, far_near, 1)

    def order(i):
        return jnp.where(in_middle & (i >= 2), jnp.where(i == 2, chunks, early + i - 1), early + i)

    @pl.loop(0, chunks - early + 1)
    def _(i):
        at = order(i)

        @pl.when(at_end & (i < 3))
        def _():
            dn_wait(source(at // cuts), at % cuts)

        @pl.when(in_middle & (i == 0))
        def _():
            pass_down(1, far_last, 0)

        @pl.when(in_middle & (i == 2))
        def _():
            dn_wait(far_last, cuts - 1)

        @pl.when(in_middle | (i < 3))
        def _():
            product(at, there)
            product(at, here)

        @pl.when(i == 0)
        def _():
            finish_here(early - 1)
            finish_half(early - 1)

        @pl.when(in_middle | (i < 3))
        def _():
            finish_there(at)
            finish_here(at)

        @pl.when((i > 0) & (in_middle | (i < 4)))
        def _():
            finish_half(order(i - 1))

    result = remote(res_out, res_s, res_r, outer, res_in)

    def collect(at, part_at):
        p = place(at)
        cols = pl.ds(part_at * mid, mid)
        both = full_in[p, 0, part_at].astype(jnp.float32) + full_in[p, 1, part_at].astype(jnp.float32)
        return fin[p, :, cols] + both

    def arrive(at):
        remote(full_in.at[place(at)], full_s, full_r.at[place(at)], along_x).wait_recv()

    @pl.when(in_middle)
    def _():
        arrive(chunks)
        for part_at in (0, 1):
            res_out[:, pl.ds(part_at * mid, mid)] = collect(chunks, part_at).astype(jnp.bfloat16)
        result.start()
        finish_half(chunks - 1)

    remote(gu.at[:, pl.ds(0, depth)], gu_s.at[0], gu_r.at[0], inner).wait_send()

    @pl.when(at_end)
    def _():
        remote(tok.at[0, pl.ds(0, rows)], z_s, z_r.at[0], inner).wait_send()
        remote(dn.at[pl.ds(0, cuts)], dn_s.at[0], dn_r.at[0], inner).wait_send()
        remote(pair_out.at[pl.ds(0, chunks - 1)], pair_s, pair_r.at[0, 0], partner).wait_send()
        remote(half_out.at[pl.ds(0, chunks - 1)], half_s, half_r.at[0], along_x).wait_send()

    @pl.when(in_middle)
    def _():
        for p in (0, 1):
            total = sum(1 if i < 12 else 2 for i in range(len(sends))) * piece
            remote(tok.at[p, pl.ds(0, total)], tok_s.at[p], tok_r.at[p, 0], partner).wait_send()
        remote(gu.at[:, pl.ds(0, depth)], gu_s.at[1], gu_r.at[0], inner).wait_send()
        remote(hid.at[1], hid_s, hid_r.at[0], outer).wait_send()
        remote(dn.at[pl.ds(0, 2 * cuts)], dn_s.at[0], dn_r.at[0], inner).wait_send()
        remote(dn.at[pl.ds(0, 3 * cuts - 1)], dn_s.at[1], dn_r.at[0], outer).wait_send()
        remote(pair_out, pair_s, pair_r.at[0, 0], partner).wait_send()
        remote(half_out, half_s, half_r.at[0], along_x).wait_send()

    squares[...] = jnp.zeros_like(squares)

    def settle(at, part_at, total):
        fin[place(at), :, pl.ds(part_at * mid, mid)] = total
        squares[...] += total * total

    @pl.loop(0, chunks)
    def _(at):
        @pl.when(in_middle | (at < chunks - 1))
        def _():
            arrive(at)
            for part_at in (0, 1):
                settle(at, part_at, collect(at, part_at))

    @pl.when(at_end)
    def _():
        result.wait_recv()
        for part_at in (0, 1):
            settle(chunks - 1, part_at, res_in[:, pl.ds(part_at * mid, mid)].astype(jnp.float32))

    scale = lax.rsqrt(jnp.sum(squares[...], axis=-1, keepdims=True) / (n * width) + EPS)
    for p in range(chunks):
        cols = pl.ds(p * sub, sub)
        out_ref[:, cols] = (fin[p] * scale * post_ref[:, cols]).astype(out_ref.dtype)

    @pl.when(at_end)
    def _():
        remote(full_out.at[pl.ds(0, chunks - 1)], full_s, full_r.at[0], along_x).wait_send()

    @pl.when(in_middle)
    def _():
        remote(full_out, full_s, full_r.at[0], along_x).wait_send()
        result.wait_send()


def chain_body(n, tokens, norm_gain, w_gate, w_up, w_down, post_gain):
    rows, model = tokens.shape
    depth, block = w_gate.shape
    width = w_down.shape[1]
    part = block // 2
    cuts = width // PIECE
    sub = width // cuts
    blocks = part // LANES
    chunks = n * cuts
    vmem, dma = pltpu.VMEM, pltpu.SemaphoreType.DMA
    low, full = jnp.bfloat16, jnp.float32
    anywhere = pl.BlockSpec(memory_space=pl.ANY)
    inside = pl.BlockSpec(memory_space=vmem)
    return pl.pallas_call(
        functools.partial(kernel, n, rows, depth, part, width, cuts, LANES),
        out_shape=pltpu.VMEM((rows, model), low),
        in_specs=[anywhere, inside, anywhere, anywhere, anywhere, inside],
        out_specs=inside,
        scratch_shapes=[
            vmem((rows, model), low),
            vmem((2, 8 * rows, model), low),
            vmem((blocks, n * depth, 2 * LANES), low),
            vmem((chunks, part, sub), low),
            vmem((2, 8 * rows, part), low),
            vmem((chunks + 1, 2, 2 * rows, sub), full),
            vmem((chunks + 1, 2, 2 * rows, sub), low),
            vmem((chunks + 1, 2, 2 * rows, sub), low),
            vmem((chunks + 1, 2, rows, sub // 2), low),
            vmem((chunks + 1, 2, rows, sub // 2), low),
            vmem((chunks + 1, 2, 2, rows, sub // 2), low),
            vmem((chunks + 1, 2, 2, rows, sub // 2), low),
            vmem((chunks + 1, rows, sub), full),
            vmem((rows, sub), low),
            vmem((rows, sub), low),
            vmem((rows, sub // 2), full),
            dma(()),
            dma((blocks,)),
            dma(()),
            dma(()),
            dma((4,)),
            dma((2,)),
            dma((2, 8)),
            dma((2,)),
            dma((2 * blocks,)),
            dma((2,)),
            dma((chunks,)),
            dma(()),
            dma((2,)),
            dma(()),
            dma((chunks + 1, 2)),
            dma(()),
            dma((chunks + 1,)),
            dma(()),
            dma((chunks + 1,)),
            dma(()),
            dma(()),
        ],
        compiler_params=pltpu.CompilerParams(
            collective_id=0, has_side_effects=True, vmem_limit_bytes=56 * 2**20
        ),
    )(tokens, norm_gain.reshape(1, -1), w_gate, w_up, w_down, post_gain.reshape(1, -1))


def solution(mesh):
    n = mesh.shape["fs"]

    def body(tokens, norm_gain, w_gate, w_up, w_down, post_gain):
        args = (tokens, norm_gain, w_gate, w_up, w_down, post_gain)
        rows = tokens.shape[0]
        fits = (
            mesh.shape["rep"] == 2 and mesh.shape["tp"] == 4 and n == 4 and rows <= 128 and rows % 128 == 0
            and w_gate.shape[1] == 6 * LANES and w_down.shape[1] == 2 * PIECE
        )
        return chain_body(n, *args) if fits else plain_body(*args)

    return jax.shard_map(
        body,
        mesh=mesh,
        in_specs=(
            P(("rep", "fs", "tp"), None),
            P(),
            P("fs", "tp"),
            P("fs", "tp"),
            P("tp", "fs"),
            P(),
        ),
        out_specs=P(("rep", "fs", "tp"), None),
        check_vma=False,
    )
```

```python
import functools

import jax
import jax.numpy as jnp
from jax import lax
from jax.experimental import pallas as pl
from jax.experimental.pallas import tpu as pltpu
from jax.sharding import PartitionSpec as P

EPS = 1e-06
MESH = pl.DeviceIdType.MESH
PIECE = 256
LANES = 128


def rms_scale(values, gain):
    return values * lax.rsqrt(jnp.mean(values * values, axis=-1, keepdims=True) + EPS) * gain


def plain_body(tokens, norm_gain, w_gate, w_up, w_down, post_gain):
    own_normed = rms_scale(tokens.astype(jnp.float32), norm_gain).astype(jnp.bfloat16)
    normed = lax.all_gather(own_normed, "tp", axis=0, tiled=True)
    gate = jnp.dot(
        normed, lax.all_gather(w_gate, "fs", axis=0, tiled=True), preferred_element_type=jnp.float32
    )
    up = jnp.dot(
        normed, lax.all_gather(w_up, "fs", axis=0, tiled=True), preferred_element_type=jnp.float32
    )
    hidden = (jax.nn.silu(gate) * up).astype(jnp.bfloat16)
    terms = jnp.dot(
        hidden, lax.all_gather(w_down, "fs", axis=1, tiled=True), preferred_element_type=jnp.float32
    )
    summed = lax.psum_scatter(
        terms.astype(jnp.bfloat16), "tp", scatter_dimension=0, tiled=True
    ).astype(jnp.float32)
    return rms_scale(summed, post_gain).astype(jnp.bfloat16)


def kernel(
    n, rows, depth, part, width, cuts, lanes,
    tok_ref, gain_ref, wg_ref, wu_ref, wd_ref, post_ref, out_ref,
    raw, tok, gu, dn, hid, kept, pair_out, pair_in, half_out, half_in, full_out, full_in, fin, res_out, res_in, squares,
    tok_l, gu_l, dn_l, z_s, z_r, tok_s, tok_r, gu_s, gu_r, dn_s, dn_r, hid_s, hid_r,
    pair_s, pair_r, half_s, half_r, full_s, full_r, res_s, res_r,
):
    r, k, t = lax.axis_index("rep"), lax.axis_index("fs"), lax.axis_index("tp")
    x, c = t // 2, t % 2
    t_pair, t_x, r_y = x * 2 + (1 - c), (1 - x) * 2 + c, 1 - r
    t_px = (1 - x) * 2 + (1 - c)
    partner, along_x, along_y, diag = {"tp": t_pair}, {"tp": t_x}, {"rep": r_y}, {"rep": r_y, "tp": t_x}
    left = k < n // 2
    last = jnp.where(left, 0, n - 1)
    near = jnp.where(left, 1, n - 2)
    far_near, far_last = n - 1 - near, n - 1 - last
    at_end = k == last
    in_middle = k != last
    inner, outer = {"fs": jnp.where(left, k + 1, k - 1)}, {"fs": last}
    blocks = part // lanes
    sub = width // cuts
    half = pl.multiple_of(r * part, part)
    piece = rows // 4
    own_depth = pl.ds(pl.multiple_of(k * depth, depth), depth)

    def gu_load(b, q):
        ref = (wg_ref, wu_ref)[q]
        return pltpu.make_async_copy(
            ref.at[:, pl.ds(half + b * lanes, lanes)], gu.at[b, own_depth, pl.ds(q * lanes, lanes)], gu_l.at[b]
        )

    def dn_load(j):
        return pltpu.make_async_copy(wd_ref.at[pl.ds(half, part), pl.ds(j * sub, sub)], dn.at[k * cuts + j], dn_l)

    tok_load = pltpu.make_async_copy(tok_ref, raw, tok_l)

    tok_load.start()
    for b in range(blocks):
        for q in (0, 1):
            gu_load(b, q).start()
    for j in range(cuts):
        dn_load(j).start()

    barrier = pltpu.get_barrier_semaphore()
    for where in (partner, along_x, along_y, diag, inner):
        pl.semaphore_signal(barrier, inc=1, device_id=where, device_id_type=MESH)

    @pl.when(in_middle)
    def _():
        pl.semaphore_signal(barrier, inc=1, device_id=outer, device_id_type=MESH)

    tok_load.wait()
    tile = 32
    first = (r * 4 + x) * rows

    @pl.loop(0, rows // tile)
    def _(i):
        at = pl.ds(pl.multiple_of(i * tile, tile), tile)
        to = pl.ds(pl.multiple_of(first + i * tile, tile), tile)
        tok[0, to, :] = rms_scale(raw[at, :].astype(jnp.float32), gain_ref[...]).astype(jnp.bfloat16)

    pl.semaphore_wait(barrier, 5 + jnp.where(in_middle, 1, 0))

    def remote(ref, send, recv, where, to=None):
        return pltpu.make_async_remote_copy(
            ref, ref if to is None else to, send, recv, device_id=where, device_id_type=MESH
        )

    pieces = 2
    step_depth = depth // pieces

    def gu_at(s, b, h):
        return gu.at[b, pl.ds(pl.multiple_of(s * depth + h * step_depth, step_depth), step_depth)]

    def gu_send(kind, b, h):
        at = jnp.where(in_middle, pieces * blocks + b, pieces * b + h)
        return remote(gu_at(last if kind else k, b, h), gu_s.at[kind], gu_r.at[at], inner)

    def gu_pass(b, h):
        remote(gu_at(last, b, h), gu_s.at[1], gu_r.at[pieces * b + h], inner).wait_recv()
        gu_send(1, b, h).start()

    def gu_wait(b):
        remote(gu.at[b, pl.ds(0, 2 * depth)], gu_s.at[0], gu_r.at[pieces * blocks + b], inner).wait_recv()

    def dn_send(way, s, j):
        at = s * cuts + j
        return remote(dn.at[at], dn_s.at[way], dn_r.at[at], outer if way else inner)

    def dn_wait(s, j):
        at = s * cuts + j
        remote(dn.at[at], dn_s.at[0], dn_r.at[at], inner).wait_recv()

    def pass_down(way, s, j):
        dn_wait(s, j)
        dn_send(way, s, j).start()

    def rows_of(p, r_at, t_at, first, count, core):
        other = (t_at % 2 + core) % 2
        base = (r_at * 4 + other * 2 + t_at // 2) * rows
        return tok.at[p, pl.ds(base + first * piece, count * piece)]

    def z_send(i):
        return remote(rows_of(0, r, t, i, 1, c), z_s, z_r.at[i], inner, rows_of(1, r, t, i, 1, c))

    def z_wait(i):
        remote(rows_of(1, r, t, i, 1, c), z_s, z_r.at[i], inner).wait_recv()

    sends = (
        [((r, t, i, 1), along_x) for i in range(4)]
        + [((r, t, i, 1), along_y) for i in range(4)]
        + [((r, t_x, 0, 1), along_y), ((r, t_x, 1, 1), along_y), ((r_y, t, 2, 1), along_x), ((r_y, t, 3, 1), along_x)]
        + [((r_at, t_at, i, 2), partner) for r_at, t_at in ((r, t), (r, t_x), (r_y, t), (r_y, t_x)) for i in (0, 2)]
    )
    groups = (
        ((0, 1), (6, 7), (2, 3), (4, 5), (8, 9), (10, 11), (12, 13, 14, 15), (16, 17, 18, 19)),
        ((0, 4), (1, 5), (6,), (7,), (2, 3), (8, 9), (10, 11), (12, 13, 14, 15, 16, 17, 18, 19)),
    )

    def group_of(p, i):
        return [g for g, held in enumerate(groups[p]) if i in held][0]

    def go(p, *which):
        for i in which:
            at, where = sends[i]
            to = rows_of(p, *at, 1 - c if i >= 12 else c)
            remote(rows_of(p, *at, c), tok_s.at[p], tok_r.at[p, group_of(p, i)], where, to).start()

    def got(p, *which):
        g = group_of(p, which[0])
        assert groups[p][g] == which
        count = sum(1 if i < 12 else 2 for i in which) * piece
        remote(tok.at[p, pl.ds(0, count)], tok_s.at[p], tok_r.at[p, g], partner).wait_recv()

    quarter = 2 * rows
    halves = 4 * rows

    def half_rows(r_at):
        return pl.ds(pl.multiple_of(r_at * halves, halves), halves)

    def hid_at(p, b, r_at):
        return hid.at[p, half_rows(r_at), pl.ds(pl.multiple_of(b * lanes, lanes), lanes)]

    def hid_send(b, r_at):
        return remote(hid_at(1, b, r_at), hid_s, hid_r.at[r_at], outer, hid_at(0, b, r_at))

    def hid_wait(r_at):
        remote(hid.at[0, half_rows(r_at)], hid_s, hid_r.at[r_at], partner).wait_recv()

    def gated(p, b, r_at):
        both = jnp.dot(tok[p, half_rows(r_at), :], gu[b], preferred_element_type=jnp.float32)
        gate, up = both[:, :lanes], both[:, lanes:]
        hid_at(p, b, r_at)[...] = (gate / (1.0 + jnp.exp(-gate)) * up).astype(jnp.bfloat16)

    def send_own_gu():
        for b in range(blocks):
            pltpu.make_async_copy(gu.at[b, own_depth], gu.at[b, own_depth], gu_l.at[b]).wait()
            for h in range(pieces):
                gu_send(0, b, h).start()

    def send_own_dn(way):
        own = dn.at[pl.ds(k * cuts, cuts)]
        pltpu.make_async_copy(own, own, dn_l).wait()
        for j in range(cuts):
            dn_send(way, k, j).start()

    @pl.when(in_middle)
    def _():
        send_own_gu()
        send_own_dn(1)

    @pl.when(at_end)
    def _():
        for i in range(4):
            z_send(i).start()
        send_own_gu()
        send_own_dn(0)

    @pl.when(in_middle)
    def _():
        @pl.loop(0, 12)
        def _(at_step):
            def step(at):
                return pl.when(at_step == at)

            @step(0)
            def _():
                go(0, 0, 1, 6, 7, 12, 13)
                z_wait(0)
                go(1, 0, 4)
                got(0, 0, 1)
                go(0, 14)
                got(0, 6, 7)
                go(0, 17)
                z_wait(1)
                go(1, 1, 5, 12)
                got(1, 0, 4)
                z_wait(2)
                go(1, 2, 6)
                got(1, 1, 5)
                go(1, 14, 16)
                z_wait(3)
                go(1, 13, 3, 7, 8, 9)
                got(1, 6)
                go(1, 10)
                gu_pass(0, 0)
                got(1, 7)
                go(1, 17, 11)
                got(1, 2, 3)
                go(1, 15)
                gu_pass(0, 1)
                go(0, 2, 4)
                gu_pass(1, 0)
                go(0, 3, 5)
                got(1, 8, 9)
                go(1, 18)
                got(1, 10, 11)
                go(1, 19)
                go(0, 8, 10)
                gu_pass(1, 1)
                got(1, 12, 13, 14, 15, 16, 17, 18, 19)
                gu_wait(0)

            @step(2)
            def _():
                go(0, 9, 11)
                gu_pass(2, 0)
                got(0, 2, 3)
                go(0, 15)
                got(0, 4, 5)
                go(0, 16)
                gu_pass(2, 1)
                gu_wait(1)

            @step(4)
            def _():
                got(0, 12, 13, 14, 15)

            @step(6)
            def _():
                dn_wait(last, 0)
                got(0, 8, 9)
                go(0, 18)
                got(0, 10, 11)
                go(0, 19)
                gu_wait(2)

            @pl.when(at_step == 6 + c)
            def _():
                for j in range(cuts):
                    dn_send(0, k, j).start()
                dn_send(0, last, 0).start()

            @step(9)
            def _():
                pass_down(0, last, 1)
                got(0, 16, 17, 18, 19)

            passed = (at_step < 4) | (at_step == 6) | (at_step == 7)
            b = jnp.where(at_step < 4, at_step // 2, jnp.where(at_step < 6, at_step - 4, jnp.where(at_step < 9, 2, at_step - 9)))
            r_at = jnp.where(passed, (r_y + at_step % 2) % 2, jnp.where(at_step < 9, r, r_y))
            gated(jnp.where(passed, 1, 0), b, r_at)

            @pl.when(passed)
            def _():
                hid_send(b, r_at).start()

    chunks = n * cuts
    mid = sub // 2
    here, there = 0, 1

    def pair_copy(p, side):
        return remote(pair_out.at[p, side], pair_s, pair_r.at[p, side], partner, pair_in.at[p, side])

    def half_copy(p, way):
        return remote(
            half_out.at[p, way], half_s, half_r.at[p], along_y if way else along_x, half_in.at[p, way]
        )

    def full_copy(p, way, part_at):
        return remote(
            full_out.at[p, way, part_at], full_s, full_r.at[p], along_y if way else along_x, full_in.at[p, way, part_at]
        )

    def source(i):
        near_or_last = jnp.where(i == 0, k, near + last - k)
        return jnp.where(i < 2, near_or_last, jnp.where(i == 2, far_near, far_last))

    def place(at):
        return jnp.where(at < chunks, source(at // cuts) * cuts + at % cuts, chunks)

    def product(at, side):
        p = place(at)
        held = jnp.where(at < chunks, p, far_last * cuts + cuts - 1)
        rows_at = half_rows(r_y if side == there else r)
        both = jnp.dot(hid[jnp.where(at < chunks, 0, 1), rows_at, :], dn[held], preferred_element_type=jnp.float32)
        pair_out[p, side] = both[quarter:].astype(jnp.bfloat16)
        pair_copy(p, side).start()
        kept[p, side] = both[:quarter]

    def of(m):
        return pl.ds(pl.multiple_of(m * rows, rows), rows)

    def summed(p, side, x_at):
        return kept[p, side, of(x_at), :] + pair_in[p, side, of(x_at), :].astype(jnp.float32)

    def finish_there(at):
        p = place(at)
        pair_copy(p, there).wait_recv()
        across = summed(p, there, 1 - x).astype(jnp.bfloat16)
        half_out[p, 0] = across[:, :mid]
        half_out[p, 1] = across[:, mid:]
        half_copy(p, 0).start()
        half_copy(p, 1).start()
        value = summed(p, there, x)
        kept[p, there, of(x), :mid] = value[:, :mid]
        full_out[p, 1, 1] = value[:, mid:].astype(jnp.bfloat16)
        full_copy(p, 1, 1).start()

    def finish_here(at):
        p = place(at)
        pair_copy(p, here).wait_recv()
        value = summed(p, here, 1 - x)
        kept[p, here, of(1 - x), mid:] = value[:, mid:]
        full_out[p, 0, 0] = value[:, :mid].astype(jnp.bfloat16)
        full_copy(p, 0, 0).start()
        fin[p] = summed(p, here, x)

    def finish_half(at):
        p = place(at)
        remote(half_in.at[p], half_s, half_r.at[p], partner).wait_recv()
        full_out[p, 0, 1] = (kept[p, here, of(1 - x), mid:] + half_in[p, 1].astype(jnp.float32)).astype(jnp.bfloat16)
        full_copy(p, 0, 1).start()
        full_out[p, 1, 0] = (kept[p, there, of(x), :mid] + half_in[p, 0].astype(jnp.float32)).astype(jnp.bfloat16)
        full_copy(p, 1, 0).start()

    early = 2 * cuts

    @pl.when(at_end)
    def _():
        for j in range(cuts):
            dn_wait(near, j)
        hid_wait(r_y)

    @pl.loop(0, early)
    def _(at):
        product(at, there)

        @pl.when(at > 0)
        def _():
            finish_there(at - 1)

        @pl.when(in_middle & (at == 1))
        def _():
            pass_down(1, far_near, 0)

    @pl.when(at_end)
    def _():
        hid_wait(r)

    @pl.loop(0, early)
    def _(at):
        product(at, here)

        @pl.when(at == 0)
        def _():
            finish_there(early - 1)

        @pl.when(at > 0)
        def _():
            finish_here(at - 1)
            finish_half(at - 1)


    def order(i):
        return jnp.where(in_middle & (i >= 2), jnp.where(i == 2, chunks, early + i - 1), early + i)

    @pl.loop(0, chunks - early + 1)
    def _(i):
        at = order(i)

        @pl.when(at_end & (i < 3))
        def _():
            dn_wait(source(at // cuts), at % cuts)

        @pl.when(in_middle & (i == 0))
        def _():
            pass_down(1, far_near, 1)

        @pl.when(in_middle & (i == 1))
        def _():
            pass_down(1, far_last, 0)

        @pl.when(in_middle & (i == 2))
        def _():
            dn_wait(far_last, cuts - 1)

        @pl.when(in_middle | (i < 3))
        def _():
            product(at, there)
            product(at, here)

        @pl.when(i == 0)
        def _():
            finish_here(early - 1)
            finish_half(early - 1)

        @pl.when(in_middle | (i < 3))
        def _():
            finish_there(at)
            finish_here(at)

        @pl.when((i > 0) & (in_middle | (i < 4)))
        def _():
            finish_half(order(i - 1))

    result = remote(res_out, res_s, res_r, outer, res_in)

    def collect(at, part_at):
        p = place(at)
        cols = pl.ds(part_at * mid, mid)
        both = full_in[p, 0, part_at].astype(jnp.float32) + full_in[p, 1, part_at].astype(jnp.float32)
        return fin[p, :, cols] + both

    def arrive(at):
        remote(full_in.at[place(at)], full_s, full_r.at[place(at)], along_x).wait_recv()

    @pl.when(in_middle)
    def _():
        arrive(chunks)
        for part_at in (0, 1):
            res_out[:, pl.ds(part_at * mid, mid)] = collect(chunks, part_at).astype(jnp.bfloat16)
        result.start()
        finish_half(chunks - 1)

    remote(gu.at[:, pl.ds(0, depth)], gu_s.at[0], gu_r.at[0], inner).wait_send()

    @pl.when(at_end)
    def _():
        remote(tok.at[0, pl.ds(0, rows)], z_s, z_r.at[0], inner).wait_send()
        remote(dn.at[pl.ds(0, cuts)], dn_s.at[0], dn_r.at[0], inner).wait_send()
        remote(pair_out.at[pl.ds(0, chunks - 1)], pair_s, pair_r.at[0, 0], partner).wait_send()
        remote(half_out.at[pl.ds(0, chunks - 1)], half_s, half_r.at[0], along_x).wait_send()

    @pl.when(in_middle)
    def _():
        for p in (0, 1):
            total = sum(1 if i < 12 else 2 for i in range(len(sends))) * piece
            remote(tok.at[p, pl.ds(0, total)], tok_s.at[p], tok_r.at[p, 0], partner).wait_send()
        remote(gu.at[:, pl.ds(0, depth)], gu_s.at[1], gu_r.at[0], inner).wait_send()
        remote(hid.at[1], hid_s, hid_r.at[0], outer).wait_send()
        remote(dn.at[pl.ds(0, 2 * cuts)], dn_s.at[0], dn_r.at[0], inner).wait_send()
        remote(dn.at[pl.ds(0, 3 * cuts - 1)], dn_s.at[1], dn_r.at[0], outer).wait_send()
        remote(pair_out, pair_s, pair_r.at[0, 0], partner).wait_send()
        remote(half_out, half_s, half_r.at[0], along_x).wait_send()

    squares[...] = jnp.zeros_like(squares)

    def settle(at, part_at, total):
        fin[place(at), :, pl.ds(part_at * mid, mid)] = total
        squares[...] += total * total

    @pl.loop(0, chunks)
    def _(at):
        @pl.when(in_middle | (at < chunks - 1))
        def _():
            arrive(at)
            for part_at in (0, 1):
                settle(at, part_at, collect(at, part_at))

    @pl.when(at_end)
    def _():
        result.wait_recv()
        for part_at in (0, 1):
            settle(chunks - 1, part_at, res_in[:, pl.ds(part_at * mid, mid)].astype(jnp.float32))

    scale = lax.rsqrt(jnp.sum(squares[...], axis=-1, keepdims=True) / (n * width) + EPS)
    for p in range(chunks):
        cols = pl.ds(p * sub, sub)
        out_ref[:, cols] = (fin[p] * scale * post_ref[:, cols]).astype(out_ref.dtype)

    @pl.when(at_end)
    def _():
        remote(full_out.at[pl.ds(0, chunks - 1)], full_s, full_r.at[0], along_x).wait_send()

    @pl.when(in_middle)
    def _():
        remote(full_out, full_s, full_r.at[0], along_x).wait_send()
        result.wait_send()


def chain_body(n, tokens, norm_gain, w_gate, w_up, w_down, post_gain):
    rows, model = tokens.shape
    depth, block = w_gate.shape
    width = w_down.shape[1]
    part = block // 2
    cuts = width // PIECE
    sub = width // cuts
    blocks = part // LANES
    chunks = n * cuts
    vmem, dma = pltpu.VMEM, pltpu.SemaphoreType.DMA
    low, full = jnp.bfloat16, jnp.float32
    anywhere = pl.BlockSpec(memory_space=pl.ANY)
    inside = pl.BlockSpec(memory_space=vmem)
    return pl.pallas_call(
        functools.partial(kernel, n, rows, depth, part, width, cuts, LANES),
        out_shape=pltpu.VMEM((rows, model), low),
        in_specs=[anywhere, inside, anywhere, anywhere, anywhere, inside],
        out_specs=inside,
        scratch_shapes=[
            vmem((rows, model), low),
            vmem((2, 8 * rows, model), low),
            vmem((blocks, n * depth, 2 * LANES), low),
            vmem((chunks, part, sub), low),
            vmem((2, 8 * rows, part), low),
            vmem((chunks + 1, 2, 2 * rows, sub), full),
            vmem((chunks + 1, 2, 2 * rows, sub), low),
            vmem((chunks + 1, 2, 2 * rows, sub), low),
            vmem((chunks + 1, 2, rows, sub // 2), low),
            vmem((chunks + 1, 2, rows, sub // 2), low),
            vmem((chunks + 1, 2, 2, rows, sub // 2), low),
            vmem((chunks + 1, 2, 2, rows, sub // 2), low),
            vmem((chunks + 1, rows, sub), full),
            vmem((rows, sub), low),
            vmem((rows, sub), low),
            vmem((rows, sub // 2), full),
            dma(()),
            dma((blocks,)),
            dma(()),
            dma(()),
            dma((4,)),
            dma((2,)),
            dma((2, 8)),
            dma((2,)),
            dma((3 * blocks,)),
            dma((2,)),
            dma((chunks,)),
            dma(()),
            dma((2,)),
            dma(()),
            dma((chunks + 1, 2)),
            dma(()),
            dma((chunks + 1,)),
            dma(()),
            dma((chunks + 1,)),
            dma(()),
            dma(()),
        ],
        compiler_params=pltpu.CompilerParams(
            collective_id=0, has_side_effects=True, vmem_limit_bytes=56 * 2**20
        ),
    )(tokens, norm_gain.reshape(1, -1), w_gate, w_up, w_down, post_gain.reshape(1, -1))


def solution(mesh):
    n = mesh.shape["fs"]

    def body(tokens, norm_gain, w_gate, w_up, w_down, post_gain):
        args = (tokens, norm_gain, w_gate, w_up, w_down, post_gain)
        rows = tokens.shape[0]
        fits = (
            mesh.shape["rep"] == 2 and mesh.shape["tp"] == 4 and n == 4 and rows <= 128 and rows % 128 == 0
            and w_gate.shape[1] == 6 * LANES and w_down.shape[1] == 2 * PIECE
        )
        return chain_body(n, *args) if fits else plain_body(*args)

    return jax.shard_map(
        body,
        mesh=mesh,
        in_specs=(
            P(("rep", "fs", "tp"), None),
            P(),
            P("fs", "tp"),
            P("fs", "tp"),
            P("tp", "fs"),
            P(),
        ),
        out_specs=P(("rep", "fs", "tp"), None),
        check_vma=False,
    )
```

```python
import functools

import jax
import jax.numpy as jnp
from jax import lax
from jax.experimental import pallas as pl
from jax.experimental.pallas import tpu as pltpu
from jax.sharding import PartitionSpec as P

EPS = 1e-06
MESH = pl.DeviceIdType.MESH
PIECE = 256
LANES = 128


def rms_scale(values, gain):
    return values * lax.rsqrt(jnp.mean(values * values, axis=-1, keepdims=True) + EPS) * gain


def plain_body(tokens, norm_gain, w_gate, w_up, w_down, post_gain):
    own_normed = rms_scale(tokens.astype(jnp.float32), norm_gain).astype(jnp.bfloat16)
    normed = lax.all_gather(own_normed, "tp", axis=0, tiled=True)
    gate = jnp.dot(
        normed, lax.all_gather(w_gate, "fs", axis=0, tiled=True), preferred_element_type=jnp.float32
    )
    up = jnp.dot(
        normed, lax.all_gather(w_up, "fs", axis=0, tiled=True), preferred_element_type=jnp.float32
    )
    hidden = (jax.nn.silu(gate) * up).astype(jnp.bfloat16)
    terms = jnp.dot(
        hidden, lax.all_gather(w_down, "fs", axis=1, tiled=True), preferred_element_type=jnp.float32
    )
    summed = lax.psum_scatter(
        terms.astype(jnp.bfloat16), "tp", scatter_dimension=0, tiled=True
    ).astype(jnp.float32)
    return rms_scale(summed, post_gain).astype(jnp.bfloat16)


def kernel(
    n, rows, depth, part, width, cuts, lanes,
    tok_ref, gain_ref, wg_ref, wu_ref, wd_ref, post_ref, out_ref,
    raw, tok, gu, dn, hid, kept, pair_out, pair_in, half_out, half_in, full_out, full_in, fin, res_out, res_in, diag_out, diag_in, squares,
    tok_l, gu_l, dn_l, z_s, z_r, tok_s, tok_r, gu_s, gu_r, dn_s, dn_r, hid_s, hid_r,
    pair_s, pair_r, half_s, half_r, full_s, full_r, res_s, res_r, diag_s, diag_r,
):
    r, k, t = lax.axis_index("rep"), lax.axis_index("fs"), lax.axis_index("tp")
    x, c = t // 2, t % 2
    t_pair, t_x, r_y = x * 2 + (1 - c), (1 - x) * 2 + c, 1 - r
    t_px = (1 - x) * 2 + (1 - c)
    partner, along_x, along_y, diag = {"tp": t_pair}, {"tp": t_x}, {"rep": r_y}, {"rep": r_y, "tp": t_x}
    left = k < n // 2
    last = jnp.where(left, 0, n - 1)
    near = jnp.where(left, 1, n - 2)
    far_near, far_last = n - 1 - near, n - 1 - last
    at_end = k == last
    in_middle = k != last
    inner, outer = {"fs": jnp.where(left, k + 1, k - 1)}, {"fs": last}
    blocks = part // lanes
    sub = width // cuts
    half = pl.multiple_of(r * part, part)
    piece = rows // 4
    own_depth = pl.ds(pl.multiple_of(k * depth, depth), depth)

    def gu_load(b, q):
        ref = (wg_ref, wu_ref)[q]
        return pltpu.make_async_copy(
            ref.at[:, pl.ds(half + b * lanes, lanes)], gu.at[b, own_depth, pl.ds(q * lanes, lanes)], gu_l.at[b]
        )

    def dn_load(j):
        return pltpu.make_async_copy(wd_ref.at[pl.ds(half, part), pl.ds(j * sub, sub)], dn.at[k * cuts + j], dn_l)

    tok_load = pltpu.make_async_copy(tok_ref, raw, tok_l)

    tok_load.start()
    for b in range(blocks):
        for q in (0, 1):
            gu_load(b, q).start()
    for j in range(cuts):
        dn_load(j).start()

    barrier = pltpu.get_barrier_semaphore()
    for where in (partner, along_x, along_y, diag, inner):
        pl.semaphore_signal(barrier, inc=1, device_id=where, device_id_type=MESH)

    @pl.when(in_middle)
    def _():
        pl.semaphore_signal(barrier, inc=1, device_id=outer, device_id_type=MESH)

    tok_load.wait()
    tile = 32
    first = (r * 4 + x) * rows

    @pl.loop(0, rows // tile)
    def _(i):
        at = pl.ds(pl.multiple_of(i * tile, tile), tile)
        to = pl.ds(pl.multiple_of(first + i * tile, tile), tile)
        tok[0, to, :] = rms_scale(raw[at, :].astype(jnp.float32), gain_ref[...]).astype(jnp.bfloat16)

    pl.semaphore_wait(barrier, 5 + jnp.where(in_middle, 1, 0))

    def remote(ref, send, recv, where, to=None):
        return pltpu.make_async_remote_copy(
            ref, ref if to is None else to, send, recv, device_id=where, device_id_type=MESH
        )

    pieces = 2
    step_depth = depth // pieces

    def gu_at(s, b, h):
        return gu.at[b, pl.ds(pl.multiple_of(s * depth + h * step_depth, step_depth), step_depth)]

    def gu_send(kind, b, h):
        at = jnp.where(in_middle, pieces * blocks + b, pieces * b + h)
        return remote(gu_at(last if kind else k, b, h), gu_s.at[kind], gu_r.at[at], inner)

    def gu_pass(b, h):
        remote(gu_at(last, b, h), gu_s.at[1], gu_r.at[pieces * b + h], inner).wait_recv()
        gu_send(1, b, h).start()

    def gu_wait(b):
        remote(gu.at[b, pl.ds(0, 2 * depth)], gu_s.at[0], gu_r.at[pieces * blocks + b], inner).wait_recv()

    def dn_send(way, s, j):
        at = s * cuts + j
        return remote(dn.at[at], dn_s.at[way], dn_r.at[at], outer if way else inner)

    def dn_wait(s, j):
        at = s * cuts + j
        remote(dn.at[at], dn_s.at[0], dn_r.at[at], inner).wait_recv()

    def pass_down(way, s, j):
        dn_wait(s, j)
        dn_send(way, s, j).start()

    def rows_of(p, r_at, t_at, first, count, core):
        other = (t_at % 2 + core) % 2
        base = (r_at * 4 + other * 2 + t_at // 2) * rows
        return tok.at[p, pl.ds(base + first * piece, count * piece)]

    def z_send(i):
        return remote(rows_of(0, r, t, i, 1, c), z_s, z_r.at[i], inner, rows_of(1, r, t, i, 1, c))

    def z_wait(i):
        remote(rows_of(1, r, t, i, 1, c), z_s, z_r.at[i], inner).wait_recv()

    sends = (
        [((r, t, i, 1), along_x) for i in range(4)]
        + [((r, t, i, 1), along_y) for i in range(4)]
        + [((r, t_x, 0, 1), along_y), ((r, t_x, 1, 1), along_y), ((r_y, t, 2, 1), along_x), ((r_y, t, 3, 1), along_x)]
        + [((r_at, t_at, i, 2), partner) for r_at, t_at in ((r, t), (r, t_x), (r_y, t), (r_y, t_x)) for i in (0, 2)]
    )
    groups = (
        ((0, 1), (6, 7), (2, 3), (4, 5), (8, 9), (10, 11), (12, 13, 14, 15), (16, 17, 18, 19)),
        ((0, 4), (1, 5), (6,), (7,), (2, 3), (8, 9), (10, 11), (12, 13, 14, 15), (16, 17, 18, 19)),
    )

    def group_of(p, i):
        return [g for g, held in enumerate(groups[p]) if i in held][0]

    def go(p, *which):
        for i in which:
            at, where = sends[i]
            to = rows_of(p, *at, 1 - c if i >= 12 else c)
            remote(rows_of(p, *at, c), tok_s.at[p], tok_r.at[p, group_of(p, i)], where, to).start()

    def got(p, *which):
        g = group_of(p, which[0])
        assert groups[p][g] == which
        count = sum(1 if i < 12 else 2 for i in which) * piece
        remote(tok.at[p, pl.ds(0, count)], tok_s.at[p], tok_r.at[p, g], partner).wait_recv()

    quarter = 2 * rows
    halves = 4 * rows

    def half_rows(r_at):
        return pl.ds(pl.multiple_of(r_at * halves, halves), halves)

    def hid_at(p, b, r_at):
        return hid.at[p, half_rows(r_at), pl.ds(pl.multiple_of(b * lanes, lanes), lanes)]

    def hid_send(b, r_at):
        return remote(hid_at(1, b, r_at), hid_s, hid_r.at[r_at], outer, hid_at(0, b, r_at))

    def hid_wait(r_at):
        remote(hid.at[0, half_rows(r_at)], hid_s, hid_r.at[r_at], partner).wait_recv()

    def gated(p, b, r_at):
        both = jnp.dot(tok[p, half_rows(r_at), :], gu[b], preferred_element_type=jnp.float32)
        gate, up = both[:, :lanes], both[:, lanes:]
        hid_at(p, b, r_at)[...] = (gate / (1.0 + jnp.exp(-gate)) * up).astype(jnp.bfloat16)

    chunks = n * cuts
    mid = sub // 2
    here, there = 0, 1

    def pair_copy(p, side):
        return remote(pair_out.at[p, side], pair_s, pair_r.at[p, side], partner, pair_in.at[p, side])

    def half_copy(p, way):
        return remote(
            half_out.at[p, way], half_s, half_r.at[p], along_y if way else along_x, half_in.at[p, way]
        )

    def full_copy(p, way, part_at):
        return remote(
            full_out.at[p, way, part_at], full_s, full_r.at[p], along_y if way else along_x, full_in.at[p, way, part_at]
        )

    def source(i):
        near_or_last = jnp.where(i == 0, k, near + last - k)
        return jnp.where(i < 2, near_or_last, jnp.where(i == 2, far_near, far_last))

    def place(at):
        return jnp.where(at < chunks, source(at // cuts) * cuts + at % cuts, chunks)

    def product(at, side):
        p = place(at)
        held = jnp.where(at < chunks, p, far_last * cuts + cuts - 1)
        rows_at = half_rows(r_y if side == there else r)
        both = jnp.dot(hid[jnp.where(at < chunks, 0, 1), rows_at, :], dn[held], preferred_element_type=jnp.float32)
        pair_out[p, side] = both[quarter:].astype(jnp.bfloat16)
        pair_copy(p, side).start()
        kept[p, side] = both[:quarter]

    def send_own_gu():
        for b in range(blocks):
            pltpu.make_async_copy(gu.at[b, own_depth], gu.at[b, own_depth], gu_l.at[b]).wait()
            for h in range(pieces):
                gu_send(0, b, h).start()

    def send_own_dn(way):
        own = dn.at[pl.ds(k * cuts, cuts)]
        pltpu.make_async_copy(own, own, dn_l).wait()
        for j in range(cuts):
            dn_send(way, k, j).start()

    @pl.when(in_middle)
    def _():
        send_own_gu()
        send_own_dn(1)

    @pl.when(at_end)
    def _():
        for i in range(4):
            z_send(i).start()
        send_own_gu()
        send_own_dn(0)

    @pl.when(in_middle)
    def _():
        @pl.loop(0, 12)
        def _(at_step):
            def step(at):
                return pl.when(at_step == at)

            @step(0)
            def _():
                go(0, 0, 1, 6, 7, 12, 13)
                z_wait(0)
                go(1, 0, 4)
                got(0, 0, 1)
                go(0, 14)
                got(0, 6, 7)
                go(0, 17)
                z_wait(1)
                go(1, 1, 5, 12)
                got(1, 0, 4)
                z_wait(2)
                go(1, 2, 6)
                got(1, 1, 5)
                go(1, 14, 16)
                z_wait(3)
                go(1, 13, 3, 7, 8, 9)
                got(1, 6)
                go(1, 10)
                gu_pass(0, 0)
                got(1, 7)
                go(1, 17, 11)
                got(1, 2, 3)
                go(1, 15)
                gu_pass(0, 1)
                go(0, 2, 4)
                gu_pass(1, 0)
                go(0, 3, 5)
                got(1, 8, 9)
                go(1, 18)
                got(1, 10, 11)
                go(1, 19)
                go(0, 8, 10)
                gu_pass(1, 1)
                got(1, 12, 13, 14, 15)
                gu_wait(0)

            @step(1)
            def _():
                got(1, 16, 17, 18, 19)

            @pl.when(at_step == 2 - c)
            def _():
                gu_pass(2, 0)

            @step(2)
            def _():
                go(0, 9, 11)
                got(0, 2, 3)
                go(0, 15)
                got(0, 4, 5)
                go(0, 16)
                gu_pass(2, 1)

            @pl.when(at_step == 2 + 4 * c)
            def _():
                for j in range(cuts):
                    dn_send(0, k, j).start()

            @step(2)
            def _():
                gu_wait(1)

            @step(4)
            def _():
                got(0, 12, 13, 14, 15)

            @step(6)
            def _():
                pass_down(0, last, 0)
                got(0, 8, 9)
                go(0, 18)
                got(0, 10, 11)
                go(0, 19)
                gu_wait(2)

            @step(8)
            def _():
                got(0, 16, 17, 18, 19)

            @step(11)
            def _():
                pl.loop(0, 2)(lambda at: product(at, there))
                pass_down(0, last, 1)

            passed = (at_step < 4) | (at_step == 6) | (at_step == 7)
            late = jnp.where(at_step < 8, 2, jnp.where(at_step < 11, at_step - 8, 2))
            b = jnp.where(at_step < 4, at_step // 2, jnp.where(at_step < 6, at_step - 4, late))
            first_r = jnp.where(at_step < 2, r, r_y)
            own_r = jnp.where((at_step < 6) | (at_step == 11), r, r_y)
            r_at = jnp.where(passed, (first_r + at_step % 2) % 2, own_r)
            gated(jnp.where(passed, 1, 0), b, r_at)

            @pl.when(passed)
            def _():
                hid_send(b, r_at).start()

    def of(m):
        return pl.ds(pl.multiple_of(m * rows, rows), rows)

    def summed(p, side, x_at):
        return kept[p, side, of(x_at), :] + pair_in[p, side, of(x_at), :].astype(jnp.float32)

    def finish_there(at):
        p = place(at)
        pair_copy(p, there).wait_recv()
        across = summed(p, there, 1 - x).astype(jnp.bfloat16)
        half_out[p, 0] = across[:, :mid]
        half_out[p, 1] = across[:, mid:]
        half_copy(p, 0).start()
        half_copy(p, 1).start()
        value = summed(p, there, x)
        kept[p, there, of(x), :mid] = value[:, :mid]
        full_out[p, 1, 1] = value[:, mid:].astype(jnp.bfloat16)
        full_copy(p, 1, 1).start()

    def finish_here(at):
        p = place(at)
        pair_copy(p, here).wait_recv()
        value = summed(p, here, 1 - x)
        kept[p, here, of(1 - x), mid:] = value[:, mid:]
        full_out[p, 0, 0] = value[:, :mid].astype(jnp.bfloat16)
        full_copy(p, 0, 0).start()
        fin[p] = summed(p, here, x)

    across_copy = remote(diag_out, diag_s, diag_r, diag, diag_in)

    def finish_direct(at):
        p = place(at)
        pair_copy(p, there).wait_recv()
        diag_out[...] = summed(p, there, 1 - x).astype(jnp.bfloat16)
        across_copy.start()
        value = summed(p, there, x).astype(jnp.bfloat16)
        for part_at in (1, 0):
            full_out[p, 1, part_at] = value[:, part_at * mid : (part_at + 1) * mid]
            full_copy(p, 1, part_at).start()
        pair_copy(p, here).wait_recv()
        value = summed(p, here, 1 - x).astype(jnp.bfloat16)
        for part_at in (0, 1):
            full_out[p, 0, part_at] = value[:, part_at * mid : (part_at + 1) * mid]
            full_copy(p, 0, part_at).start()
        fin[p] = summed(p, here, x)

    def finish_half(at):
        p = place(at)
        remote(half_in.at[p], half_s, half_r.at[p], partner).wait_recv()
        full_out[p, 0, 1] = (kept[p, here, of(1 - x), mid:] + half_in[p, 1].astype(jnp.float32)).astype(jnp.bfloat16)
        full_copy(p, 0, 1).start()
        full_out[p, 1, 0] = (kept[p, there, of(x), :mid] + half_in[p, 0].astype(jnp.float32)).astype(jnp.bfloat16)
        full_copy(p, 1, 0).start()

    early = 2 * cuts

    @pl.when(at_end)
    def _():
        for j in range(cuts):
            dn_wait(near, j)
        hid_wait(r_y)

    @pl.loop(0, early)
    def _(at):
        @pl.when(at_end | (at > 1))
        def _():
            product(at, there)

        @pl.when(at > 0)
        def _():
            finish_there(at - 1)

        @pl.when(in_middle & (at == 0))
        def _():
            pass_down(1, far_near, 0)

    @pl.when(at_end)
    def _():
        hid_wait(r)

    @pl.loop(0, early)
    def _(at):
        product(at, here)

        @pl.when(at == 0)
        def _():
            finish_there(early - 1)

        @pl.when(at > 0)
        def _():
            finish_here(at - 1)
            finish_half(at - 1)

        @pl.when(in_middle & (at == 2))
        def _():
            pass_down(1, far_near, 1)


    def order(i):
        return jnp.where(in_middle & (i >= 2), jnp.where(i == 2, chunks, early + i - 1), early + i)

    @pl.loop(0, chunks - early + 1)
    def _(i):
        at = order(i)

        @pl.when(at_end & (i < 3))
        def _():
            dn_wait(source(at // cuts), at % cuts)

        @pl.when(in_middle & (i == 0))
        def _():
            pass_down(1, far_last, 0)

        @pl.when(in_middle & (i == 2))
        def _():
            dn_wait(far_last, cuts - 1)

        @pl.when(in_middle | (i < 3))
        def _():
            product(at, there)
            product(at, here)

        @pl.when(i == 0)
        def _():
            finish_here(early - 1)
            finish_half(early - 1)

        @pl.when(in_middle | (i < 2))
        def _():
            finish_there(at)
            finish_here(at)

        @pl.when(at_end & (i == 2))
        def _():
            finish_direct(at)

        @pl.when((i > 0) & (in_middle | (i < 3)))
        def _():
            finish_half(order(i - 1))

    result = remote(res_out, res_s, res_r, outer, res_in)

    def collect(at, part_at):
        p = place(at)
        cols = pl.ds(part_at * mid, mid)
        both = full_in[p, 0, part_at].astype(jnp.float32) + full_in[p, 1, part_at].astype(jnp.float32)
        return fin[p, :, cols] + both

    def arrive(at):
        remote(full_in.at[place(at)], full_s, full_r.at[place(at)], along_x).wait_recv()

    @pl.when(in_middle)
    def _():
        arrive(chunks)
        for part_at in (0, 1):
            res_out[:, pl.ds(part_at * mid, mid)] = collect(chunks, part_at).astype(jnp.bfloat16)
        result.start()
        finish_half(chunks - 1)

    remote(gu.at[:, pl.ds(0, depth)], gu_s.at[0], gu_r.at[0], inner).wait_send()

    @pl.when(at_end)
    def _():
        remote(tok.at[0, pl.ds(0, rows)], z_s, z_r.at[0], inner).wait_send()
        remote(dn.at[pl.ds(0, cuts)], dn_s.at[0], dn_r.at[0], inner).wait_send()
        remote(pair_out.at[pl.ds(0, chunks - 1)], pair_s, pair_r.at[0, 0], partner).wait_send()
        remote(half_out.at[pl.ds(0, chunks - 2)], half_s, half_r.at[0], along_x).wait_send()
        across_copy.wait_send()

    @pl.when(in_middle)
    def _():
        for p in (0, 1):
            total = sum(1 if i < 12 else 2 for i in range(len(sends))) * piece
            remote(tok.at[p, pl.ds(0, total)], tok_s.at[p], tok_r.at[p, 0], partner).wait_send()
        remote(gu.at[:, pl.ds(0, depth)], gu_s.at[1], gu_r.at[0], inner).wait_send()
        remote(hid.at[1], hid_s, hid_r.at[0], outer).wait_send()
        remote(dn.at[pl.ds(0, 2 * cuts)], dn_s.at[0], dn_r.at[0], inner).wait_send()
        remote(dn.at[pl.ds(0, 3 * cuts - 1)], dn_s.at[1], dn_r.at[0], outer).wait_send()
        remote(pair_out, pair_s, pair_r.at[0, 0], partner).wait_send()
        remote(half_out, half_s, half_r.at[0], along_x).wait_send()

    squares[...] = jnp.zeros_like(squares)

    def settle(at, part_at, total):
        fin[place(at), :, pl.ds(part_at * mid, mid)] = total
        squares[...] += total * total

    @pl.loop(0, chunks)
    def _(at):
        @pl.when(in_middle | (at < chunks - 2))
        def _():
            arrive(at)
            for part_at in (0, 1):
                settle(at, part_at, collect(at, part_at))

    @pl.when(at_end)
    def _():
        across_copy.wait_recv()
        p = place(chunks - 2)
        for part_at in (0, 1):
            cols = pl.ds(part_at * mid, mid)
            fin[p, :, cols] = fin[p, :, cols] + diag_in[:, cols].astype(jnp.float32)
        arrive(chunks - 2)
        for part_at in (0, 1):
            settle(chunks - 2, part_at, collect(chunks - 2, part_at))
        result.wait_recv()
        for part_at in (0, 1):
            settle(chunks - 1, part_at, res_in[:, pl.ds(part_at * mid, mid)].astype(jnp.float32))

    scale = lax.rsqrt(jnp.sum(squares[...], axis=-1, keepdims=True) / (n * width) + EPS)
    for p in range(chunks):
        cols = pl.ds(p * sub, sub)
        out_ref[:, cols] = (fin[p] * scale * post_ref[:, cols]).astype(out_ref.dtype)

    @pl.when(at_end)
    def _():
        remote(full_out.at[pl.ds(0, chunks - 1)], full_s, full_r.at[0], along_x).wait_send()

    @pl.when(in_middle)
    def _():
        remote(full_out, full_s, full_r.at[0], along_x).wait_send()
        result.wait_send()


def chain_body(n, tokens, norm_gain, w_gate, w_up, w_down, post_gain):
    rows, model = tokens.shape
    depth, block = w_gate.shape
    width = w_down.shape[1]
    part = block // 2
    cuts = width // PIECE
    sub = width // cuts
    blocks = part // LANES
    chunks = n * cuts
    vmem, dma = pltpu.VMEM, pltpu.SemaphoreType.DMA
    low, full = jnp.bfloat16, jnp.float32
    anywhere = pl.BlockSpec(memory_space=pl.ANY)
    inside = pl.BlockSpec(memory_space=vmem)
    return pl.pallas_call(
        functools.partial(kernel, n, rows, depth, part, width, cuts, LANES),
        out_shape=pltpu.VMEM((rows, model), low),
        in_specs=[anywhere, inside, anywhere, anywhere, anywhere, inside],
        out_specs=inside,
        scratch_shapes=[
            vmem((rows, model), low),
            vmem((2, 8 * rows, model), low),
            vmem((blocks, n * depth, 2 * LANES), low),
            vmem((chunks, part, sub), low),
            vmem((2, 8 * rows, part), low),
            vmem((chunks + 1, 2, 2 * rows, sub), full),
            vmem((chunks + 1, 2, 2 * rows, sub), low),
            vmem((chunks + 1, 2, 2 * rows, sub), low),
            vmem((chunks + 1, 2, rows, sub // 2), low),
            vmem((chunks + 1, 2, rows, sub // 2), low),
            vmem((chunks + 1, 2, 2, rows, sub // 2), low),
            vmem((chunks + 1, 2, 2, rows, sub // 2), low),
            vmem((chunks + 1, rows, sub), full),
            vmem((rows, sub), low),
            vmem((rows, sub), low),
            vmem((rows, sub), low),
            vmem((rows, sub), low),
            vmem((rows, sub // 2), full),
            dma(()),
            dma((blocks,)),
            dma(()),
            dma(()),
            dma((4,)),
            dma((2,)),
            dma((2, 9)),
            dma((2,)),
            dma((3 * blocks,)),
            dma((2,)),
            dma((chunks,)),
            dma(()),
            dma((2,)),
            dma(()),
            dma((chunks + 1, 2)),
            dma(()),
            dma((chunks + 1,)),
            dma(()),
            dma((chunks + 1,)),
            dma(()),
            dma(()),
            dma(()),
            dma(()),
        ],
        compiler_params=pltpu.CompilerParams(
            collective_id=0, has_side_effects=True, vmem_limit_bytes=56 * 2**20
        ),
    )(tokens, norm_gain.reshape(1, -1), w_gate, w_up, w_down, post_gain.reshape(1, -1))


def solution(mesh):
    n = mesh.shape["fs"]

    def body(tokens, norm_gain, w_gate, w_up, w_down, post_gain):
        args = (tokens, norm_gain, w_gate, w_up, w_down, post_gain)
        rows = tokens.shape[0]
        fits = (
            mesh.shape["rep"] == 2 and mesh.shape["tp"] == 4 and n == 4 and rows <= 128 and rows % 128 == 0
            and w_gate.shape[1] == 6 * LANES and w_down.shape[1] == 2 * PIECE
        )
        return chain_body(n, *args) if fits else plain_body(*args)

    return jax.shard_map(
        body,
        mesh=mesh,
        in_specs=(
            P(("rep", "fs", "tp"), None),
            P(),
            P("fs", "tp"),
            P("fs", "tp"),
            P("tp", "fs"),
            P(),
        ),
        out_specs=P(("rep", "fs", "tp"), None),
        check_vma=False,
    )
```

```python
import functools

import jax
import jax.numpy as jnp
from jax import lax
from jax.experimental import pallas as pl
from jax.experimental.pallas import tpu as pltpu
from jax.sharding import PartitionSpec as P

EPS = 1e-06
MESH = pl.DeviceIdType.MESH
PIECE = 256
LANES = 128


def rms_scale(values, gain):
    return values * lax.rsqrt(jnp.mean(values * values, axis=-1, keepdims=True) + EPS) * gain


def plain_body(tokens, norm_gain, w_gate, w_up, w_down, post_gain):
    own_normed = rms_scale(tokens.astype(jnp.float32), norm_gain).astype(jnp.bfloat16)
    normed = lax.all_gather(own_normed, "tp", axis=0, tiled=True)
    gate = jnp.dot(
        normed, lax.all_gather(w_gate, "fs", axis=0, tiled=True), preferred_element_type=jnp.float32
    )
    up = jnp.dot(
        normed, lax.all_gather(w_up, "fs", axis=0, tiled=True), preferred_element_type=jnp.float32
    )
    hidden = (jax.nn.silu(gate) * up).astype(jnp.bfloat16)
    terms = jnp.dot(
        hidden, lax.all_gather(w_down, "fs", axis=1, tiled=True), preferred_element_type=jnp.float32
    )
    summed = lax.psum_scatter(
        terms.astype(jnp.bfloat16), "tp", scatter_dimension=0, tiled=True
    ).astype(jnp.float32)
    return rms_scale(summed, post_gain).astype(jnp.bfloat16)


def kernel(
    n, rows, depth, part, width, cuts, lanes,
    tok_ref, gain_ref, wg_ref, wu_ref, wd_ref, post_ref, out_ref,
    raw, tok, gu, dn, hid, kept, pair_out, pair_in, half_out, half_in, full_out, full_in, fin, res_out, res_in, diag_out, diag_in, squares,
    tok_l, gu_l, dn_l, z_s, z_r, tok_s, tok_r, gu_s, gu_r, dn_s, dn_r, hid_s, hid_r,
    pair_s, pair_r, half_s, half_r, full_s, full_r, res_s, res_r, diag_s, diag_r,
):
    r, k, t = lax.axis_index("rep"), lax.axis_index("fs"), lax.axis_index("tp")
    x, c = t // 2, t % 2
    t_pair, t_x, r_y = x * 2 + (1 - c), (1 - x) * 2 + c, 1 - r
    t_px = (1 - x) * 2 + (1 - c)
    partner, along_x, along_y, diag = {"tp": t_pair}, {"tp": t_x}, {"rep": r_y}, {"rep": r_y, "tp": t_x}
    left = k < n // 2
    last = jnp.where(left, 0, n - 1)
    near = jnp.where(left, 1, n - 2)
    far_near, far_last = n - 1 - near, n - 1 - last
    at_end = k == last
    in_middle = k != last
    inner, outer = {"fs": jnp.where(left, k + 1, k - 1)}, {"fs": last}
    blocks = part // lanes
    sub = width // cuts
    half = pl.multiple_of(r * part, part)
    piece = rows // 4
    own_depth = pl.ds(pl.multiple_of(k * depth, depth), depth)

    def gu_load(b, q):
        ref = (wg_ref, wu_ref)[q]
        return pltpu.make_async_copy(
            ref.at[:, pl.ds(half + b * lanes, lanes)], gu.at[b, own_depth, pl.ds(q * lanes, lanes)], gu_l.at[b]
        )

    def dn_load(j):
        return pltpu.make_async_copy(wd_ref.at[pl.ds(half, part), pl.ds(j * sub, sub)], dn.at[k * cuts + j], dn_l)

    tok_load = pltpu.make_async_copy(tok_ref, raw, tok_l)

    tok_load.start()
    for b in range(blocks):
        for q in (0, 1):
            gu_load(b, q).start()
    for j in range(cuts):
        dn_load(j).start()

    barrier = pltpu.get_barrier_semaphore()
    for where in (partner, along_x, along_y, diag, inner):
        pl.semaphore_signal(barrier, inc=1, device_id=where, device_id_type=MESH)

    @pl.when(in_middle)
    def _():
        pl.semaphore_signal(barrier, inc=1, device_id=outer, device_id_type=MESH)

    tok_load.wait()
    tile = 32
    first = (r * 4 + x) * rows

    @pl.loop(0, rows // tile)
    def _(i):
        at = pl.ds(pl.multiple_of(i * tile, tile), tile)
        to = pl.ds(pl.multiple_of(first + i * tile, tile), tile)
        tok[0, to, :] = rms_scale(raw[at, :].astype(jnp.float32), gain_ref[...]).astype(jnp.bfloat16)

    pl.semaphore_wait(barrier, 5 + jnp.where(in_middle, 1, 0))

    def remote(ref, send, recv, where, to=None):
        return pltpu.make_async_remote_copy(
            ref, ref if to is None else to, send, recv, device_id=where, device_id_type=MESH
        )

    pieces = 2
    step_depth = depth // pieces

    def gu_at(s, b, h):
        return gu.at[b, pl.ds(pl.multiple_of(s * depth + h * step_depth, step_depth), step_depth)]

    def gu_send(kind, b, h):
        at = jnp.where(in_middle, pieces * blocks + b, pieces * b + h)
        return remote(gu_at(last if kind else k, b, h), gu_s.at[kind], gu_r.at[at], inner)

    def gu_pass(b, h):
        remote(gu_at(last, b, h), gu_s.at[1], gu_r.at[pieces * b + h], inner).wait_recv()
        gu_send(1, b, h).start()

    def gu_wait(b):
        remote(gu.at[b, pl.ds(0, 2 * depth)], gu_s.at[0], gu_r.at[pieces * blocks + b], inner).wait_recv()

    def dn_send(way, s, j):
        at = s * cuts + j
        return remote(dn.at[at], dn_s.at[way], dn_r.at[at], outer if way else inner)

    def dn_wait(s, j):
        at = s * cuts + j
        remote(dn.at[at], dn_s.at[0], dn_r.at[at], inner).wait_recv()

    def pass_down(way, s, j):
        dn_wait(s, j)
        dn_send(way, s, j).start()

    def rows_of(p, r_at, t_at, first, count, core):
        other = (t_at % 2 + core) % 2
        base = (r_at * 4 + other * 2 + t_at // 2) * rows
        return tok.at[p, pl.ds(base + first * piece, count * piece)]

    def z_send(i):
        return remote(rows_of(0, r, t, i, 1, c), z_s, z_r.at[i], inner, rows_of(1, r, t, i, 1, c))

    def z_wait(i):
        remote(rows_of(1, r, t, i, 1, c), z_s, z_r.at[i], inner).wait_recv()

    sends = (
        [((r, t, i, 1), along_x) for i in range(4)]
        + [((r, t, i, 1), along_y) for i in range(4)]
        + [((r, t_x, 0, 1), along_y), ((r, t_x, 1, 1), along_y), ((r_y, t, 2, 1), along_x), ((r_y, t, 3, 1), along_x)]
        + [((r_at, t_at, i, 2), partner) for r_at, t_at in ((r, t), (r, t_x), (r_y, t), (r_y, t_x)) for i in (0, 2)]
    )
    groups = (
        ((0, 1), (6, 7), (2, 3), (4, 5), (8, 9), (10, 11), (12, 13, 14, 15), (16, 17, 18, 19)),
        ((0, 4), (1, 5), (6,), (7,), (2, 3), (8, 9), (10, 11), (12, 13, 14, 15), (16, 17, 18, 19)),
    )

    def group_of(p, i):
        return [g for g, held in enumerate(groups[p]) if i in held][0]

    def go(p, *which):
        for i in which:
            at, where = sends[i]
            to = rows_of(p, *at, 1 - c if i >= 12 else c)
            remote(rows_of(p, *at, c), tok_s.at[p], tok_r.at[p, group_of(p, i)], where, to).start()

    def got(p, *which):
        g = group_of(p, which[0])
        assert groups[p][g] == which
        count = sum(1 if i < 12 else 2 for i in which) * piece
        remote(tok.at[p, pl.ds(0, count)], tok_s.at[p], tok_r.at[p, g], partner).wait_recv()

    quarter = 2 * rows
    halves = 4 * rows

    def half_rows(r_at):
        return pl.ds(pl.multiple_of(r_at * halves, halves), halves)

    def hid_at(p, b, r_at):
        return hid.at[p, half_rows(r_at), pl.ds(pl.multiple_of(b * lanes, lanes), lanes)]

    def hid_send(b, r_at):
        sem = jnp.where((b == 0) & (r_at == r), 2, r_at)
        return remote(hid_at(1, b, r_at), hid_s, hid_r.at[sem], outer, hid_at(0, b, r_at))

    def hid_wait(r_at, first, count, sem):
        held = hid.at[0, half_rows(r_at), pl.ds(first * lanes, count * lanes)]
        remote(held, hid_s, hid_r.at[sem], partner).wait_recv()

    def gated(p, b, r_at):
        both = jnp.dot(tok[p, half_rows(r_at), :], gu[b], preferred_element_type=jnp.float32)
        gate, up = both[:, :lanes], both[:, lanes:]
        hid_at(p, b, r_at)[...] = (gate / (1.0 + jnp.exp(-gate)) * up).astype(jnp.bfloat16)

    chunks = n * cuts
    mid = sub // 2
    here, there = 0, 1

    def pair_copy(p, side):
        return remote(pair_out.at[p, side], pair_s, pair_r.at[p, side], partner, pair_in.at[p, side])

    def half_copy(p, way):
        return remote(
            half_out.at[p, way], half_s, half_r.at[p], along_y if way else along_x, half_in.at[p, way]
        )

    def full_copy(p, way, part_at):
        return remote(
            full_out.at[p, way, part_at], full_s, full_r.at[p], along_y if way else along_x, full_in.at[p, way, part_at]
        )

    def source(i):
        near_or_last = jnp.where(i == 0, k, near + last - k)
        return jnp.where(i < 2, near_or_last, jnp.where(i == 2, far_near, far_last))

    def place(at):
        return jnp.where(at < chunks, source(at // cuts) * cuts + at % cuts, chunks)

    def product(at, side):
        p = place(at)
        held = jnp.where(at < chunks, p, far_last * cuts + cuts - 1)
        rows_at = half_rows(r_y if side == there else r)
        both = jnp.dot(hid[jnp.where(at < chunks, 0, 1), rows_at, :], dn[held], preferred_element_type=jnp.float32)
        pair_out[p, side] = both[quarter:].astype(jnp.bfloat16)
        pair_copy(p, side).start()
        kept[p, side] = both[:quarter]

    def send_own_gu():
        for b in range(blocks):
            pltpu.make_async_copy(gu.at[b, own_depth], gu.at[b, own_depth], gu_l.at[b]).wait()
            for h in range(pieces):
                gu_send(0, b, h).start()

    def send_own_dn(way):
        own = dn.at[pl.ds(k * cuts, cuts)]
        pltpu.make_async_copy(own, own, dn_l).wait()
        for j in range(cuts):
            dn_send(way, k, j).start()

    @pl.when(in_middle)
    def _():
        send_own_gu()
        send_own_dn(1)

    @pl.when(at_end)
    def _():
        for i in range(4):
            z_send(i).start()
        send_own_gu()
        hid_wait(r, 0, 1, 2)
        send_own_dn(0)

    @pl.when(in_middle)
    def _():
        @pl.loop(0, 12)
        def _(at_step):
            def step(at):
                return pl.when(at_step == at)

            @step(0)
            def _():
                go(0, 0, 1, 6, 7, 12, 13)
                z_wait(0)
                go(1, 0, 4)
                got(0, 0, 1)
                go(0, 14)
                got(0, 6, 7)
                go(0, 17)
                z_wait(1)
                go(1, 1, 5, 12)
                got(1, 0, 4)
                z_wait(2)
                go(1, 2, 6)
                got(1, 1, 5)
                go(1, 14, 16)
                z_wait(3)
                go(1, 13, 3, 7, 8, 9)
                got(1, 6)
                go(1, 10)
                gu_pass(0, 0)
                got(1, 7)
                go(1, 17, 11)
                got(1, 2, 3)
                go(1, 15)
                gu_pass(0, 1)
                go(0, 2, 4)
                gu_pass(1, 0)
                go(0, 3, 5)
                got(1, 8, 9)
                go(1, 18)
                got(1, 10, 11)
                go(1, 19)
                go(0, 8, 10)
                gu_pass(1, 1)
                got(1, 12, 13, 14, 15)
                gu_wait(0)

            @step(1)
            def _():
                got(1, 16, 17, 18, 19)

            @pl.when(at_step == 2 - c)
            def _():
                gu_pass(2, 0)

            @step(2)
            def _():
                go(0, 9, 11)
                got(0, 2, 3)
                go(0, 15)
                got(0, 4, 5)
                go(0, 16)
                gu_pass(2, 1)

            @pl.when(at_step == 2 + 4 * c)
            def _():
                for j in range(cuts):
                    dn_send(0, k, j).start()

            @step(2)
            def _():
                gu_wait(1)

            @step(4)
            def _():
                got(0, 12, 13, 14, 15)

            @step(6)
            def _():
                got(0, 8, 9)
                go(0, 18)
                got(0, 10, 11)
                go(0, 19)
                gu_wait(2)

            @step(8)
            def _():
                got(0, 16, 17, 18, 19)

            @step(10)
            def _():
                pass_down(0, last, 0)

            @step(11)
            def _():
                pl.loop(0, 2)(lambda at: product(at, there))
                pass_down(0, last, 1)

            passed = (at_step < 4) | (at_step == 6) | (at_step == 7)
            late = jnp.where(at_step < 8, 2, jnp.where(at_step < 11, at_step - 8, 2))
            b = jnp.where(at_step < 4, at_step // 2, jnp.where(at_step < 6, at_step - 4, late))
            first_r = jnp.where(at_step < 2, r, r_y)
            own_r = jnp.where((at_step < 6) | (at_step == 11), r, r_y)
            r_at = jnp.where(passed, (first_r + at_step % 2) % 2, own_r)
            gated(jnp.where(passed, 1, 0), b, r_at)

            @pl.when(passed)
            def _():
                hid_send(b, r_at).start()

    def of(m):
        return pl.ds(pl.multiple_of(m * rows, rows), rows)

    def summed(p, side, x_at):
        return kept[p, side, of(x_at), :] + pair_in[p, side, of(x_at), :].astype(jnp.float32)

    def finish_there(at):
        p = place(at)
        pair_copy(p, there).wait_recv()
        across = summed(p, there, 1 - x).astype(jnp.bfloat16)
        half_out[p, 0] = across[:, :mid]
        half_out[p, 1] = across[:, mid:]
        half_copy(p, 0).start()
        half_copy(p, 1).start()
        value = summed(p, there, x)
        kept[p, there, of(x), :mid] = value[:, :mid]
        full_out[p, 1, 1] = value[:, mid:].astype(jnp.bfloat16)
        full_copy(p, 1, 1).start()

    def finish_here(at):
        p = place(at)
        pair_copy(p, here).wait_recv()
        value = summed(p, here, 1 - x)
        kept[p, here, of(1 - x), mid:] = value[:, mid:]
        full_out[p, 0, 0] = value[:, :mid].astype(jnp.bfloat16)
        full_copy(p, 0, 0).start()
        fin[p] = summed(p, here, x)

    across_copy = remote(diag_out, diag_s, diag_r, diag, diag_in)

    def finish_direct(at):
        p = place(at)
        pair_copy(p, there).wait_recv()
        diag_out[...] = summed(p, there, 1 - x).astype(jnp.bfloat16)
        across_copy.start()
        value = summed(p, there, x).astype(jnp.bfloat16)
        for part_at in (1, 0):
            full_out[p, 1, part_at] = value[:, part_at * mid : (part_at + 1) * mid]
            full_copy(p, 1, part_at).start()
        pair_copy(p, here).wait_recv()
        value = summed(p, here, 1 - x).astype(jnp.bfloat16)
        for part_at in (0, 1):
            full_out[p, 0, part_at] = value[:, part_at * mid : (part_at + 1) * mid]
            full_copy(p, 0, part_at).start()
        fin[p] = summed(p, here, x)

    def finish_half(at):
        p = place(at)
        remote(half_in.at[p], half_s, half_r.at[p], partner).wait_recv()
        full_out[p, 0, 1] = (kept[p, here, of(1 - x), mid:] + half_in[p, 1].astype(jnp.float32)).astype(jnp.bfloat16)
        full_copy(p, 0, 1).start()
        full_out[p, 1, 0] = (kept[p, there, of(x), :mid] + half_in[p, 0].astype(jnp.float32)).astype(jnp.bfloat16)
        full_copy(p, 1, 0).start()

    early = 2 * cuts

    @pl.when(at_end)
    def _():
        for j in range(cuts):
            dn_wait(near, j)
        hid_wait(r_y, 0, blocks, r_y)

    @pl.loop(0, early)
    def _(at):
        @pl.when(at_end | (at > 1))
        def _():
            product(at, there)

        @pl.when(at > 0)
        def _():
            finish_there(at - 1)

        @pl.when(in_middle & (at == 0))
        def _():
            pass_down(1, far_near, 0)

    @pl.when(at_end)
    def _():
        hid_wait(r, 1, blocks - 1, r)

    @pl.loop(0, early)
    def _(at):
        product(at, here)

        @pl.when(at == 0)
        def _():
            finish_there(early - 1)

        @pl.when(at > 0)
        def _():
            finish_here(at - 1)
            finish_half(at - 1)

        @pl.when(in_middle & (at == 2))
        def _():
            pass_down(1, far_near, 1)


    result = remote(res_out, res_s, res_r, outer, res_in)

    def collect(at, part_at):
        p = place(at)
        cols = pl.ds(part_at * mid, mid)
        both = full_in[p, 0, part_at].astype(jnp.float32) + full_in[p, 1, part_at].astype(jnp.float32)
        return fin[p, :, cols] + both

    def arrive(at):
        remote(full_in.at[place(at)], full_s, full_r.at[place(at)], along_x).wait_recv()

    def order(i):
        return jnp.where(in_middle & (i >= 2), jnp.where(i == 2, chunks, early + i - 1), early + i)

    @pl.loop(0, chunks - early + 1)
    def _(i):
        at = order(i)

        @pl.when(at_end & (i < 3))
        def _():
            dn_wait(source(at // cuts), at % cuts)

        @pl.when(in_middle & (i == 1 * c))
        def _():
            pass_down(1, far_last, 0)

        @pl.when(in_middle & (i == 2))
        def _():
            dn_wait(far_last, cuts - 1)

        @pl.when(in_middle | (i < 3))
        def _():
            product(at, there)
            product(at, here)

        @pl.when(i == 0)
        def _():
            finish_here(early - 1)
            finish_half(early - 1)

        @pl.when(in_middle & (i == 3))
        def _():
            finish_half(chunks)

        @pl.when(in_middle | (i < 2))
        def _():
            finish_there(at)
            finish_here(at)

        @pl.when(at_end & (i == 2))
        def _():
            finish_direct(at)

        @pl.when(in_middle & (i == 4))
        def _():
            arrive(chunks)
            for part_at in (0, 1):
                res_out[:, pl.ds(part_at * mid, mid)] = collect(chunks, part_at).astype(jnp.bfloat16)
            result.start()

        @pl.when((i > 0) & (i != 3) & (in_middle | (i < 3)))
        def _():
            finish_half(order(i - 1))

    @pl.when(in_middle)
    def _():
        finish_half(chunks - 1)

    remote(gu.at[:, pl.ds(0, depth)], gu_s.at[0], gu_r.at[0], inner).wait_send()

    @pl.when(at_end)
    def _():
        remote(tok.at[0, pl.ds(0, rows)], z_s, z_r.at[0], inner).wait_send()
        remote(dn.at[pl.ds(0, cuts)], dn_s.at[0], dn_r.at[0], inner).wait_send()
        remote(pair_out.at[pl.ds(0, chunks - 1)], pair_s, pair_r.at[0, 0], partner).wait_send()
        remote(half_out.at[pl.ds(0, chunks - 2)], half_s, half_r.at[0], along_x).wait_send()
        across_copy.wait_send()

    @pl.when(in_middle)
    def _():
        for p in (0, 1):
            total = sum(1 if i < 12 else 2 for i in range(len(sends))) * piece
            remote(tok.at[p, pl.ds(0, total)], tok_s.at[p], tok_r.at[p, 0], partner).wait_send()
        remote(gu.at[:, pl.ds(0, depth)], gu_s.at[1], gu_r.at[0], inner).wait_send()
        remote(hid.at[1], hid_s, hid_r.at[0], outer).wait_send()
        remote(dn.at[pl.ds(0, 2 * cuts)], dn_s.at[0], dn_r.at[0], inner).wait_send()
        remote(dn.at[pl.ds(0, 3 * cuts - 1)], dn_s.at[1], dn_r.at[0], outer).wait_send()
        remote(pair_out, pair_s, pair_r.at[0, 0], partner).wait_send()
        remote(half_out, half_s, half_r.at[0], along_x).wait_send()

    squares[...] = jnp.zeros_like(squares)

    def settle(at, part_at, total):
        fin[place(at), :, pl.ds(part_at * mid, mid)] = total
        squares[...] += total * total

    @pl.loop(0, chunks)
    def _(at):
        @pl.when(in_middle | (at < chunks - 2))
        def _():
            arrive(at)
            for part_at in (0, 1):
                settle(at, part_at, collect(at, part_at))

    @pl.when(at_end)
    def _():
        across_copy.wait_recv()
        p = place(chunks - 2)
        for part_at in (0, 1):
            cols = pl.ds(part_at * mid, mid)
            fin[p, :, cols] = fin[p, :, cols] + diag_in[:, cols].astype(jnp.float32)
        arrive(chunks - 2)
        for part_at in (0, 1):
            settle(chunks - 2, part_at, collect(chunks - 2, part_at))
        result.wait_recv()
        for part_at in (0, 1):
            settle(chunks - 1, part_at, res_in[:, pl.ds(part_at * mid, mid)].astype(jnp.float32))

    scale = lax.rsqrt(jnp.sum(squares[...], axis=-1, keepdims=True) / (n * width) + EPS)
    for p in range(chunks):
        cols = pl.ds(p * sub, sub)
        out_ref[:, cols] = (fin[p] * scale * post_ref[:, cols]).astype(out_ref.dtype)

    @pl.when(at_end)
    def _():
        remote(full_out.at[pl.ds(0, chunks - 1)], full_s, full_r.at[0], along_x).wait_send()

    @pl.when(in_middle)
    def _():
        remote(full_out, full_s, full_r.at[0], along_x).wait_send()
        result.wait_send()


def chain_body(n, tokens, norm_gain, w_gate, w_up, w_down, post_gain):
    rows, model = tokens.shape
    depth, block = w_gate.shape
    width = w_down.shape[1]
    part = block // 2
    cuts = width // PIECE
    sub = width // cuts
    blocks = part // LANES
    chunks = n * cuts
    vmem, dma = pltpu.VMEM, pltpu.SemaphoreType.DMA
    low, full = jnp.bfloat16, jnp.float32
    anywhere = pl.BlockSpec(memory_space=pl.ANY)
    inside = pl.BlockSpec(memory_space=vmem)
    return pl.pallas_call(
        functools.partial(kernel, n, rows, depth, part, width, cuts, LANES),
        out_shape=pltpu.VMEM((rows, model), low),
        in_specs=[anywhere, inside, anywhere, anywhere, anywhere, inside],
        out_specs=inside,
        scratch_shapes=[
            vmem((rows, model), low),
            vmem((2, 8 * rows, model), low),
            vmem((blocks, n * depth, 2 * LANES), low),
            vmem((chunks, part, sub), low),
            vmem((2, 8 * rows, part), low),
            vmem((chunks + 1, 2, 2 * rows, sub), full),
            vmem((chunks + 1, 2, 2 * rows, sub), low),
            vmem((chunks + 1, 2, 2 * rows, sub), low),
            vmem((chunks + 1, 2, rows, sub // 2), low),
            vmem((chunks + 1, 2, rows, sub // 2), low),
            vmem((chunks + 1, 2, 2, rows, sub // 2), low),
            vmem((chunks + 1, 2, 2, rows, sub // 2), low),
            vmem((chunks + 1, rows, sub), full),
            vmem((rows, sub), low),
            vmem((rows, sub), low),
            vmem((rows, sub), low),
            vmem((rows, sub), low),
            vmem((rows, sub // 2), full),
            dma(()),
            dma((blocks,)),
            dma(()),
            dma(()),
            dma((4,)),
            dma((2,)),
            dma((2, 9)),
            dma((2,)),
            dma((3 * blocks,)),
            dma((2,)),
            dma((chunks,)),
            dma(()),
            dma((3,)),
            dma(()),
            dma((chunks + 1, 2)),
            dma(()),
            dma((chunks + 1,)),
            dma(()),
            dma((chunks + 1,)),
            dma(()),
            dma(()),
            dma(()),
            dma(()),
        ],
        compiler_params=pltpu.CompilerParams(
            collective_id=0, has_side_effects=True, vmem_limit_bytes=56 * 2**20
        ),
    )(tokens, norm_gain.reshape(1, -1), w_gate, w_up, w_down, post_gain.reshape(1, -1))


def solution(mesh):
    n = mesh.shape["fs"]

    def body(tokens, norm_gain, w_gate, w_up, w_down, post_gain):
        args = (tokens, norm_gain, w_gate, w_up, w_down, post_gain)
        rows = tokens.shape[0]
        fits = (
            mesh.shape["rep"] == 2 and mesh.shape["tp"] == 4 and n == 4 and rows <= 128 and rows % 128 == 0
            and w_gate.shape[1] == 6 * LANES and w_down.shape[1] == 2 * PIECE
        )
        return chain_body(n, *args) if fits else plain_body(*args)

    return jax.shard_map(
        body,
        mesh=mesh,
        in_specs=(
            P(("rep", "fs", "tp"), None),
            P(),
            P("fs", "tp"),
            P("fs", "tp"),
            P("tp", "fs"),
            P(),
        ),
        out_specs=P(("rep", "fs", "tp"), None),
        check_vma=False,
    )
```

```python
import functools

import jax
import jax.numpy as jnp
from jax import lax
from jax.experimental import pallas as pl
from jax.experimental.pallas import tpu as pltpu
from jax.sharding import PartitionSpec as P

EPS = 1e-06
MESH = pl.DeviceIdType.MESH
PIECE = 256
LANES = 128


def rms_scale(values, gain):
    return values * lax.rsqrt(jnp.mean(values * values, axis=-1, keepdims=True) + EPS) * gain


def plain_body(tokens, norm_gain, w_gate, w_up, w_down, post_gain):
    own_normed = rms_scale(tokens.astype(jnp.float32), norm_gain).astype(jnp.bfloat16)
    normed = lax.all_gather(own_normed, "tp", axis=0, tiled=True)
    gate = jnp.dot(
        normed, lax.all_gather(w_gate, "fs", axis=0, tiled=True), preferred_element_type=jnp.float32
    )
    up = jnp.dot(
        normed, lax.all_gather(w_up, "fs", axis=0, tiled=True), preferred_element_type=jnp.float32
    )
    hidden = (jax.nn.silu(gate) * up).astype(jnp.bfloat16)
    terms = jnp.dot(
        hidden, lax.all_gather(w_down, "fs", axis=1, tiled=True), preferred_element_type=jnp.float32
    )
    summed = lax.psum_scatter(
        terms.astype(jnp.bfloat16), "tp", scatter_dimension=0, tiled=True
    ).astype(jnp.float32)
    return rms_scale(summed, post_gain).astype(jnp.bfloat16)


def kernel(
    n, rows, depth, part, width, cuts, lanes,
    tok_ref, gain_ref, wg_ref, wu_ref, wd_ref, post_ref, out_ref,
    gain, post, raw, tok, gu, dn, hid, kept, pair_out, pair_in, half_out, half_in, full_out, full_in, fin, res_out, res_in, diag_out, diag_in, squares,
    gain_l, post_l, tok_l, gu_l, dn_l, z_s, z_r, tok_s, tok_r, gu_s, gu_r, dn_s, dn_r, hid_s, hid_r,
    pair_s, pair_r, half_s, half_r, full_s, full_r, res_s, res_r, diag_s, diag_r,
):
    r, k, t = lax.axis_index("rep"), lax.axis_index("fs"), lax.axis_index("tp")
    x, c = t // 2, t % 2
    t_pair, t_x, r_y = x * 2 + (1 - c), (1 - x) * 2 + c, 1 - r
    t_px = (1 - x) * 2 + (1 - c)
    partner, along_x, along_y, diag = {"tp": t_pair}, {"tp": t_x}, {"rep": r_y}, {"rep": r_y, "tp": t_x}
    left = k < n // 2
    last = jnp.where(left, 0, n - 1)
    near = jnp.where(left, 1, n - 2)
    far_near, far_last = n - 1 - near, n - 1 - last
    at_end = k == last
    in_middle = k != last
    inner, outer = {"fs": jnp.where(left, k + 1, k - 1)}, {"fs": last}
    blocks = part // lanes
    sub = width // cuts
    half = pl.multiple_of(r * part, part)
    piece = rows // 4
    own_depth = pl.ds(pl.multiple_of(k * depth, depth), depth)

    def gu_load(b, q):
        ref = (wg_ref, wu_ref)[q]
        return pltpu.make_async_copy(
            ref.at[:, pl.ds(half + b * lanes, lanes)], gu.at[b, own_depth, pl.ds(q * lanes, lanes)], gu_l.at[b]
        )

    def dn_load(j):
        return pltpu.make_async_copy(wd_ref.at[pl.ds(half, part), pl.ds(j * sub, sub)], dn.at[k * cuts + j], dn_l)

    tok_load = pltpu.make_async_copy(tok_ref, raw, tok_l)
    gain_load = pltpu.make_async_copy(gain_ref, gain, gain_l)
    post_load = pltpu.make_async_copy(post_ref, post, post_l)

    tok_load.start()
    gain_load.start()
    for b in range(blocks):
        for q in (0, 1):
            gu_load(b, q).start()
    for j in range(cuts):
        dn_load(j).start()
    post_load.start()

    barrier = pltpu.get_barrier_semaphore()
    for where in (partner, along_x, along_y, diag, inner):
        pl.semaphore_signal(barrier, inc=1, device_id=where, device_id_type=MESH)

    @pl.when(in_middle)
    def _():
        pl.semaphore_signal(barrier, inc=1, device_id=outer, device_id_type=MESH)

    tok_load.wait()
    gain_load.wait()
    tile = 32
    first = (r * 4 + x) * rows

    @pl.loop(0, rows // tile)
    def _(i):
        at = pl.ds(pl.multiple_of(i * tile, tile), tile)
        to = pl.ds(pl.multiple_of(first + i * tile, tile), tile)
        tok[0, to, :] = rms_scale(raw[at, :].astype(jnp.float32), gain[...]).astype(jnp.bfloat16)

    pl.semaphore_wait(barrier, 5 + jnp.where(in_middle, 1, 0))

    def remote(ref, send, recv, where, to=None):
        return pltpu.make_async_remote_copy(
            ref, ref if to is None else to, send, recv, device_id=where, device_id_type=MESH
        )

    pieces = 2
    step_depth = depth // pieces

    def gu_at(s, b, h):
        return gu.at[b, pl.ds(pl.multiple_of(s * depth + h * step_depth, step_depth), step_depth)]

    def gu_send(kind, b, h):
        at = jnp.where(in_middle, pieces * blocks + b, pieces * b + h)
        return remote(gu_at(last if kind else k, b, h), gu_s.at[kind], gu_r.at[at], inner)

    def gu_pass(b, h):
        remote(gu_at(last, b, h), gu_s.at[1], gu_r.at[pieces * b + h], inner).wait_recv()
        gu_send(1, b, h).start()

    def gu_wait(b):
        remote(gu.at[b, pl.ds(0, 2 * depth)], gu_s.at[0], gu_r.at[pieces * blocks + b], inner).wait_recv()

    def dn_send(way, s, j):
        at = s * cuts + j
        return remote(dn.at[at], dn_s.at[way], dn_r.at[at], outer if way else inner)

    def dn_wait(s, j):
        at = s * cuts + j
        remote(dn.at[at], dn_s.at[0], dn_r.at[at], inner).wait_recv()

    def pass_down(way, s, j):
        dn_wait(s, j)
        dn_send(way, s, j).start()

    def rows_of(p, r_at, t_at, first, count, core):
        other = (t_at % 2 + core) % 2
        base = (r_at * 4 + other * 2 + t_at // 2) * rows
        return tok.at[p, pl.ds(base + first * piece, count * piece)]

    def z_send(i):
        return remote(rows_of(0, r, t, i, 1, c), z_s, z_r.at[i], inner, rows_of(1, r, t, i, 1, c))

    def z_wait(i):
        remote(rows_of(1, r, t, i, 1, c), z_s, z_r.at[i], inner).wait_recv()

    sends = (
        [((r, t, i, 1), along_x) for i in range(4)]
        + [((r, t, i, 1), along_y) for i in range(4)]
        + [((r, t_x, 0, 1), along_y), ((r, t_x, 1, 1), along_y), ((r_y, t, 2, 1), along_x), ((r_y, t, 3, 1), along_x)]
        + [((r_at, t_at, i, 2), partner) for r_at, t_at in ((r, t), (r, t_x), (r_y, t), (r_y, t_x)) for i in (0, 2)]
    )
    groups = (
        ((0, 1), (6, 7), (2, 3), (4, 5), (8, 9), (10, 11), (12, 13, 14, 15), (16, 17, 18, 19)),
        ((0, 4), (1, 5), (6,), (7,), (2, 3), (8, 9), (10, 11), (12, 13, 14, 15), (16, 17, 18, 19)),
    )

    def group_of(p, i):
        return [g for g, held in enumerate(groups[p]) if i in held][0]

    def go(p, *which):
        for i in which:
            at, where = sends[i]
            to = rows_of(p, *at, 1 - c if i >= 12 else c)
            remote(rows_of(p, *at, c), tok_s.at[p], tok_r.at[p, group_of(p, i)], where, to).start()

    def got(p, *which):
        g = group_of(p, which[0])
        assert groups[p][g] == which
        count = sum(1 if i < 12 else 2 for i in which) * piece
        remote(tok.at[p, pl.ds(0, count)], tok_s.at[p], tok_r.at[p, g], partner).wait_recv()

    quarter = 2 * rows
    halves = 4 * rows

    def half_rows(r_at):
        return pl.ds(pl.multiple_of(r_at * halves, halves), halves)

    def hid_at(p, b, r_at):
        return hid.at[p, half_rows(r_at), pl.ds(pl.multiple_of(b * lanes, lanes), lanes)]

    def hid_send(b, r_at):
        sem = jnp.where((b == 0) & (r_at == r), 2, r_at)
        return remote(hid_at(1, b, r_at), hid_s, hid_r.at[sem], outer, hid_at(0, b, r_at))

    def hid_wait(r_at, first, count, sem):
        held = hid.at[0, half_rows(r_at), pl.ds(first * lanes, count * lanes)]
        remote(held, hid_s, hid_r.at[sem], partner).wait_recv()

    def gated(p, b, r_at):
        both = jnp.dot(tok[p, half_rows(r_at), :], gu[b], preferred_element_type=jnp.float32)
        gate, up = both[:, :lanes], both[:, lanes:]
        hid_at(p, b, r_at)[...] = (gate / (1.0 + jnp.exp(-gate)) * up).astype(jnp.bfloat16)

    chunks = n * cuts
    mid = sub // 2
    here, there = 0, 1

    def pair_copy(p, side):
        return remote(pair_out.at[p, side], pair_s, pair_r.at[p, side], partner, pair_in.at[p, side])

    def half_copy(p, way):
        return remote(
            half_out.at[p, way], half_s, half_r.at[p], along_y if way else along_x, half_in.at[p, way]
        )

    def full_copy(p, way, part_at):
        return remote(
            full_out.at[p, way, part_at], full_s, full_r.at[p], along_y if way else along_x, full_in.at[p, way, part_at]
        )

    def source(i):
        near_or_last = jnp.where(i == 0, k, near + last - k)
        return jnp.where(i < 2, near_or_last, jnp.where(i == 2, far_near, far_last))

    def place(at):
        return jnp.where(at < chunks, source(at // cuts) * cuts + at % cuts, chunks)

    def product(at, side):
        p = place(at)
        held = jnp.where(at < chunks, p, far_last * cuts + cuts - 1)
        rows_at = half_rows(r_y if side == there else r)
        both = jnp.dot(hid[jnp.where(at < chunks, 0, 1), rows_at, :], dn[held], preferred_element_type=jnp.float32)
        pair_out[p, side] = both[quarter:].astype(jnp.bfloat16)
        pair_copy(p, side).start()
        kept[p, side] = both[:quarter]

    def send_own_gu():
        for b in range(blocks):
            pltpu.make_async_copy(gu.at[b, own_depth], gu.at[b, own_depth], gu_l.at[b]).wait()
            for h in range(pieces):
                gu_send(0, b, h).start()

    def send_own_dn(way):
        own = dn.at[pl.ds(k * cuts, cuts)]
        pltpu.make_async_copy(own, own, dn_l).wait()
        for j in range(cuts):
            dn_send(way, k, j).start()

    @pl.when(in_middle)
    def _():
        send_own_gu()
        send_own_dn(1)

    @pl.when(at_end)
    def _():
        for i in range(4):
            z_send(i).start()
        send_own_gu()
        hid_wait(r, 0, 1, 2)
        send_own_dn(0)

    @pl.when(in_middle)
    def _():
        @pl.loop(0, 12)
        def _(at_step):
            def step(at):
                return pl.when(at_step == at)

            @step(0)
            def _():
                go(0, 0, 1, 6, 7, 12, 13)
                z_wait(0)
                go(1, 0, 4)
                got(0, 0, 1)
                go(0, 14)
                got(0, 6, 7)
                go(0, 17)
                z_wait(1)
                go(1, 1, 5, 12)
                got(1, 0, 4)
                z_wait(2)
                go(1, 2, 6)
                got(1, 1, 5)
                go(1, 14, 16)
                z_wait(3)
                go(1, 13, 3, 7, 8, 9)
                got(1, 6)
                go(1, 10)
                gu_pass(0, 0)
                got(1, 7)
                go(1, 17, 11)
                got(1, 2, 3)
                go(1, 15)
                gu_pass(0, 1)
                go(0, 2, 4)
                gu_pass(1, 0)
                go(0, 3, 5)
                got(1, 8, 9)
                go(1, 18)
                got(1, 10, 11)
                go(1, 19)
                go(0, 8, 10)
                gu_pass(1, 1)
                got(1, 12, 13, 14, 15)
                gu_wait(0)

            @step(1)
            def _():
                got(1, 16, 17, 18, 19)

            @pl.when(at_step == 2 - c)
            def _():
                gu_pass(2, 0)

            @step(2)
            def _():
                go(0, 9, 11)
                got(0, 2, 3)
                go(0, 15)
                got(0, 4, 5)
                go(0, 16)
                gu_pass(2, 1)

            @pl.when(at_step == 2 + 4 * c)
            def _():
                for j in range(cuts):
                    dn_send(0, k, j).start()

            @step(2)
            def _():
                gu_wait(1)

            @step(4)
            def _():
                got(0, 12, 13, 14, 15)

            @step(6)
            def _():
                got(0, 8, 9)
                go(0, 18)
                got(0, 10, 11)
                go(0, 19)
                gu_wait(2)

            @step(8)
            def _():
                got(0, 16, 17, 18, 19)

            @step(10)
            def _():
                pass_down(0, last, 0)

            @step(11)
            def _():
                pl.loop(0, 2)(lambda at: product(at, there))
                pass_down(0, last, 1)

            passed = (at_step < 4) | (at_step == 6) | (at_step == 7)
            late = jnp.where(at_step < 8, 2, jnp.where(at_step < 11, at_step - 8, 2))
            b = jnp.where(at_step < 4, at_step // 2, jnp.where(at_step < 6, at_step - 4, late))
            first_r = jnp.where(at_step < 2, r, r_y)
            own_r = jnp.where((at_step < 6) | (at_step == 11), r, r_y)
            r_at = jnp.where(passed, (first_r + at_step % 2) % 2, own_r)
            gated(jnp.where(passed, 1, 0), b, r_at)

            @pl.when(passed)
            def _():
                hid_send(b, r_at).start()

    def of(m):
        return pl.ds(pl.multiple_of(m * rows, rows), rows)

    def summed(p, side, x_at):
        return kept[p, side, of(x_at), :] + pair_in[p, side, of(x_at), :].astype(jnp.float32)

    def finish_there(at):
        p = place(at)
        pair_copy(p, there).wait_recv()
        across = summed(p, there, 1 - x).astype(jnp.bfloat16)
        half_out[p, 0] = across[:, :mid]
        half_out[p, 1] = across[:, mid:]
        half_copy(p, 0).start()
        half_copy(p, 1).start()
        value = summed(p, there, x)
        kept[p, there, of(x), :mid] = value[:, :mid]
        full_out[p, 1, 1] = value[:, mid:].astype(jnp.bfloat16)
        full_copy(p, 1, 1).start()

    def finish_here(at):
        p = place(at)
        pair_copy(p, here).wait_recv()
        value = summed(p, here, 1 - x)
        kept[p, here, of(1 - x), mid:] = value[:, mid:]
        full_out[p, 0, 0] = value[:, :mid].astype(jnp.bfloat16)
        full_copy(p, 0, 0).start()
        fin[p] = summed(p, here, x)

    across_copy = remote(diag_out, diag_s, diag_r, diag, diag_in)

    def finish_direct(at):
        p = place(at)
        pair_copy(p, there).wait_recv()
        diag_out[...] = summed(p, there, 1 - x).astype(jnp.bfloat16)
        across_copy.start()
        value = summed(p, there, x).astype(jnp.bfloat16)
        for part_at in (1, 0):
            full_out[p, 1, part_at] = value[:, part_at * mid : (part_at + 1) * mid]
            full_copy(p, 1, part_at).start()
        pair_copy(p, here).wait_recv()
        value = summed(p, here, 1 - x).astype(jnp.bfloat16)
        for part_at in (0, 1):
            full_out[p, 0, part_at] = value[:, part_at * mid : (part_at + 1) * mid]
            full_copy(p, 0, part_at).start()
        fin[p] = summed(p, here, x)

    def finish_half(at):
        p = place(at)
        remote(half_in.at[p], half_s, half_r.at[p], partner).wait_recv()
        full_out[p, 0, 1] = (kept[p, here, of(1 - x), mid:] + half_in[p, 1].astype(jnp.float32)).astype(jnp.bfloat16)
        full_copy(p, 0, 1).start()
        full_out[p, 1, 0] = (kept[p, there, of(x), :mid] + half_in[p, 0].astype(jnp.float32)).astype(jnp.bfloat16)
        full_copy(p, 1, 0).start()

    early = 2 * cuts

    @pl.when(at_end)
    def _():
        for j in range(cuts):
            dn_wait(near, j)
        hid_wait(r_y, 0, blocks, r_y)

    @pl.loop(0, early)
    def _(at):
        @pl.when(at_end | (at > 1))
        def _():
            product(at, there)

        @pl.when(at > 0)
        def _():
            finish_there(at - 1)

        @pl.when(in_middle & (at == 0))
        def _():
            pass_down(1, far_near, 0)

    @pl.when(at_end)
    def _():
        hid_wait(r, 1, blocks - 1, r)

    @pl.loop(0, early)
    def _(at):
        product(at, here)

        @pl.when(at == 0)
        def _():
            finish_there(early - 1)

        @pl.when(at > 0)
        def _():
            finish_here(at - 1)
            finish_half(at - 1)

        @pl.when(in_middle & (at == 2))
        def _():
            pass_down(1, far_near, 1)


    result = remote(res_out, res_s, res_r, outer, res_in)

    def collect(at, part_at):
        p = place(at)
        cols = pl.ds(part_at * mid, mid)
        both = full_in[p, 0, part_at].astype(jnp.float32) + full_in[p, 1, part_at].astype(jnp.float32)
        return fin[p, :, cols] + both

    def arrive(at):
        remote(full_in.at[place(at)], full_s, full_r.at[place(at)], along_x).wait_recv()

    def order(i):
        return jnp.where(in_middle & (i >= 2), jnp.where(i == 2, chunks, early + i - 1), early + i)

    @pl.loop(0, chunks - early + 1)
    def _(i):
        at = order(i)

        @pl.when(at_end & (i < 3))
        def _():
            dn_wait(source(at // cuts), at % cuts)

        @pl.when(in_middle & (i == 0) & (c == 0))
        def _():
            pass_down(1, far_last, 0)

        @pl.when(in_middle & (i == 2))
        def _():
            dn_wait(far_last, cuts - 1)

        @pl.when(in_middle | (i < 3))
        def _():
            product(at, there)
            product(at, here)

        @pl.when(i == 0)
        def _():
            finish_here(early - 1)
            finish_half(early - 1)

        @pl.when(in_middle & (i == 3))
        def _():
            finish_half(chunks)

        @pl.when(in_middle | (i < 2))
        def _():
            finish_there(at)
            finish_here(at)

        @pl.when(at_end & (i == 2))
        def _():
            finish_direct(at)

        @pl.when(in_middle & (i == 1) & (c == 1))
        def _():
            pass_down(1, far_last, 0)

        @pl.when(in_middle & (i == 4))
        def _():
            arrive(chunks)
            for part_at in (0, 1):
                res_out[:, pl.ds(part_at * mid, mid)] = collect(chunks, part_at).astype(jnp.bfloat16)
            result.start()

        @pl.when((i > 0) & (i != 3) & (in_middle | (i < 3)))
        def _():
            finish_half(order(i - 1))

    @pl.when(in_middle)
    def _():
        finish_half(chunks - 1)

    remote(gu.at[:, pl.ds(0, depth)], gu_s.at[0], gu_r.at[0], inner).wait_send()

    @pl.when(at_end)
    def _():
        remote(tok.at[0, pl.ds(0, rows)], z_s, z_r.at[0], inner).wait_send()
        remote(dn.at[pl.ds(0, cuts)], dn_s.at[0], dn_r.at[0], inner).wait_send()
        remote(pair_out.at[pl.ds(0, chunks - 1)], pair_s, pair_r.at[0, 0], partner).wait_send()
        remote(half_out.at[pl.ds(0, chunks - 2)], half_s, half_r.at[0], along_x).wait_send()
        across_copy.wait_send()

    @pl.when(in_middle)
    def _():
        for p in (0, 1):
            total = sum(1 if i < 12 else 2 for i in range(len(sends))) * piece
            remote(tok.at[p, pl.ds(0, total)], tok_s.at[p], tok_r.at[p, 0], partner).wait_send()
        remote(gu.at[:, pl.ds(0, depth)], gu_s.at[1], gu_r.at[0], inner).wait_send()
        remote(hid.at[1], hid_s, hid_r.at[0], outer).wait_send()
        remote(dn.at[pl.ds(0, 2 * cuts)], dn_s.at[0], dn_r.at[0], inner).wait_send()
        remote(dn.at[pl.ds(0, 3 * cuts - 1)], dn_s.at[1], dn_r.at[0], outer).wait_send()
        remote(pair_out, pair_s, pair_r.at[0, 0], partner).wait_send()
        remote(half_out, half_s, half_r.at[0], along_x).wait_send()

    squares[...] = jnp.zeros_like(squares)

    def settle(at, part_at, total):
        fin[place(at), :, pl.ds(part_at * mid, mid)] = total
        squares[...] += total * total

    @pl.loop(0, chunks)
    def _(at):
        @pl.when(in_middle | (at < chunks - 2))
        def _():
            arrive(at)
            for part_at in (0, 1):
                settle(at, part_at, collect(at, part_at))

    @pl.when(at_end)
    def _():
        across_copy.wait_recv()
        p = place(chunks - 2)
        for part_at in (0, 1):
            cols = pl.ds(part_at * mid, mid)
            fin[p, :, cols] = fin[p, :, cols] + diag_in[:, cols].astype(jnp.float32)
        arrive(chunks - 2)
        for part_at in (0, 1):
            settle(chunks - 2, part_at, collect(chunks - 2, part_at))
        result.wait_recv()
        for part_at in (0, 1):
            settle(chunks - 1, part_at, res_in[:, pl.ds(part_at * mid, mid)].astype(jnp.float32))

    post_load.wait()
    scale = lax.rsqrt(jnp.sum(squares[...], axis=-1, keepdims=True) / (n * width) + EPS)
    for p in range(chunks):
        cols = pl.ds(p * sub, sub)
        out_ref[:, cols] = (fin[p] * scale * post[:, cols]).astype(out_ref.dtype)

    @pl.when(at_end)
    def _():
        remote(full_out.at[pl.ds(0, chunks - 1)], full_s, full_r.at[0], along_x).wait_send()

    @pl.when(in_middle)
    def _():
        remote(full_out, full_s, full_r.at[0], along_x).wait_send()
        result.wait_send()


def chain_body(n, tokens, norm_gain, w_gate, w_up, w_down, post_gain):
    rows, model = tokens.shape
    depth, block = w_gate.shape
    width = w_down.shape[1]
    part = block // 2
    cuts = width // PIECE
    sub = width // cuts
    blocks = part // LANES
    chunks = n * cuts
    vmem, dma = pltpu.VMEM, pltpu.SemaphoreType.DMA
    low, full = jnp.bfloat16, jnp.float32
    anywhere = pl.BlockSpec(memory_space=pl.ANY)
    inside = pl.BlockSpec(memory_space=vmem)
    return pl.pallas_call(
        functools.partial(kernel, n, rows, depth, part, width, cuts, LANES),
        out_shape=pltpu.VMEM((rows, model), low),
        in_specs=[anywhere] * 6,
        out_specs=inside,
        scratch_shapes=[
            vmem((1, model), full),
            vmem((1, model), full),
            vmem((rows, model), low),
            vmem((2, 8 * rows, model), low),
            vmem((blocks, n * depth, 2 * LANES), low),
            vmem((chunks, part, sub), low),
            vmem((2, 8 * rows, part), low),
            vmem((chunks + 1, 2, 2 * rows, sub), full),
            vmem((chunks + 1, 2, 2 * rows, sub), low),
            vmem((chunks + 1, 2, 2 * rows, sub), low),
            vmem((chunks + 1, 2, rows, sub // 2), low),
            vmem((chunks + 1, 2, rows, sub // 2), low),
            vmem((chunks + 1, 2, 2, rows, sub // 2), low),
            vmem((chunks + 1, 2, 2, rows, sub // 2), low),
            vmem((chunks + 1, rows, sub), full),
            vmem((rows, sub), low),
            vmem((rows, sub), low),
            vmem((rows, sub), low),
            vmem((rows, sub), low),
            vmem((rows, sub // 2), full),
            dma(()),
            dma(()),
            dma(()),
            dma((blocks,)),
            dma(()),
            dma(()),
            dma((4,)),
            dma((2,)),
            dma((2, 9)),
            dma((2,)),
            dma((3 * blocks,)),
            dma((2,)),
            dma((chunks,)),
            dma(()),
            dma((3,)),
            dma(()),
            dma((chunks + 1, 2)),
            dma(()),
            dma((chunks + 1,)),
            dma(()),
            dma((chunks + 1,)),
            dma(()),
            dma(()),
            dma(()),
            dma(()),
        ],
        compiler_params=pltpu.CompilerParams(
            collective_id=0, has_side_effects=True, vmem_limit_bytes=56 * 2**20
        ),
    )(tokens, norm_gain.reshape(1, -1), w_gate, w_up, w_down, post_gain.reshape(1, -1))


def solution(mesh):
    n = mesh.shape["fs"]

    def body(tokens, norm_gain, w_gate, w_up, w_down, post_gain):
        args = (tokens, norm_gain, w_gate, w_up, w_down, post_gain)
        rows = tokens.shape[0]
        fits = (
            mesh.shape["rep"] == 2 and mesh.shape["tp"] == 4 and n == 4 and rows <= 128 and rows % 128 == 0
            and w_gate.shape[1] == 6 * LANES and w_down.shape[1] == 2 * PIECE
        )
        return chain_body(n, *args) if fits else plain_body(*args)

    return jax.shard_map(
        body,
        mesh=mesh,
        in_specs=(
            P(("rep", "fs", "tp"), None),
            P(),
            P("fs", "tp"),
            P("fs", "tp"),
            P("tp", "fs"),
            P(),
        ),
        out_specs=P(("rep", "fs", "tp"), None),
        check_vma=False,
    )
```

```python
import functools

import jax
import jax.numpy as jnp
from jax import lax
from jax.experimental import pallas as pl
from jax.experimental.pallas import tpu as pltpu
from jax.sharding import PartitionSpec as P

EPS = 1e-06
MESH = pl.DeviceIdType.MESH
PIECE = 256
LANES = 128


def rms_scale(values, gain):
    return values * lax.rsqrt(jnp.mean(values * values, axis=-1, keepdims=True) + EPS) * gain


def plain_body(tokens, norm_gain, w_gate, w_up, w_down, post_gain):
    own_normed = rms_scale(tokens.astype(jnp.float32), norm_gain).astype(jnp.bfloat16)
    normed = lax.all_gather(own_normed, "tp", axis=0, tiled=True)
    gate = jnp.dot(
        normed, lax.all_gather(w_gate, "fs", axis=0, tiled=True), preferred_element_type=jnp.float32
    )
    up = jnp.dot(
        normed, lax.all_gather(w_up, "fs", axis=0, tiled=True), preferred_element_type=jnp.float32
    )
    hidden = (jax.nn.silu(gate) * up).astype(jnp.bfloat16)
    terms = jnp.dot(
        hidden, lax.all_gather(w_down, "fs", axis=1, tiled=True), preferred_element_type=jnp.float32
    )
    summed = lax.psum_scatter(
        terms.astype(jnp.bfloat16), "tp", scatter_dimension=0, tiled=True
    ).astype(jnp.float32)
    return rms_scale(summed, post_gain).astype(jnp.bfloat16)


def kernel(
    n, rows, depth, part, width, cuts, lanes,
    tok_ref, gain_ref, wg_ref, wu_ref, wd_ref, post_ref, out_ref,
    gain, post, raw, tok, gu, dn, hid, kept, pair_out, pair_in, half_out, half_in, full_out, full_in, fin, res_out, res_in, diag_out, diag_in, squares,
    gain_l, post_l, tok_l, gu_l, dn_l, z_s, z_r, tok_s, tok_r, gu_s, gu_r, dn_s, dn_r,
    pair_s, pair_r, half_s, half_r, full_s, full_r, res_s,
):
    r, k, t = lax.axis_index("rep"), lax.axis_index("fs"), lax.axis_index("tp")
    x, c = t // 2, t % 2
    t_pair, t_x, r_y = x * 2 + (1 - c), (1 - x) * 2 + c, 1 - r
    t_px = (1 - x) * 2 + (1 - c)
    partner, along_x, along_y, diag = {"tp": t_pair}, {"tp": t_x}, {"rep": r_y}, {"rep": r_y, "tp": t_x}
    left = k < n // 2
    last = jnp.where(left, 0, n - 1)
    near = jnp.where(left, 1, n - 2)
    far_near, far_last = n - 1 - near, n - 1 - last
    at_end = k == last
    in_middle = k != last
    inner, outer = {"fs": jnp.where(left, k + 1, k - 1)}, {"fs": last}
    blocks = part // lanes
    sub = width // cuts
    half = pl.multiple_of(r * part, part)
    piece = rows // 4
    own_depth = pl.ds(pl.multiple_of(k * depth, depth), depth)

    def gu_load(b, q):
        ref = (wg_ref, wu_ref)[q]
        return pltpu.make_async_copy(
            ref.at[:, pl.ds(half + b * lanes, lanes)], gu.at[b, own_depth, pl.ds(q * lanes, lanes)], gu_l.at[b]
        )

    def dn_load(j):
        return pltpu.make_async_copy(wd_ref.at[pl.ds(half, part), pl.ds(j * sub, sub)], dn.at[k * cuts + j], dn_l)

    tok_load = pltpu.make_async_copy(tok_ref, raw, tok_l)
    gain_load = pltpu.make_async_copy(gain_ref, gain, gain_l)
    post_load = pltpu.make_async_copy(post_ref, post, post_l)

    tok_load.start()
    gain_load.start()

    barrier = pltpu.get_barrier_semaphore()
    for where in (partner, along_x, along_y, diag, inner):
        pl.semaphore_signal(barrier, inc=1, device_id=where, device_id_type=MESH)

    @pl.when(in_middle)
    def _():
        pl.semaphore_signal(barrier, inc=1, device_id=outer, device_id_type=MESH)

    for b in range(blocks):
        for q in (0, 1):
            gu_load(b, q).start()
    for j in range(cuts):
        dn_load(j).start()
    post_load.start()

    tok_load.wait()
    gain_load.wait()
    tile = 32
    first = (r * 4 + x) * rows

    @pl.loop(0, rows // tile)
    def _(i):
        at = pl.ds(pl.multiple_of(i * tile, tile), tile)
        to = pl.ds(pl.multiple_of(first + i * tile, tile), tile)
        tok[0, to, :] = rms_scale(raw[at, :].astype(jnp.float32), gain[...]).astype(jnp.bfloat16)

    pl.semaphore_wait(barrier, 5 + jnp.where(in_middle, 1, 0))

    def remote(ref, send, recv, where, to=None):
        return pltpu.make_async_remote_copy(
            ref, ref if to is None else to, send, recv, device_id=where, device_id_type=MESH
        )

    pieces = 2
    step_depth = depth // pieces

    def gu_at(s, b, h):
        return gu.at[b, pl.ds(pl.multiple_of(s * depth + h * step_depth, step_depth), step_depth)]

    def gu_send(kind, b, h):
        at = jnp.where(in_middle, pieces * blocks + b, pieces * b + h)
        return remote(gu_at(last if kind else k, b, h), gu_s.at[kind], gu_r.at[at], inner)

    def gu_pass(b, h):
        remote(gu_at(last, b, h), gu_s.at[1], gu_r.at[pieces * b + h], inner).wait_recv()
        gu_send(1, b, h).start()

    def gu_wait(b):
        remote(gu.at[b, pl.ds(0, 2 * depth)], gu_s.at[0], gu_r.at[pieces * blocks + b], inner).wait_recv()

    def dn_send(way, s, j):
        at = s * cuts + j
        return remote(dn.at[at], dn_s.at[way], dn_r.at[at], outer if way else inner)

    def dn_wait(s, j):
        at = s * cuts + j
        remote(dn.at[at], dn_s.at[0], dn_r.at[at], inner).wait_recv()

    def pass_down(way, s, j):
        dn_wait(s, j)
        dn_send(way, s, j).start()

    def rows_of(p, r_at, t_at, first, count, core):
        other = (t_at % 2 + core) % 2
        base = (r_at * 4 + other * 2 + t_at // 2) * rows
        return tok.at[p, pl.ds(base + first * piece, count * piece)]

    def z_send(i):
        return remote(rows_of(0, r, t, i, 1, c), z_s, z_r.at[i], inner, rows_of(1, r, t, i, 1, c))

    def z_wait(i):
        remote(rows_of(1, r, t, i, 1, c), z_s, z_r.at[i], inner).wait_recv()

    sends = (
        [((r, t, i, 1), along_x) for i in range(4)]
        + [((r, t, i, 1), along_y) for i in range(4)]
        + [((r, t_x, 0, 1), along_y), ((r, t_x, 1, 1), along_y), ((r_y, t, 2, 1), along_x), ((r_y, t, 3, 1), along_x)]
        + [((r_at, t_at, i, 2), partner) for r_at, t_at in ((r, t), (r, t_x), (r_y, t), (r_y, t_x)) for i in (0, 2)]
    )
    groups = (
        ((0, 1, 6, 7), (2, 3, 4, 5), (8, 9, 10, 11), (12, 13, 14, 15), (16, 17, 18, 19)),
        ((0, 4), (1, 5), (6,), (2, 3, 7), (8, 9, 10, 11), (12, 13, 14, 15), (16, 17, 18, 19)),
    )

    def group_of(p, i):
        return [g for g, held in enumerate(groups[p]) if i in held][0]

    def go(p, *which):
        for i in which:
            at, where = sends[i]
            to = rows_of(p, *at, 1 - c if i >= 12 else c)
            remote(rows_of(p, *at, c), tok_s.at[p], tok_r.at[5 * p + group_of(p, i)], where, to).start()

    def got(p, *which):
        g = group_of(p, which[0])
        assert groups[p][g] == which
        count = sum(1 if i < 12 else 2 for i in which) * piece
        remote(tok.at[p, pl.ds(0, count)], tok_s.at[p], tok_r.at[5 * p + g], partner).wait_recv()

    quarter = 2 * rows
    halves = 4 * rows

    def half_rows(r_at):
        return pl.ds(pl.multiple_of(r_at * halves, halves), halves)

    def hid_at(p, b, r_at):
        return hid.at[p, half_rows(r_at), pl.ds(pl.multiple_of(b * lanes, lanes), lanes)]

    def hid_send(b, r_at):
        sem = jnp.where((b == 0) & (r_at == r), 2, r_at)
        return remote(hid_at(1, b, r_at), z_s, gu_r.at[sem], outer, hid_at(0, b, r_at))

    def hid_wait(r_at, first, count, sem):
        held = hid.at[0, half_rows(r_at), pl.ds(first * lanes, count * lanes)]
        remote(held, z_s, gu_r.at[sem], partner).wait_recv()

    def gated(p, b, r_at):
        both = jnp.dot(tok[p, half_rows(r_at), :], gu[b], preferred_element_type=jnp.float32)
        gate, up = both[:, :lanes], both[:, lanes:]
        hid_at(p, b, r_at)[...] = (gate / (1.0 + jnp.exp(-gate)) * up).astype(jnp.bfloat16)

    chunks = n * cuts
    mid = sub // 2
    here, there = 0, 1

    def pair_copy(at, side):
        p = place(at)
        return remote(pair_out.at[p, side], pair_s, pair_r.at[at % 4, side], partner, pair_in.at[p, side])

    def half_copy(p, way):
        return remote(
            half_out.at[p, way], half_s, half_r.at[p], along_y if way else along_x, half_in.at[p, way]
        )

    def full_sem(at):
        return full_r.at[jnp.maximum(at - early + 1, 0)]

    def full_copy(at, way, part_at):
        p = place(at)
        return remote(
            full_out.at[p, way, part_at], full_s, full_sem(at), along_y if way else along_x, full_in.at[p, way, part_at]
        )

    def source(i):
        near_or_last = jnp.where(i == 0, k, near + last - k)
        return jnp.where(i < 2, near_or_last, jnp.where(i == 2, far_near, far_last))

    def place(at):
        return jnp.where(at < chunks, source(at // cuts) * cuts + at % cuts, chunks)

    def product(at, side):
        p = place(at)
        held = jnp.where(at < chunks, p, far_last * cuts + cuts - 1)
        rows_at = half_rows(r_y if side == there else r)
        both = jnp.dot(hid[jnp.where(at < chunks, 0, 1), rows_at, :], dn[held], preferred_element_type=jnp.float32)
        pair_out[p, side] = both[quarter:].astype(jnp.bfloat16)
        pair_copy(at, side).start()
        kept[p, side] = both[:quarter]

    def send_own_gu():
        for b in range(blocks):
            pltpu.make_async_copy(gu.at[b, own_depth], gu.at[b, own_depth], gu_l.at[b]).wait()
            for h in range(pieces):
                gu_send(0, b, h).start()

    def send_own_dn(way):
        own = dn.at[pl.ds(k * cuts, cuts)]
        pltpu.make_async_copy(own, own, dn_l).wait()
        for j in range(cuts):
            dn_send(way, k, j).start()

    @pl.when(in_middle)
    def _():
        send_own_gu()
        send_own_dn(1)

    @pl.when(at_end)
    def _():
        for i in range(4):
            z_send(i).start()
        send_own_gu()
        hid_wait(r, 0, 1, 2)
        send_own_dn(0)

    @pl.when(in_middle)
    def _():
        @pl.loop(0, 12)
        def _(at_step):
            def step(at):
                return pl.when(at_step == at)

            @step(0)
            def _():
                go(0, 0, 1, 6, 7, 12, 13)
                z_wait(0)
                go(1, 0, 4)
                got(0, 0, 1, 6, 7)
                go(0, 14, 17)
                z_wait(1)
                go(1, 1, 5, 12)
                got(1, 0, 4)
                z_wait(2)
                go(1, 2, 6)
                got(1, 1, 5)
                go(1, 14, 16)
                z_wait(3)
                go(1, 13, 3, 7, 8, 9)
                got(1, 6)
                go(1, 10)
                gu_pass(0, 0)
                got(1, 2, 3, 7)
                go(1, 17, 11, 15)
                gu_pass(0, 1)
                go(0, 2, 4)
                gu_pass(1, 0)
                go(0, 3, 5)
                got(1, 8, 9, 10, 11)
                go(1, 18, 19)
                go(0, 8, 10)
                gu_pass(1, 1)
                got(1, 12, 13, 14, 15)
                gu_wait(0)

            @step(1)
            def _():
                got(1, 16, 17, 18, 19)

            @pl.when(at_step == 2 - c)
            def _():
                gu_pass(2, 0)

            @step(2)
            def _():
                go(0, 9, 11)
                got(0, 2, 3, 4, 5)
                go(0, 15, 16)
                gu_pass(2, 1)

            @pl.when(at_step == 2 + 4 * c)
            def _():
                for j in range(cuts):
                    dn_send(0, k, j).start()

            @step(2)
            def _():
                gu_wait(1)

            @step(4)
            def _():
                got(0, 12, 13, 14, 15)

            @step(6)
            def _():
                got(0, 8, 9, 10, 11)
                go(0, 18, 19)
                gu_wait(2)

            @step(8)
            def _():
                got(0, 16, 17, 18, 19)

            @step(10)
            def _():
                pass_down(0, last, 0)

            @step(11)
            def _():
                pl.loop(0, 2)(lambda at: product(at, there))
                pass_down(0, last, 1)

            passed = (at_step < 4) | (at_step == 6) | (at_step == 7)
            late = jnp.where(at_step < 8, 2, jnp.where(at_step < 11, at_step - 8, 2))
            b = jnp.where(at_step < 4, at_step // 2, jnp.where(at_step < 6, at_step - 4, late))
            first_r = jnp.where(at_step < 2, r, r_y)
            own_r = jnp.where((at_step < 6) | (at_step == 11), r, r_y)
            r_at = jnp.where(passed, (first_r + at_step % 2) % 2, own_r)
            gated(jnp.where(passed, 1, 0), b, r_at)

            @pl.when(passed)
            def _():
                hid_send(b, r_at).start()

    def of(m):
        return pl.ds(pl.multiple_of(m * rows, rows), rows)

    def summed(p, side, x_at):
        return kept[p, side, of(x_at), :] + pair_in[p, side, of(x_at), :].astype(jnp.float32)

    def finish_there(at):
        p = place(at)
        pair_copy(at, there).wait_recv()
        across = summed(p, there, 1 - x).astype(jnp.bfloat16)
        half_out[p, 0] = across[:, :mid]
        half_out[p, 1] = across[:, mid:]
        half_copy(p, 0).start()
        half_copy(p, 1).start()
        value = summed(p, there, x)
        kept[p, there, of(x), :mid] = value[:, :mid]
        full_out[p, 1, 1] = value[:, mid:].astype(jnp.bfloat16)
        full_copy(at, 1, 1).start()

    def finish_here(at):
        p = place(at)
        pair_copy(at, here).wait_recv()
        value = summed(p, here, 1 - x)
        kept[p, here, of(1 - x), mid:] = value[:, mid:]
        full_out[p, 0, 0] = value[:, :mid].astype(jnp.bfloat16)
        full_copy(at, 0, 0).start()
        fin[p] = summed(p, here, x)

    across_copy = remote(diag_out, res_s, z_r.at[1], diag, diag_in)

    def finish_direct(at):
        p = place(at)
        pair_copy(at, there).wait_recv()
        diag_out[...] = summed(p, there, 1 - x).astype(jnp.bfloat16)
        across_copy.start()
        value = summed(p, there, x).astype(jnp.bfloat16)
        for part_at in (1, 0):
            full_out[p, 1, part_at] = value[:, part_at * mid : (part_at + 1) * mid]
            full_copy(at, 1, part_at).start()
        pair_copy(at, here).wait_recv()
        value = summed(p, here, 1 - x).astype(jnp.bfloat16)
        for part_at in (0, 1):
            full_out[p, 0, part_at] = value[:, part_at * mid : (part_at + 1) * mid]
            full_copy(at, 0, part_at).start()
        fin[p] = summed(p, here, x)

    def finish_half(at):
        p = place(at)
        remote(half_in.at[p], half_s, half_r.at[p], partner).wait_recv()
        full_out[p, 0, 1] = (kept[p, here, of(1 - x), mid:] + half_in[p, 1].astype(jnp.float32)).astype(jnp.bfloat16)
        full_copy(at, 0, 1).start()
        full_out[p, 1, 0] = (kept[p, there, of(x), :mid] + half_in[p, 0].astype(jnp.float32)).astype(jnp.bfloat16)
        full_copy(at, 1, 0).start()

    early = 2 * cuts

    @pl.when(at_end)
    def _():
        for j in range(cuts):
            dn_wait(near, j)
        hid_wait(r_y, 0, blocks, r_y)

    @pl.loop(0, early)
    def _(at):
        @pl.when(at_end | (at > 1))
        def _():
            product(at, there)

        @pl.when(at > 0)
        def _():
            finish_there(at - 1)

        @pl.when(in_middle & (at == 0))
        def _():
            pass_down(1, far_near, 0)

    @pl.when(at_end)
    def _():
        hid_wait(r, 1, blocks - 1, r)

    @pl.loop(0, early)
    def _(at):
        product(at, here)

        @pl.when(at == 0)
        def _():
            finish_there(early - 1)

        @pl.when(at > 0)
        def _():
            finish_here(at - 1)
            finish_half(at - 1)

        @pl.when(in_middle & (at == 2))
        def _():
            pass_down(1, far_near, 1)


    result = remote(res_out, res_s, z_r.at[0], outer, res_in)

    def collect(at, part_at):
        p = place(at)
        cols = pl.ds(part_at * mid, mid)
        both = full_in[p, 0, part_at].astype(jnp.float32) + full_in[p, 1, part_at].astype(jnp.float32)
        return fin[p, :, cols] + both

    def arrive(at):
        remote(full_in.at[place(at)], full_s, full_sem(at), along_x).wait_recv()

    def order(i):
        return jnp.where(in_middle & (i >= 2), jnp.where(i == 2, chunks, early + i - 1), early + i)

    @pl.loop(0, chunks - early + 1)
    def _(i):
        at = order(i)

        @pl.when(at_end & (i < 3))
        def _():
            dn_wait(source(at // cuts), at % cuts)

        @pl.when(in_middle & (i == 0) & (c == 0))
        def _():
            pass_down(1, far_last, 0)

        @pl.when(in_middle & (i == 2))
        def _():
            dn_wait(far_last, cuts - 1)

        @pl.when(in_middle | (i < 3))
        def _():
            product(at, there)
            product(at, here)

        @pl.when(i == 0)
        def _():
            finish_here(early - 1)
            finish_half(early - 1)

        @pl.when(in_middle & (i == 3))
        def _():
            finish_half(chunks)

        @pl.when(in_middle | (i < 2))
        def _():
            finish_there(at)
            finish_here(at)

        @pl.when(at_end & (i == 2))
        def _():
            finish_direct(at)

        @pl.when(in_middle & (i == 1) & (c == 1))
        def _():
            pass_down(1, far_last, 0)

        @pl.when(in_middle & (i == 4))
        def _():
            arrive(chunks)
            for part_at in (0, 1):
                res_out[:, pl.ds(part_at * mid, mid)] = collect(chunks, part_at).astype(jnp.bfloat16)
            result.start()

        @pl.when((i > 0) & (i != 3) & (in_middle | (i < 3)))
        def _():
            finish_half(order(i - 1))

    @pl.when(in_middle)
    def _():
        finish_half(chunks - 1)

    remote(gu.at[:, pl.ds(0, depth)], gu_s.at[0], gu_r.at[0], inner).wait_send()

    @pl.when(at_end)
    def _():
        remote(tok.at[0, pl.ds(0, rows)], z_s, z_r.at[0], inner).wait_send()
        remote(dn.at[pl.ds(0, cuts)], dn_s.at[0], dn_r.at[0], inner).wait_send()
        remote(pair_out.at[pl.ds(0, chunks - 1)], pair_s, pair_r.at[0, 0], partner).wait_send()
        remote(half_out.at[pl.ds(0, chunks - 2)], half_s, half_r.at[0], along_x).wait_send()
        across_copy.wait_send()

    @pl.when(in_middle)
    def _():
        for p in (0, 1):
            total = sum(1 if i < 12 else 2 for i in range(len(sends))) * piece
            remote(tok.at[p, pl.ds(0, total)], tok_s.at[p], tok_r.at[p], partner).wait_send()
        remote(gu.at[:, pl.ds(0, depth)], gu_s.at[1], gu_r.at[0], inner).wait_send()
        remote(hid.at[1], z_s, gu_r.at[0], outer).wait_send()
        remote(dn.at[pl.ds(0, 2 * cuts)], dn_s.at[0], dn_r.at[0], inner).wait_send()
        remote(dn.at[pl.ds(0, 3 * cuts - 1)], dn_s.at[1], dn_r.at[0], outer).wait_send()
        remote(pair_out, pair_s, pair_r.at[0, 0], partner).wait_send()
        remote(half_out, half_s, half_r.at[0], along_x).wait_send()

    squares[...] = jnp.zeros_like(squares)

    def settle(at, part_at, total):
        fin[place(at), :, pl.ds(part_at * mid, mid)] = total
        squares[...] += total * total

    @pl.loop(0, chunks)
    def _(at):
        @pl.when(at == 0)
        def _():
            remote(full_in.at[pl.ds(0, early)], full_s, full_sem(0), along_x).wait_recv()

        @pl.when((at >= early) & (in_middle | (at < chunks - 2)))
        def _():
            arrive(at)

        @pl.when(in_middle | (at < chunks - 2))
        def _():
            for part_at in (0, 1):
                settle(at, part_at, collect(at, part_at))

    @pl.when(at_end)
    def _():
        across_copy.wait_recv()
        p = place(chunks - 2)
        for part_at in (0, 1):
            cols = pl.ds(part_at * mid, mid)
            fin[p, :, cols] = fin[p, :, cols] + diag_in[:, cols].astype(jnp.float32)
        arrive(chunks - 2)
        for part_at in (0, 1):
            settle(chunks - 2, part_at, collect(chunks - 2, part_at))
        result.wait_recv()
        for part_at in (0, 1):
            settle(chunks - 1, part_at, res_in[:, pl.ds(part_at * mid, mid)].astype(jnp.float32))

    post_load.wait()
    scale = lax.rsqrt(jnp.sum(squares[...], axis=-1, keepdims=True) / (n * width) + EPS)
    for p in range(chunks):
        cols = pl.ds(p * sub, sub)
        out_ref[:, cols] = (fin[p] * scale * post[:, cols]).astype(out_ref.dtype)

    @pl.when(at_end)
    def _():
        remote(full_out.at[pl.ds(0, chunks - 1)], full_s, full_r.at[0], along_x).wait_send()

    @pl.when(in_middle)
    def _():
        remote(full_out, full_s, full_r.at[0], along_x).wait_send()
        result.wait_send()


def chain_body(n, tokens, norm_gain, w_gate, w_up, w_down, post_gain):
    rows, model = tokens.shape
    depth, block = w_gate.shape
    width = w_down.shape[1]
    part = block // 2
    cuts = width // PIECE
    sub = width // cuts
    blocks = part // LANES
    chunks = n * cuts
    vmem, dma = pltpu.VMEM, pltpu.SemaphoreType.DMA
    low, full = jnp.bfloat16, jnp.float32
    anywhere = pl.BlockSpec(memory_space=pl.ANY)
    inside = pl.BlockSpec(memory_space=vmem)
    return pl.pallas_call(
        functools.partial(kernel, n, rows, depth, part, width, cuts, LANES),
        out_shape=pltpu.VMEM((rows, model), low),
        in_specs=[anywhere] * 6,
        out_specs=inside,
        scratch_shapes=[
            vmem((1, model), full),
            vmem((1, model), full),
            vmem((rows, model), low),
            vmem((2, 8 * rows, model), low),
            vmem((blocks, n * depth, 2 * LANES), low),
            vmem((chunks, part, sub), low),
            vmem((2, 8 * rows, part), low),
            vmem((chunks + 1, 2, 2 * rows, sub), full),
            vmem((chunks + 1, 2, 2 * rows, sub), low),
            vmem((chunks + 1, 2, 2 * rows, sub), low),
            vmem((chunks + 1, 2, rows, sub // 2), low),
            vmem((chunks + 1, 2, rows, sub // 2), low),
            vmem((chunks + 1, 2, 2, rows, sub // 2), low),
            vmem((chunks + 1, 2, 2, rows, sub // 2), low),
            vmem((chunks + 1, rows, sub), full),
            vmem((rows, sub), low),
            vmem((rows, sub), low),
            vmem((rows, sub), low),
            vmem((rows, sub), low),
            vmem((rows, sub // 2), full),
            dma(()),
            dma(()),
            dma(()),
            dma((blocks,)),
            dma(()),
            dma(()),
            dma((4,)),
            dma((2,)),
            dma((12,)),
            dma((2,)),
            dma((3 * blocks,)),
            dma((2,)),
            dma((chunks,)),
            dma(()),
            dma((4, 2)),
            dma(()),
            dma((chunks + 1,)),
            dma(()),
            dma((chunks + 2 - 2 * cuts,)),
            dma(()),
        ],
        compiler_params=pltpu.CompilerParams(
            collective_id=0, has_side_effects=True, vmem_limit_bytes=56 * 2**20
        ),
    )(tokens, norm_gain.reshape(1, -1), w_gate, w_up, w_down, post_gain.reshape(1, -1))


def solution(mesh):
    n = mesh.shape["fs"]

    def body(tokens, norm_gain, w_gate, w_up, w_down, post_gain):
        args = (tokens, norm_gain, w_gate, w_up, w_down, post_gain)
        rows = tokens.shape[0]
        fits = (
            mesh.shape["rep"] == 2 and mesh.shape["tp"] == 4 and n == 4 and rows <= 128 and rows % 128 == 0
            and w_gate.shape[1] == 6 * LANES and w_down.shape[1] == 2 * PIECE
        )
        return chain_body(n, *args) if fits else plain_body(*args)

    return jax.shard_map(
        body,
        mesh=mesh,
        in_specs=(
            P(("rep", "fs", "tp"), None),
            P(),
            P("fs", "tp"),
            P("fs", "tp"),
            P("tp", "fs"),
            P(),
        ),
        out_specs=P(("rep", "fs", "tp"), None),
        check_vma=False,
    )
```

```python
import functools

import jax
import jax.numpy as jnp
from jax import lax
from jax.experimental import pallas as pl
from jax.experimental.pallas import tpu as pltpu
from jax.sharding import PartitionSpec as P

EPS = 1e-06
MESH = pl.DeviceIdType.MESH
PIECE = 256
LANES = 128


def rms_scale(values, gain):
    return values * lax.rsqrt(jnp.mean(values * values, axis=-1, keepdims=True) + EPS) * gain


def plain_body(tokens, norm_gain, w_gate, w_up, w_down, post_gain):
    own_normed = rms_scale(tokens.astype(jnp.float32), norm_gain).astype(jnp.bfloat16)
    normed = lax.all_gather(own_normed, "tp", axis=0, tiled=True)
    gate = jnp.dot(
        normed, lax.all_gather(w_gate, "fs", axis=0, tiled=True), preferred_element_type=jnp.float32
    )
    up = jnp.dot(
        normed, lax.all_gather(w_up, "fs", axis=0, tiled=True), preferred_element_type=jnp.float32
    )
    hidden = (jax.nn.silu(gate) * up).astype(jnp.bfloat16)
    terms = jnp.dot(
        hidden, lax.all_gather(w_down, "fs", axis=1, tiled=True), preferred_element_type=jnp.float32
    )
    summed = lax.psum_scatter(
        terms.astype(jnp.bfloat16), "tp", scatter_dimension=0, tiled=True
    ).astype(jnp.float32)
    return rms_scale(summed, post_gain).astype(jnp.bfloat16)


def kernel(
    n, rows, depth, part, width, cuts, lanes,
    tok_ref, gain_ref, wg_ref, wu_ref, wd_ref, post_ref, out_ref,
    gain, post, raw, tok, gu, dn, hid, kept, pair_out, pair_in, half_out, half_in, full_out, full_in, fin, res_out, res_in, diag_out, diag_in, squares,
    gain_l, post_l, tok_l, gu_l, dn_l, z_s, z_r, tok_s, tok_r, gu_s, gu_r, dn_s, dn_r,
    pair_s, pair_r, half_s, half_r, full_s, full_r, res_s,
):
    r, k, t = lax.axis_index("rep"), lax.axis_index("fs"), lax.axis_index("tp")
    x, c = t // 2, t % 2
    t_pair, t_x, r_y = x * 2 + (1 - c), (1 - x) * 2 + c, 1 - r
    t_px = (1 - x) * 2 + (1 - c)
    partner, along_x, along_y, diag = {"tp": t_pair}, {"tp": t_x}, {"rep": r_y}, {"rep": r_y, "tp": t_x}
    left = k < n // 2
    last = jnp.where(left, 0, n - 1)
    near = jnp.where(left, 1, n - 2)
    far_near, far_last = n - 1 - near, n - 1 - last
    at_end = k == last
    in_middle = k != last
    inner, outer = {"fs": jnp.where(left, k + 1, k - 1)}, {"fs": last}
    blocks = part // lanes
    sub = width // cuts
    half = pl.multiple_of(r * part, part)
    piece = rows // 4
    own_depth = pl.ds(pl.multiple_of(k * depth, depth), depth)

    def gu_load(b, q):
        ref = (wg_ref, wu_ref)[q]
        return pltpu.make_async_copy(
            ref.at[:, pl.ds(half + b * lanes, lanes)], gu.at[b, own_depth, pl.ds(q * lanes, lanes)], gu_l.at[b]
        )

    def dn_load(j):
        return pltpu.make_async_copy(wd_ref.at[pl.ds(half, part), pl.ds(j * sub, sub)], dn.at[k * cuts + j], dn_l)

    tok_load = pltpu.make_async_copy(tok_ref, raw, tok_l)
    gain_load = pltpu.make_async_copy(gain_ref, gain, gain_l)
    post_load = pltpu.make_async_copy(post_ref, post, post_l)

    tok_load.start()
    gain_load.start()

    barrier = pltpu.get_barrier_semaphore()
    for where in (partner, along_x, along_y, inner):
        pl.semaphore_signal(barrier, inc=1, device_id=where, device_id_type=MESH)

    @pl.when(in_middle)
    def _():
        pl.semaphore_signal(barrier, inc=1, device_id=outer, device_id_type=MESH)

    for b in range(blocks):
        for q in (0, 1):
            gu_load(b, q).start()
    for j in range(cuts):
        dn_load(j).start()
    post_load.start()

    tok_load.wait()
    gain_load.wait()
    tile = 32
    first = (r * 4 + x) * rows

    @pl.loop(0, rows // tile)
    def _(i):
        at = pl.ds(pl.multiple_of(i * tile, tile), tile)
        to = pl.ds(pl.multiple_of(first + i * tile, tile), tile)
        tok[0, to, :] = rms_scale(raw[at, :].astype(jnp.float32), gain[...]).astype(jnp.bfloat16)

    pl.semaphore_wait(barrier, 4 + jnp.where(in_middle, 1, 0))

    def remote(ref, send, recv, where, to=None):
        return pltpu.make_async_remote_copy(
            ref, ref if to is None else to, send, recv, device_id=where, device_id_type=MESH
        )

    pieces = 2
    step_depth = depth // pieces

    def gu_at(s, b, h):
        return gu.at[b, pl.ds(pl.multiple_of(s * depth + h * step_depth, step_depth), step_depth)]

    def gu_send(kind, b, h):
        at = jnp.where(in_middle, pieces * blocks + b, pieces * b + h)
        return remote(gu_at(last if kind else k, b, h), gu_s.at[kind], gu_r.at[at], inner)

    def gu_pass(b, h):
        remote(gu_at(last, b, h), gu_s.at[1], gu_r.at[pieces * b + h], inner).wait_recv()
        gu_send(1, b, h).start()

    def gu_wait(b):
        remote(gu.at[b, pl.ds(0, 2 * depth)], gu_s.at[0], gu_r.at[pieces * blocks + b], inner).wait_recv()

    def dn_send(way, s, j):
        at = s * cuts + j
        return remote(dn.at[at], dn_s.at[way], dn_r.at[at], outer if way else inner)

    def dn_wait(s, j):
        at = s * cuts + j
        remote(dn.at[at], dn_s.at[0], dn_r.at[at], inner).wait_recv()

    def pass_down(way, s, j):
        dn_wait(s, j)
        dn_send(way, s, j).start()

    def rows_of(p, r_at, t_at, first, count, core):
        other = (t_at % 2 + core) % 2
        base = (r_at * 4 + other * 2 + t_at // 2) * rows
        return tok.at[p, pl.ds(base + first * piece, count * piece)]

    def z_send(i):
        return remote(rows_of(0, r, t, i, 1, c), z_s, z_r.at[i], inner, rows_of(1, r, t, i, 1, c))

    def z_wait(i):
        remote(rows_of(1, r, t, i, 1, c), z_s, z_r.at[i], inner).wait_recv()

    sends = (
        [((r, t, i, 1), along_x) for i in range(4)]
        + [((r, t, i, 1), along_y) for i in range(4)]
        + [((r, t_x, 0, 1), along_y), ((r, t_x, 1, 1), along_y), ((r_y, t, 2, 1), along_x), ((r_y, t, 3, 1), along_x)]
        + [((r_at, t_at, i, 2), partner) for r_at, t_at in ((r, t), (r, t_x), (r_y, t), (r_y, t_x)) for i in (0, 2)]
    )
    groups = (
        ((0, 1, 6, 7), (2, 3, 4, 5), (8, 9, 10, 11), (12, 13, 14, 15), (16, 17, 18, 19)),
        ((0, 4), (1, 5), (6,), (2, 3, 7), (8, 9, 10, 11), (12, 13, 14, 15), (16, 17, 18, 19)),
    )

    def group_of(p, i):
        return [g for g, held in enumerate(groups[p]) if i in held][0]

    def go(p, *which):
        for i in which:
            at, where = sends[i]
            to = rows_of(p, *at, 1 - c if i >= 12 else c)
            remote(rows_of(p, *at, c), tok_s.at[p], tok_r.at[5 * p + group_of(p, i)], where, to).start()

    def got(p, *which):
        g = group_of(p, which[0])
        assert groups[p][g] == which
        count = sum(1 if i < 12 else 2 for i in which) * piece
        remote(tok.at[p, pl.ds(0, count)], tok_s.at[p], tok_r.at[5 * p + g], partner).wait_recv()

    quarter = 2 * rows
    halves = 4 * rows

    def half_rows(r_at):
        return pl.ds(pl.multiple_of(r_at * halves, halves), halves)

    def hid_at(p, b, r_at):
        return hid.at[p, half_rows(r_at), pl.ds(pl.multiple_of(b * lanes, lanes), lanes)]

    def hid_send(b, r_at):
        sem = jnp.where((b == 0) & (r_at == r), 2, r_at)
        return remote(hid_at(1, b, r_at), z_s, gu_r.at[sem], outer, hid_at(0, b, r_at))

    def hid_wait(r_at, first, count, sem):
        held = hid.at[0, half_rows(r_at), pl.ds(first * lanes, count * lanes)]
        remote(held, z_s, gu_r.at[sem], partner).wait_recv()

    def gated(p, b, r_at):
        both = jnp.dot(tok[p, half_rows(r_at), :], gu[b], preferred_element_type=jnp.float32)
        gate, up = both[:, :lanes], both[:, lanes:]
        hid_at(p, b, r_at)[...] = (gate / (1.0 + jnp.exp(-gate)) * up).astype(jnp.bfloat16)

    chunks = n * cuts
    mid = sub // 2
    here, there = 0, 1

    def pair_copy(at, side):
        p = place(at)
        return remote(pair_out.at[p, side], pair_s, pair_r.at[at % 4, side], partner, pair_in.at[p, side])

    def half_copy(p, way):
        return remote(
            half_out.at[p, way], half_s, half_r.at[p], along_y if way else along_x, half_in.at[p, way]
        )

    def full_sem(at):
        return full_r.at[jnp.maximum(at - early + 1, 0)]

    def full_copy(at, way, part_at):
        p = place(at)
        return remote(
            full_out.at[p, way, part_at], full_s, full_sem(at), along_y if way else along_x, full_in.at[p, way, part_at]
        )

    def source(i):
        near_or_last = jnp.where(i == 0, k, near + last - k)
        return jnp.where(i < 2, near_or_last, jnp.where(i == 2, far_near, far_last))

    def place(at):
        return jnp.where(at < chunks, source(at // cuts) * cuts + at % cuts, chunks)

    def product(at, side):
        p = place(at)
        held = jnp.where(at < chunks, p, far_last * cuts + cuts - 1)
        rows_at = half_rows(r_y if side == there else r)
        both = jnp.dot(hid[jnp.where(at < chunks, 0, 1), rows_at, :], dn[held], preferred_element_type=jnp.float32)
        pair_out[p, side] = both[quarter:].astype(jnp.bfloat16)
        pair_copy(at, side).start()
        kept[p, side] = both[:quarter]

    def send_own_gu():
        for b in range(blocks):
            pltpu.make_async_copy(gu.at[b, own_depth], gu.at[b, own_depth], gu_l.at[b]).wait()
            for h in range(pieces):
                gu_send(0, b, h).start()

    def send_own_dn(way):
        own = dn.at[pl.ds(k * cuts, cuts)]
        pltpu.make_async_copy(own, own, dn_l).wait()
        for j in range(cuts):
            dn_send(way, k, j).start()

    @pl.when(in_middle)
    def _():
        send_own_gu()
        send_own_dn(1)

    @pl.when(at_end)
    def _():
        for i in range(4):
            z_send(i).start()
        send_own_gu()
        hid_wait(r, 0, 1, 2)
        send_own_dn(0)

    @pl.when(in_middle)
    def _():
        @pl.loop(0, 12)
        def _(at_step):
            def step(at):
                return pl.when(at_step == at)

            @step(0)
            def _():
                go(0, 0, 1, 6, 7, 12, 13)
                z_wait(0)
                go(1, 0, 4)
                got(0, 0, 1, 6, 7)
                go(0, 14, 17)
                z_wait(1)
                go(1, 1, 5, 12)
                got(1, 0, 4)
                z_wait(2)
                go(1, 2, 6)
                got(1, 1, 5)
                go(1, 14, 16)
                z_wait(3)
                go(1, 13, 3, 7, 8, 9)
                got(1, 6)
                go(1, 10)
                gu_pass(0, 0)
                got(1, 2, 3, 7)
                go(1, 17, 11, 15)
                gu_pass(0, 1)
                go(0, 2, 4)
                gu_pass(1, 0)
                go(0, 3, 5)
                got(1, 8, 9, 10, 11)
                go(1, 18, 19)
                go(0, 8, 10)
                gu_pass(1, 1)
                got(1, 12, 13, 14, 15)
                gu_wait(0)

            @step(1)
            def _():
                got(1, 16, 17, 18, 19)

            @pl.when(at_step == 2 - c)
            def _():
                gu_pass(2, 0)

            @step(2)
            def _():
                go(0, 9, 11)
                got(0, 2, 3, 4, 5)
                go(0, 15, 16)
                gu_pass(2, 1)

            @pl.when(at_step == 2 + 4 * c)
            def _():
                for j in range(cuts):
                    dn_send(0, k, j).start()

            @step(2)
            def _():
                gu_wait(1)

            @step(4)
            def _():
                got(0, 12, 13, 14, 15)

            @step(6)
            def _():
                got(0, 8, 9, 10, 11)
                go(0, 18, 19)
                gu_wait(2)

            @step(8)
            def _():
                got(0, 16, 17, 18, 19)

            @step(10)
            def _():
                pass_down(0, last, 0)

            @step(11)
            def _():
                pl.loop(0, 2)(lambda at: product(at, there))
                pass_down(0, last, 1)

            passed = (at_step < 4) | (at_step == 6) | (at_step == 7)
            late = jnp.where(at_step < 8, 2, jnp.where(at_step < 11, at_step - 8, 2))
            b = jnp.where(at_step < 4, at_step // 2, jnp.where(at_step < 6, at_step - 4, late))
            first_r = jnp.where(at_step < 2, r, r_y)
            own_r = jnp.where((at_step < 6) | (at_step == 11), r, r_y)
            r_at = jnp.where(passed, (first_r + at_step % 2) % 2, own_r)
            gated(jnp.where(passed, 1, 0), b, r_at)

            @pl.when(passed)
            def _():
                hid_send(b, r_at).start()

    def of(m):
        return pl.ds(pl.multiple_of(m * rows, rows), rows)

    def summed(p, side, x_at):
        return kept[p, side, of(x_at), :] + pair_in[p, side, of(x_at), :].astype(jnp.float32)

    def finish_there(at):
        p = place(at)
        pair_copy(at, there).wait_recv()
        across = summed(p, there, 1 - x).astype(jnp.bfloat16)
        half_out[p, 0] = across[:, :mid]
        half_out[p, 1] = across[:, mid:]
        half_copy(p, 0).start()
        half_copy(p, 1).start()
        value = summed(p, there, x)
        kept[p, there, of(x), :mid] = value[:, :mid]
        full_out[p, 1, 1] = value[:, mid:].astype(jnp.bfloat16)
        full_copy(at, 1, 1).start()

    def finish_here(at):
        p = place(at)
        pair_copy(at, here).wait_recv()
        value = summed(p, here, 1 - x)
        kept[p, here, of(1 - x), mid:] = value[:, mid:]
        full_out[p, 0, 0] = value[:, :mid].astype(jnp.bfloat16)
        full_copy(at, 0, 0).start()
        fin[p] = summed(p, here, x)

    across_copy = remote(diag_out, res_s, z_r.at[1], diag, diag_in)

    def finish_direct(at):
        p = place(at)
        pair_copy(at, there).wait_recv()
        diag_out[...] = summed(p, there, 1 - x).astype(jnp.bfloat16)
        across_copy.start()
        value = summed(p, there, x).astype(jnp.bfloat16)
        for part_at in (1, 0):
            full_out[p, 1, part_at] = value[:, part_at * mid : (part_at + 1) * mid]
            full_copy(at, 1, part_at).start()
        pair_copy(at, here).wait_recv()
        value = summed(p, here, 1 - x).astype(jnp.bfloat16)
        for part_at in (0, 1):
            full_out[p, 0, part_at] = value[:, part_at * mid : (part_at + 1) * mid]
            full_copy(at, 0, part_at).start()
        fin[p] = summed(p, here, x)

    def finish_half(at):
        p = place(at)
        remote(half_in.at[p], half_s, half_r.at[p], partner).wait_recv()
        full_out[p, 0, 1] = (kept[p, here, of(1 - x), mid:] + half_in[p, 1].astype(jnp.float32)).astype(jnp.bfloat16)
        full_copy(at, 0, 1).start()
        full_out[p, 1, 0] = (kept[p, there, of(x), :mid] + half_in[p, 0].astype(jnp.float32)).astype(jnp.bfloat16)
        full_copy(at, 1, 0).start()

    early = 2 * cuts

    @pl.when(at_end)
    def _():
        for j in range(cuts):
            dn_wait(near, j)
        hid_wait(r_y, 0, blocks, r_y)

    @pl.loop(0, early)
    def _(at):
        @pl.when(at_end | (at > 1))
        def _():
            product(at, there)

        @pl.when(at > 0)
        def _():
            finish_there(at - 1)

        @pl.when(in_middle & (at == 0))
        def _():
            pass_down(1, far_near, 0)

    @pl.when(at_end)
    def _():
        hid_wait(r, 1, blocks - 1, r)

    @pl.loop(0, early)
    def _(at):
        product(at, here)

        @pl.when(at == 0)
        def _():
            finish_there(early - 1)

        @pl.when(at > 0)
        def _():
            finish_here(at - 1)
            finish_half(at - 1)

        @pl.when(in_middle & (at == 2))
        def _():
            pass_down(1, far_near, 1)


    result = remote(res_out, res_s, z_r.at[0], outer, res_in)

    def collect(at, part_at):
        p = place(at)
        cols = pl.ds(part_at * mid, mid)
        both = full_in[p, 0, part_at].astype(jnp.float32) + full_in[p, 1, part_at].astype(jnp.float32)
        return fin[p, :, cols] + both

    def arrive(at):
        remote(full_in.at[place(at)], full_s, full_sem(at), along_x).wait_recv()

    def order(i):
        return jnp.where(in_middle & (i >= 2), jnp.where(i == 2, chunks, early + i - 1), early + i)

    @pl.loop(0, chunks - early + 1)
    def _(i):
        at = order(i)

        @pl.when(at_end & (i < 3))
        def _():
            dn_wait(source(at // cuts), at % cuts)

        @pl.when(in_middle & (i == 0) & (c == 0))
        def _():
            pass_down(1, far_last, 0)

        @pl.when(in_middle & (i == 2))
        def _():
            dn_wait(far_last, cuts - 1)

        @pl.when(in_middle | (i < 3))
        def _():
            product(at, there)
            product(at, here)

        @pl.when(i == 0)
        def _():
            finish_here(early - 1)
            finish_half(early - 1)

        @pl.when(in_middle & (i == 3))
        def _():
            finish_half(chunks)

        @pl.when(in_middle | (i < 2))
        def _():
            finish_there(at)
            finish_here(at)

        @pl.when(at_end & (i == 2))
        def _():
            finish_direct(at)

        @pl.when(in_middle & (i == 1) & (c == 1))
        def _():
            pass_down(1, far_last, 0)

        @pl.when(in_middle & (i == 4))
        def _():
            arrive(chunks)
            for part_at in (0, 1):
                res_out[:, pl.ds(part_at * mid, mid)] = collect(chunks, part_at).astype(jnp.bfloat16)
            result.start()

        @pl.when((i > 0) & (i != 3) & (in_middle | (i < 3)))
        def _():
            finish_half(order(i - 1))

    @pl.when(in_middle)
    def _():
        finish_half(chunks - 1)

    remote(gu.at[:, pl.ds(0, depth)], gu_s.at[0], gu_r.at[0], inner).wait_send()

    @pl.when(at_end)
    def _():
        remote(tok.at[0, pl.ds(0, rows)], z_s, z_r.at[0], inner).wait_send()
        remote(dn.at[pl.ds(0, cuts)], dn_s.at[0], dn_r.at[0], inner).wait_send()
        remote(pair_out.at[pl.ds(0, chunks - 1)], pair_s, pair_r.at[0, 0], partner).wait_send()
        remote(half_out.at[pl.ds(0, chunks - 2)], half_s, half_r.at[0], along_x).wait_send()
        across_copy.wait_send()

    @pl.when(in_middle)
    def _():
        for p in (0, 1):
            total = sum(1 if i < 12 else 2 for i in range(len(sends))) * piece
            remote(tok.at[p, pl.ds(0, total)], tok_s.at[p], tok_r.at[p], partner).wait_send()
        remote(gu.at[:, pl.ds(0, depth)], gu_s.at[1], gu_r.at[0], inner).wait_send()
        remote(hid.at[1], z_s, gu_r.at[0], outer).wait_send()
        remote(dn.at[pl.ds(0, 2 * cuts)], dn_s.at[0], dn_r.at[0], inner).wait_send()
        remote(dn.at[pl.ds(0, 3 * cuts - 1)], dn_s.at[1], dn_r.at[0], outer).wait_send()
        remote(pair_out, pair_s, pair_r.at[0, 0], partner).wait_send()
        remote(half_out, half_s, half_r.at[0], along_x).wait_send()

    squares[...] = jnp.zeros_like(squares)

    def settle(at, part_at, total):
        fin[place(at), :, pl.ds(part_at * mid, mid)] = total
        squares[...] += total * total

    @pl.loop(0, chunks)
    def _(at):
        @pl.when(at == 0)
        def _():
            remote(full_in.at[pl.ds(0, early)], full_s, full_sem(0), along_x).wait_recv()

        @pl.when((at >= early) & (in_middle | (at < chunks - 2)))
        def _():
            arrive(at)

        @pl.when(in_middle | (at < chunks - 2))
        def _():
            for part_at in (0, 1):
                settle(at, part_at, collect(at, part_at))

    @pl.when(at_end)
    def _():
        across_copy.wait_recv()
        p = place(chunks - 2)
        for part_at in (0, 1):
            cols = pl.ds(part_at * mid, mid)
            fin[p, :, cols] = fin[p, :, cols] + diag_in[:, cols].astype(jnp.float32)
        arrive(chunks - 2)
        for part_at in (0, 1):
            settle(chunks - 2, part_at, collect(chunks - 2, part_at))
        result.wait_recv()
        for part_at in (0, 1):
            settle(chunks - 1, part_at, res_in[:, pl.ds(part_at * mid, mid)].astype(jnp.float32))

    post_load.wait()
    scale = lax.rsqrt(jnp.sum(squares[...], axis=-1, keepdims=True) / (n * width) + EPS)
    for p in range(chunks):
        cols = pl.ds(p * sub, sub)
        out_ref[:, cols] = (fin[p] * scale * post[:, cols]).astype(out_ref.dtype)

    @pl.when(at_end)
    def _():
        remote(full_out.at[pl.ds(0, chunks - 1)], full_s, full_r.at[0], along_x).wait_send()

    @pl.when(in_middle)
    def _():
        remote(full_out, full_s, full_r.at[0], along_x).wait_send()
        result.wait_send()


def chain_body(n, tokens, norm_gain, w_gate, w_up, w_down, post_gain):
    rows, model = tokens.shape
    depth, block = w_gate.shape
    width = w_down.shape[1]
    part = block // 2
    cuts = width // PIECE
    sub = width // cuts
    blocks = part // LANES
    chunks = n * cuts
    vmem, dma = pltpu.VMEM, pltpu.SemaphoreType.DMA
    low, full = jnp.bfloat16, jnp.float32
    anywhere = pl.BlockSpec(memory_space=pl.ANY)
    inside = pl.BlockSpec(memory_space=vmem)
    return pl.pallas_call(
        functools.partial(kernel, n, rows, depth, part, width, cuts, LANES),
        out_shape=pltpu.VMEM((rows, model), low),
        in_specs=[anywhere] * 6,
        out_specs=inside,
        scratch_shapes=[
            vmem((1, model), full),
            vmem((1, model), full),
            vmem((rows, model), low),
            vmem((2, 8 * rows, model), low),
            vmem((blocks, n * depth, 2 * LANES), low),
            vmem((chunks, part, sub), low),
            vmem((2, 8 * rows, part), low),
            vmem((chunks + 1, 2, 2 * rows, sub), full),
            vmem((chunks + 1, 2, 2 * rows, sub), low),
            vmem((chunks + 1, 2, 2 * rows, sub), low),
            vmem((chunks + 1, 2, rows, sub // 2), low),
            vmem((chunks + 1, 2, rows, sub // 2), low),
            vmem((chunks + 1, 2, 2, rows, sub // 2), low),
            vmem((chunks + 1, 2, 2, rows, sub // 2), low),
            vmem((chunks + 1, rows, sub), full),
            vmem((rows, sub), low),
            vmem((rows, sub), low),
            vmem((rows, sub), low),
            vmem((rows, sub), low),
            vmem((rows, sub // 2), full),
            dma(()),
            dma(()),
            dma(()),
            dma((blocks,)),
            dma(()),
            dma(()),
            dma((4,)),
            dma((2,)),
            dma((12,)),
            dma((2,)),
            dma((3 * blocks,)),
            dma((2,)),
            dma((chunks,)),
            dma(()),
            dma((4, 2)),
            dma(()),
            dma((chunks + 1,)),
            dma(()),
            dma((chunks + 2 - 2 * cuts,)),
            dma(()),
        ],
        compiler_params=pltpu.CompilerParams(
            collective_id=0, has_side_effects=True, vmem_limit_bytes=56 * 2**20
        ),
    )(tokens, norm_gain.reshape(1, -1), w_gate, w_up, w_down, post_gain.reshape(1, -1))


def solution(mesh):
    n = mesh.shape["fs"]

    def body(tokens, norm_gain, w_gate, w_up, w_down, post_gain):
        args = (tokens, norm_gain, w_gate, w_up, w_down, post_gain)
        rows = tokens.shape[0]
        fits = (
            mesh.shape["rep"] == 2 and mesh.shape["tp"] == 4 and n == 4 and rows <= 128 and rows % 128 == 0
            and w_gate.shape[1] == 6 * LANES and w_down.shape[1] == 2 * PIECE
        )
        return chain_body(n, *args) if fits else plain_body(*args)

    return jax.shard_map(
        body,
        mesh=mesh,
        in_specs=(
            P(("rep", "fs", "tp"), None),
            P(),
            P("fs", "tp"),
            P("fs", "tp"),
            P("tp", "fs"),
            P(),
        ),
        out_specs=P(("rep", "fs", "tp"), None),
        check_vma=False,
    )
```
